32 devices in a mesh: sp: 16 (over z, y, x), tp: 2 (over core).
Axes of the slice: x: 2, y: 2, z: 4, core: 2. Of those that a mesh axis runs over, the one named last changes fastest.
Arguments:
- mixer_output: bfloat16 [2048, 2048], P('sp'), may hold values from -6 to 6
- layer_cotangent: bfloat16 [2048, 2048], P('sp'), may hold values from -6 to 6
- expert_choice: int32 [2048, 2], P('sp'), may hold values from 0 to 15, all different within a row; in each aligned block of 128 rows (0 to 127, 128 to 255, ...) at most 32 rows name the same one
- route_weight: float32 [2048, 2], P('sp'), may hold values from 0.1 to 0.9
- gate_pre: bfloat16 [16, 512, 1024], P('sp', None, 'tp'), may hold values from -15 to 15
- up_pre: bfloat16 [16, 512, 1024], P('sp', None, 'tp'), may hold values from -15 to 15
- w_gate: bfloat16 [16, 2048, 1024], P('sp', None, 'tp'), may hold values from -0.125 to 0.125
- w_up: bfloat16 [16, 2048, 1024], P('sp', None, 'tp'), may hold values from -0.125 to 0.125
- w_down: bfloat16 [16, 1024, 2048], P('sp', 'tp'), may hold values from -0.1875 to 0.1875
- w_out: bfloat16 [2048, 2048], P('tp'), may hold values from -0.125 to 0.125
- norm_gain: bfloat16 [2048], P('tp'), may hold values from 0.099609375 to 1.8984375
- scan_in: bfloat16 [2048, 2048], P('sp', 'tp'), may hold values from -6 to 6
- gate_in: bfloat16 [2048, 2048], P('sp', 'tp'), may hold values from -9 to 9
- b_proj: bfloat16 [2048, 1024], P('sp', 'tp'), may hold values from -1.796875 to 1.796875
- c_proj: bfloat16 [2048, 1024], P('sp', 'tp'), may hold values from -1.796875 to 1.796875
- log_decay: float32 [2048, 32], P('sp', 'tp'), may hold values from -3 to 0
- entry_state: float32 [16, 32, 64, 128], P('sp', 'tp'), may hold values from -24 to 24
Outputs:
- grad_w_gate: bfloat16 [16, 2048, 1024], P('sp', None, 'tp')
- grad_w_up: bfloat16 [16, 2048, 1024], P('sp', None, 'tp')
- grad_w_down: bfloat16 [16, 1024, 2048], P('sp', 'tp')
- grad_out_proj: float32 [2048, 2048], P('sp', 'tp')
- grad_scan_in: bfloat16 [2048, 2048], P('sp', 'tp')
- grad_gate_in: bfloat16 [2048, 2048], P('sp', 'tp')
- grad_b_proj: bfloat16 [2048, 1024], P('sp', 'tp')
- grad_c_proj: bfloat16 [2048, 1024], P('sp', 'tp')
- grad_log_decay: float32 [2048, 32], P('sp', 'tp')
The draws below stay inside these ranges and needn't reach their ends.
Inputs may be any that keep to these rules, and one draw needn't show every extreme that they name: `expert_choice`: in the 128 rows of one device no expert is named more than 32 times, a bound that some blocks reach; the 2 entries of a row differ.
All inputs are finite; a program needn't handle non-finite values.
Results may differ from the reference program's by a relative error of at most 0.012.
Values may be sent and summed in bfloat16 or wider, within the bound.
A program may use at most 192 MiB of HBM per device.

```python
import math
from functools import partial
import jax
import jax.numpy as jnp
import numpy as np
from jax import lax

D = 2048
MIXER_HEADS = 32
HEAD_DIM = 64
GROUPS = 8
STATE = 128
FF = 1024
TOPK = 2
TOK_DEV = 128
SEQUENCE_TOKENS = 2048
EXPERTS = 16
INNER = 2048
CAP = 32
EXPERT_ROWS = 512
N_SP = 16
N_TP = 2


def draw_log_decay(key, part):
    random_keys_split = jax.random.split(key, 7)
    fast_share = 0.5
    is_fast = jax.random.uniform(random_keys_split[0], (MIXER_HEADS,)) < fast_share
    fast_rate = jax.random.uniform(random_keys_split[1], (MIXER_HEADS,), minval=1.0 / 100.0, maxval=1.0 / 30.0)
    slow_rate = jax.random.uniform(random_keys_split[2], (MIXER_HEADS,), minval=0.05, maxval=0.3) * math.log(10.0) / SEQUENCE_TOKENS
    base_rate = jnp.where(is_fast, fast_rate, slow_rate)
    block_count = SEQUENCE_TOKENS // TOK_DEV
    block_factor = jnp.exp(jax.random.uniform(random_keys_split[3], (block_count, 1, MIXER_HEADS), minval=math.log(0.5), maxval=math.log(2.0)))
    token_factor = jnp.exp(jax.random.uniform(random_keys_split[4], (block_count, TOK_DEV, MIXER_HEADS), minval=math.log(0.5), maxval=math.log(2.0)))
    decay_rate_table = (base_rate[None, None, :] * block_factor * token_factor).reshape(SEQUENCE_TOKENS, MIXER_HEADS)
    spike_positions = jax.random.randint(random_keys_split[5], (3, MIXER_HEADS), 0, SEQUENCE_TOKENS)
    spike_length = jnp.log(jax.random.uniform(random_keys_split[6], (3, MIXER_HEADS), minval=0.5, maxval=0.8))
    token_locations = jnp.arange(SEQUENCE_TOKENS)[:, None]
    spike_events = jnp.zeros((SEQUENCE_TOKENS, MIXER_HEADS), jnp.float32)
    for event_count in range(3):
        spike_events = spike_events + jnp.where(token_locations == spike_positions[event_count][None, :], spike_length[event_count][None, :], 0.0)
    return (spike_events - decay_rate_table).astype(jnp.float32)


def raised(drawn, rng, source, target, parts, factor):
    owner, partner = [(jnp.arange(drawn.shape[dim]) // (drawn.shape[dim] // parts)).reshape([-1 if axis == dim else 1 for axis in range(drawn.ndim)]) for dim in (source, target)]
    chosen = jax.random.permutation(rng, parts)[partner]
    strong = (owner == chosen) | (owner == (partner + parts // 2) % parts)
    return jnp.where(strong, factor * drawn, drawn)


def steps_of(key, extent, shards, low, top_value):
    loudness, own = 1.0, jax.random.fold_in(key, 6)
    for dim, blocks in shards:
        draws = jnp.exp(jax.random.uniform(jax.random.fold_in(own, dim), (blocks,), jnp.float32, low / len(shards), top_value / len(shards)))
        loudness = loudness * jnp.repeat(draws, extent[dim] // blocks).reshape([-1 if axis == dim else 1 for axis in range(len(extent))])
    return loudness


def shared_out(own_key, own, number, rows, count, top, most, lean):
    ranking = jax.random.permutation(own_key, count)
    crowded, usual = load_shares(count, rows * top, most, lean, True), load_shares(count, rows * top, most, lean, False)
    places = jnp.arange(count)

    def named(sizes, offset_by):
        used = int((sizes > 0).sum())
        fixed = max(1, used // 4)
        shifted = fixed + (places - fixed + offset_by * (used - fixed)) % max(1, count - fixed)
        return jnp.zeros((count,), jnp.int32).at[ranking[jnp.where(places < fixed, places, shifted)]].set(jnp.asarray(sizes, jnp.int32))

    sizes = jnp.where(number % 4 == 0, named(crowded, number // 4), named(usual, number - number // 4 - 1))
    mixed = jax.random.permutation(jax.random.fold_in(own, 3), count)
    giver, sink = mixed[0:count // 2 * 2:2], mixed[1:count // 2 * 2:2]
    room = jnp.minimum(sizes[giver] - 1, most - sizes[sink]) // 2
    room = jnp.where((giver == ranking[0]) | (sink == ranking[0]) | (sizes[sink] == 0), 0, jnp.maximum(room, 0))
    shifted = jax.random.randint(jax.random.fold_in(own, 4), (count // 2,), 0, 1 << 20) % (room + 1)
    sizes = sizes.at[giver].add(-shifted).at[sink].add(shifted)
    items = jnp.searchsorted(jnp.cumsum(sizes), jnp.arange(rows * top), side="right").astype(jnp.int32)
    listing = items.reshape(top, rows).T
    listing = listing[jax.random.permutation(jax.random.fold_in(own, 1), rows)]
    offset_by = jax.random.randint(jax.random.fold_in(own, 2), (rows, 1), 0, top)
    return jnp.take_along_axis(listing, (jnp.arange(top)[None, :] + offset_by) % top, axis=1)


def load_shares(number_of, total, most, skew, full):
    portions = [(1 << 20) // math.isqrt(grade ** skew) + 1 for grade in range(1, number_of + 1)]
    largest = most if full else min(most, max(-(-total // number_of), total * portions[0] // sum(portions)))
    least = 1 if total - largest >= number_of - 1 else 0
    given, surplus = [largest] + [least] * (number_of - 1), total - largest - least * (number_of - 1)
    while surplus > 0:
        candidates = [i for i in range(1, number_of) if given[i] < largest] or [i for i in range(1, number_of) if given[i] < most]
        whole, remaining = sum([portions[i] for i in candidates]), surplus
        for i in candidates:
            extra = min(most - given[i], max(1, remaining * portions[i] // whole), surplus)
            given[i] = given[i] + extra
            surplus = surplus - extra
    return np.array(given)


def normal_values(stream_key, dims, deviation, reach, cuts=(), kind=jnp.bfloat16):
    drawn = deviation * jax.random.normal(stream_key, dims, jnp.float32)
    if cuts:
        drawn = drawn * steps_of(stream_key, dims, cuts, -0.22, 0.18)
    return jnp.clip(drawn, -reach, reach).astype(kind)


def bell_draw_with(own_key, extent, spread, bound, cuts, heavy, kind=jnp.bfloat16):
    values = spread * jax.random.normal(own_key, extent, jnp.float32)
    if cuts:
        values = values * steps_of(own_key, extent, cuts, -0.22, 0.18)
    return jnp.clip(raised(values, jax.random.fold_in(own_key, 3), *heavy), -bound, bound).astype(kind)


def setup_inputs(seed: int = 0) -> dict:
    streams_of = jax.random.split(jax.random.key(seed), 18)
    mixer_output = normal_values(streams_of[0], (SEQUENCE_TOKENS, D), 1.0, 6.0, ((0, 16),))
    layer_cotangent = bell_draw_with(streams_of[1], (SEQUENCE_TOKENS, D), 1.0, 6.0, ((0, 16),), (0, 1, 16, 2.0))
    expert_choice_keys = jax.random.split(jax.random.fold_in(streams_of[2], 1), SEQUENCE_TOKENS // TOK_DEV)
    expert_choice_turns = jax.random.permutation(jax.random.fold_in(streams_of[2], 3), SEQUENCE_TOKENS // TOK_DEV)
    expert_choice = jax.vmap(lambda own, number: shared_out(jax.random.fold_in(streams_of[2], 2), own, number, TOK_DEV, EXPERTS, TOPK, CAP, 1))(expert_choice_keys, expert_choice_turns).reshape((SEQUENCE_TOKENS, TOPK))
    route_weight = jnp.clip(0.1 + 0.79999997 * jax.random.uniform(streams_of[3], (SEQUENCE_TOKENS, TOPK), jnp.float32) ** steps_of(streams_of[3], (SEQUENCE_TOKENS, TOPK), ((0, 16),), -0.2, 0.2), 0.1, 0.9)
    gate_pre = normal_values(streams_of[4], (EXPERTS, EXPERT_ROWS, FF), 3.0, 15.0, ((0, 16), (2, 2)))
    up_pre = normal_values(streams_of[5], (EXPERTS, EXPERT_ROWS, FF), 3.0, 15.0, ((0, 16), (2, 2)))
    w_gate = normal_values(streams_of[6], (EXPERTS, D, FF), D ** -0.5, 0.125, ((0, 16), (2, 2)))
    w_up = normal_values(streams_of[7], (EXPERTS, D, FF), D ** -0.5, 0.125, ((0, 16), (2, 2)))
    w_down = normal_values(streams_of[8], (EXPERTS, FF, D), FF ** -0.5, 0.1875, ((0, 16), (1, 2)))
    w_out = normal_values(streams_of[9], (INNER, D), INNER ** -0.5, 0.125, ((0, 2),))
    norm_gain = jnp.clip(1.0 + 0.18 * jax.random.normal(streams_of[10], (INNER,), jnp.float32), 0.099609375, 1.8984375).astype(jnp.bfloat16)
    scan_in = normal_values(streams_of[11], (SEQUENCE_TOKENS, INNER), 1.0, 6.0, ((0, 16), (1, 2)))
    gate_in = normal_values(streams_of[12], (SEQUENCE_TOKENS, INNER), 1.5, 9.0, ((0, 16), (1, 2)))
    b_proj = normal_values(streams_of[13], (SEQUENCE_TOKENS, GROUPS * STATE), 0.3, 1.796875, ((0, 16), (1, 2)))
    c_proj = normal_values(streams_of[14], (SEQUENCE_TOKENS, GROUPS * STATE), 0.3, 1.796875, ((0, 16), (1, 2)))
    log_decay = draw_log_decay(jax.random.fold_in(streams_of[17], 71), 0)
    entry_state = normal_values(streams_of[16], (N_SP, MIXER_HEADS, HEAD_DIM, STATE), 4.0, 24.0, ((0, 16), (1, 2)), jnp.float32)
    return {"mixer_output": mixer_output, "layer_cotangent": layer_cotangent, "expert_choice": expert_choice, "route_weight": route_weight, "gate_pre": gate_pre, "up_pre": up_pre, "w_gate": w_gate, "w_up": w_up, "w_down": w_down, "w_out": w_out, "norm_gain": norm_gain, "scan_in": scan_in, "gate_in": gate_in, "b_proj": b_proj, "c_proj": c_proj, "log_decay": log_decay, "entry_state": entry_state}


rms_epsilon = 1e-05
clamp_limit = 7.0
swish_alpha = 1.702

def slot_ranks(expert_ids, expert_count):
    targets = expert_ids.reshape(-1)
    one_hot = (targets[:, None] == jnp.arange(expert_count, dtype=jnp.int32)[None, :]).astype(jnp.int32)
    earlier = jnp.cumsum(one_hot, axis=0) - one_hot
    return (targets, lax.optimization_barrier(jnp.sum(earlier * one_hot, axis=1)).astype(jnp.int32))

def fill_slots(rows, targets, ranked):
    buffer = jnp.zeros((N_SP, CAP, rows.shape[1]), rows.dtype)
    return buffer.at[targets, ranked].set(rows)

def pick_rows(buffer, targets, ranked):
    return buffer[targets, ranked]

def expert_ref(inputs):
    hidden_rows, grad_rows, gate_value, up_value, gate_weight, up_weight, down_weight = inputs
    act_grad = jnp.dot(grad_rows, down_weight.T, preferred_element_type=jnp.float32)
    gate_full = gate_value.astype(jnp.float32)
    up_full = up_value.astype(jnp.float32)
    gate_clip = jnp.minimum(gate_full, clamp_limit)
    up_clip = jnp.clip(up_full, -clamp_limit, clamp_limit)
    sigmoid_gate = jax.nn.sigmoid(swish_alpha * gate_clip)
    swish_gate = gate_clip * sigmoid_gate
    active = ((up_clip + 1.0) * swish_gate).astype(jnp.bfloat16)
    up_grad = jnp.where((up_full > -clamp_limit) & (up_full < clamp_limit), act_grad * swish_gate, 0.0).astype(jnp.bfloat16)
    slope = sigmoid_gate + swish_alpha * gate_clip * sigmoid_gate * (1.0 - sigmoid_gate)
    gate_grad = jnp.where(gate_full < clamp_limit, act_grad * (up_clip + 1.0) * slope, 0.0).astype(jnp.bfloat16)
    down_wgrad = jnp.dot(active.T, grad_rows, preferred_element_type=jnp.float32).astype(jnp.bfloat16)
    gate_wgrad = jnp.dot(hidden_rows.T, gate_grad, preferred_element_type=jnp.float32).astype(jnp.bfloat16)
    up_wgrad = jnp.dot(hidden_rows.T, up_grad, preferred_element_type=jnp.float32).astype(jnp.bfloat16)
    row_count = gate_grad.shape[0]
    part_width = FF // N_TP
    gate_split = gate_grad.reshape(row_count, N_TP, part_width).astype(jnp.float32)
    up_split = up_grad.reshape(row_count, N_TP, part_width).astype(jnp.float32)
    gate_parts = gate_weight.reshape(D, N_TP, part_width).astype(jnp.float32)
    up_parts = up_weight.reshape(D, N_TP, part_width).astype(jnp.float32)
    partial_rows = jnp.einsum('rjf,djf->jrd', gate_split, gate_parts) + jnp.einsum('rjf,djf->jrd', up_split, up_parts)
    rounded = lax.optimization_barrier(partial_rows.astype(jnp.bfloat16))
    back_rows = lax.optimization_barrier(jnp.sum(rounded.astype(jnp.float32), axis=0)).astype(jnp.bfloat16)
    return (gate_wgrad, up_wgrad, down_wgrad, back_rows)

def block_step(carry, inputs, w_out, norm_gain):
    later_state, later_grad = carry
    scan_block, gate_block, b_block, c_block, decay_block, state_block, hidden_block = inputs
    length = scan_block.shape[0]
    per_group = MIXER_HEADS // GROUPS
    scan_heads = scan_block.reshape(length, MIXER_HEADS, HEAD_DIM).astype(jnp.float32)
    b_groups = b_block.reshape(length, GROUPS, STATE).astype(jnp.float32)
    c_groups = c_block.reshape(length, GROUPS, STATE).astype(jnp.float32)
    cumulative = jnp.cumsum(decay_block, axis=0)
    growth = jnp.exp(cumulative)
    tail_decay = jnp.exp(cumulative[-1][None, :] - cumulative)
    token_locations = jnp.arange(length)
    causal = token_locations[:, None] >= token_locations[None, :]
    log_gaps = cumulative.T[:, :, None] - cumulative.T[:, None, :]
    decay_mat = jnp.exp(jnp.where(causal[None], log_gaps, -jnp.inf))
    inner_prod = jnp.einsum('tgn,sgn->gts', c_groups, b_groups)
    mix_weights = (jnp.repeat(inner_prod, per_group, axis=0) * decay_mat).astype(jnp.bfloat16).astype(jnp.float32)
    state_groups = state_block.reshape(GROUPS, per_group, HEAD_DIM, STATE)
    y_inner = jnp.einsum('hts,shp->thp', mix_weights, scan_heads)
    y_carry = jnp.einsum('tgn,grpn->tgrp', c_groups, state_groups, precision=lax.Precision.HIGHEST).reshape(length, MIXER_HEADS, HEAD_DIM)
    scan_out = y_inner + y_carry * growth[:, :, None]
    gate_float = gate_block.astype(jnp.float32)
    gate_sig = jax.nn.sigmoid(gate_float)
    gate_silu = gate_float * gate_sig
    gated = scan_out.reshape(length, -1) * gate_silu
    grouped = gated.reshape(length, GROUPS, -1)
    inv_rms = lax.rsqrt(lax.optimization_barrier(jnp.mean(grouped * grouped, axis=-1, keepdims=True)) + rms_epsilon)
    unit = grouped * inv_rms
    gain_groups = norm_gain.astype(jnp.float32).reshape(GROUPS, -1)
    mixed = (unit * gain_groups).reshape(length, -1).astype(jnp.bfloat16)
    grad_mixed = jnp.dot(hidden_block, w_out.T, preferred_element_type=jnp.float32)
    grad_unit = grad_mixed.reshape(length, GROUPS, -1) * gain_groups
    grad_grouped = inv_rms * (grad_unit - unit * lax.optimization_barrier(jnp.mean(grad_unit * unit, axis=-1, keepdims=True)))
    grad_gated = grad_grouped.reshape(length, -1)
    grad_gate = (grad_gated * scan_out.reshape(length, -1) * gate_sig * (1.0 + gate_float * (1.0 - gate_sig))).astype(jnp.bfloat16)
    grad_y = (grad_gated * gate_silu).reshape(length, MIXER_HEADS, HEAD_DIM)
    grad_y_b = grad_y.astype(jnp.bfloat16).astype(jnp.float32)
    grad_x_inner = jnp.einsum('hts,thp->shp', mix_weights, grad_y_b)
    grad_weights = (jnp.einsum('thp,shp->hts', grad_y_b, scan_heads) * decay_mat).reshape(GROUPS, per_group, length, length).sum(axis=1)
    grad_weights = grad_weights.astype(jnp.bfloat16).astype(jnp.float32)
    grad_c_inner = jnp.einsum('gts,sgn->tgn', grad_weights, b_groups)
    grad_b_inner = jnp.einsum('gts,tgn->sgn', grad_weights, c_groups)
    grown_grads = (grad_y * growth[:, :, None]).reshape(length, GROUPS, per_group, HEAD_DIM)
    grad_c_carry = jnp.einsum('tgrp,grpn->tgn', grown_grads, state_groups, precision=lax.Precision.HIGHEST)
    block_state = jnp.einsum('tgrp,tgn->grpn', grown_grads, c_groups, precision=lax.Precision.HIGHEST).reshape(MIXER_HEADS, HEAD_DIM, STATE)
    later_groups = later_state.reshape(GROUPS, per_group, HEAD_DIM, STATE)
    grad_x_carry = jnp.einsum('sgn,grpn->sgrp', b_groups, later_groups, precision=lax.Precision.HIGHEST).reshape(length, MIXER_HEADS, HEAD_DIM)
    grad_x = grad_x_inner + grad_x_carry * tail_decay[:, :, None]
    x_tail = (scan_heads * tail_decay[:, :, None]).reshape(length, GROUPS, per_group, HEAD_DIM)
    grad_b_carry = jnp.einsum('sgrp,grpn->sgn', x_tail, later_groups, precision=lax.Precision.HIGHEST)
    grad_a = lax.optimization_barrier(jnp.sum(grad_y * scan_out, axis=2)) - lax.optimization_barrier(jnp.sum(scan_heads * grad_x, axis=2))
    grad_decay = jnp.flip(jnp.cumsum(jnp.flip(grad_a, 0), axis=0), 0) + later_grad[None, :]
    new_state = block_state + jnp.exp(cumulative[-1])[:, None, None] * later_state
    new_grad = later_grad + lax.optimization_barrier(jnp.sum(grad_a, axis=0))
    outputs = (grad_x.reshape(length, -1).astype(jnp.bfloat16), grad_gate, (grad_b_inner + grad_b_carry).reshape(length, -1).astype(jnp.bfloat16), (grad_c_inner + grad_c_carry).reshape(length, -1).astype(jnp.bfloat16), grad_decay, mixed)
    return ((new_state, new_grad), outputs)

def reference(mixer_output, layer_cotangent, expert_choice, route_weight, gate_pre, up_pre, w_gate, w_up, w_down, w_out, norm_gain, scan_in, gate_in, b_proj, c_proj, log_decay, entry_state):
    id_blocks = expert_choice.reshape(N_SP, TOK_DEV, TOPK)
    targets, ranked = jax.vmap(partial(slot_ranks, expert_count=N_SP))(id_blocks)
    token_of = jnp.arange(SEQUENCE_TOKENS * TOPK, dtype=jnp.int32) // TOPK
    hidden_rows = mixer_output[token_of].reshape(N_SP, TOK_DEV * TOPK, D)
    grad_rows = (route_weight.reshape(-1)[:, None] * layer_cotangent[token_of].astype(jnp.float32)).astype(jnp.bfloat16)
    grad_rows = grad_rows.reshape(N_SP, TOK_DEV * TOPK, D)
    send_hidden = jax.vmap(fill_slots)(hidden_rows, targets, ranked)
    send_grads = jax.vmap(fill_slots)(grad_rows, targets, ranked)
    recv_hidden = jnp.transpose(send_hidden, (1, 0, 2, 3)).reshape(N_SP, N_SP * CAP, D)
    recv_grads = jnp.transpose(send_grads, (1, 0, 2, 3)).reshape(N_SP, N_SP * CAP, D)
    gate_wgrad, up_wgrad, down_wgrad, back_rows = lax.map(expert_ref, (recv_hidden, recv_grads, gate_pre, up_pre, w_gate, w_up, w_down))
    returned = jnp.transpose(back_rows.reshape(N_SP, N_SP, CAP, D), (1, 0, 2, 3))
    picked = jax.vmap(pick_rows)(returned, targets, ranked)
    moe_terms = picked.astype(jnp.float32).reshape(SEQUENCE_TOKENS, TOPK, D).sum(axis=1)
    grad_hidden = (layer_cotangent.astype(jnp.float32) + moe_terms).astype(jnp.bfloat16)

    def blocks_of(array):
        return array.reshape((N_SP, TOK_DEV) + array.shape[1:])
    initial = (jnp.zeros((MIXER_HEADS, HEAD_DIM, STATE), jnp.float32), jnp.zeros((MIXER_HEADS,), jnp.float32))
    stepper = partial(block_step, w_out=w_out, norm_gain=norm_gain)
    block_inputs = (blocks_of(scan_in), blocks_of(gate_in), blocks_of(b_proj), blocks_of(c_proj), blocks_of(log_decay), entry_state, blocks_of(grad_hidden))
    results = lax.scan(stepper, initial, block_inputs, reverse=True)[1]
    grad_scan, grad_gate, grad_b, grad_c, grad_decay, mixed = [item.reshape((SEQUENCE_TOKENS,) + item.shape[2:]) for item in results]
    grad_out_proj = jnp.dot(grad_hidden.T, mixed, preferred_element_type=jnp.float32)
    return (gate_wgrad, up_wgrad, down_wgrad, grad_out_proj, grad_scan, grad_gate, grad_b, grad_c, grad_decay)
```

```python
import functools

import jax
import jax.numpy as jnp
from jax import lax
from jax.sharding import PartitionSpec as P

from jax.experimental import pallas as pl
from jax.experimental.pallas import tpu as pltpu

HEAD_DIM = 64
STATE = 128


rms_epsilon = 1e-05
clamp_limit = 7.0
swish_alpha = 1.702


MESH = pl.DeviceIdType.MESH
f32, bf16 = jnp.float32, jnp.bfloat16


def dot_nn(a, b):
    return jnp.dot(a, b, preferred_element_type=f32)


def dot_nt(a, b):
    return lax.dot_general(a, b, (((1,), (1,)), ((), ())), preferred_element_type=f32)


def dot_tn(a, b):
    return lax.dot_general(a, b, (((0,), (0,)), ((), ())), preferred_element_type=f32)


def dot_full(a, b):
    return jnp.dot(a, b, precision=lax.Precision.HIGHEST, preferred_element_type=f32)


def xor(value, bits):
    bit = 1
    while bit <= bits:
        if bits & bit:
            value = value + bit * (1 - 2 * ((value // bit) % 2))
        bit *= 2
    return value


def iota(shape, dim):
    return lax.broadcasted_iota(jnp.int32, shape, dim)


def aligned(value, unit):
    return pl.multiple_of(value, unit)


def fused(
    dims,
    choice, choice_t, weight_t, decay, decay_t, gain, scan_x, gate_x, b_in, c_in, entry,
    cot_hbm, hid_hbm, gpre_hbm, upre_hbm, wg_hbm, wu_hbm, wd_hbm, wo_hbm,
    owg, owu, owd, oproj, oscan, ogate, ob, oc, odecay,
    cot, hid, gpre, upre, wg, wu, wd, wo,
    send_g, send_h, g_full, h_full, part_send, part_recv, ret_send, ret_recv,
    active, gate_grad, up_grad, places_t,
    mixed_z, hidden, hidden_z, rs_send, rs_recv,
    scan_out, unit, inv_rms, gy, mix_t, decays, growth_s, tail_s, entry_b, block_state,
    st_send, st_recv, rv_send, rv_recv, tot_send, tot_recv, gat_send, gat_recv,
    grad_wg, grad_wu, grad_wd,
    in_sem, out_sem, g_s, g_r, h_s, h_r, ret_s, ret_r, st_s, st_r, rv_s, rv_r,
    tot_s, tot_r, gat_s, gat_r, fg_s, fg_r, fh_s, fh_r, px_s, px_r, mz_s, mz_r,
    gh_s, gh_r, hz_s, hz_r, fz_s, fz_r, rs_s, rs_r,
):
    n, outer, cap = dims
    inner = n // outer
    tokens, half = cot.shape
    rows = n * cap
    zrows = inner * cap
    heads = decay.shape[1]
    groups = b_in.shape[1] // STATE
    pairs_in_group = heads // groups // 2
    gwidth = pairs_in_group * 128
    per_half = outer // 2
    dchunk = hidden.shape[2]
    srows = st_send.shape[0] // n
    dcols = dchunk // inner
    thalf = tokens // 2
    me = lax.axis_index("sp")
    tp = lax.axis_index("tp")
    other = 1 - tp
    my_z = me // inner
    my_q = me % inner
    peers = [xor(me, k) for k in range(n)]

    def remote(src, dst, s, r, sp_id, tp_id):
        return pltpu.make_async_remote_copy(
            src_ref=src, dst_ref=dst, send_sem=s, recv_sem=r,
            device_id=(sp_id, tp_id), device_id_type=MESH,
        )

    def rowblock(block, size):
        return pl.ds(aligned(block * size, size), size)

    barrier = pltpu.get_barrier_semaphore()
    for k in range(1, n):
        pl.semaphore_signal(barrier, inc=1, device_id=(peers[k], tp), device_id_type=MESH)
    pl.semaphore_signal(barrier, inc=1, device_id=(me, other), device_id_type=MESH)

    own_cols = pl.ds(aligned(tp * half, half), half)
    loads = [
        pltpu.make_async_copy(cot_hbm.at[:, own_cols], cot, in_sem.at[0]),
        pltpu.make_async_copy(hid_hbm.at[:, own_cols], hid, in_sem.at[1]),
        pltpu.make_async_copy(wd_hbm, wd, in_sem.at[2]),
        pltpu.make_async_copy(gpre_hbm, gpre, in_sem.at[3]),
        pltpu.make_async_copy(upre_hbm, upre, in_sem.at[4]),
        pltpu.make_async_copy(wg_hbm, wg, in_sem.at[5]),
        pltpu.make_async_copy(wu_hbm, wu, in_sem.at[6]),
        pltpu.make_async_copy(wo_hbm, wo, in_sem.at[7]),
    ]
    for load in loads:
        load.start()

    expert_s = iota((n, tokens), 0)
    first_t = choice_t[0:1, :] == expert_s
    second_t = choice_t[1:2, :] == expert_s
    row_id = iota((tokens, tokens), 0)
    col_id = iota((tokens, tokens), 1)
    named_t = jnp.where(first_t | second_t, 1.0, 0.0).astype(bf16)
    before_t = jnp.where(row_id < col_id, 1.0, 0.0).astype(bf16)
    base_t = dot_nn(named_t, before_t) + (cap * expert_s).astype(f32)
    slot0_t = jnp.sum(jnp.where(first_t, base_t, 0.0), axis=0, keepdims=True)
    slot1_t = jnp.sum(jnp.where(second_t, base_t, 0.0), axis=0, keepdims=True)

    expert_l = iota((tokens, n), 1)
    first = choice[:, 0:1] == expert_l
    second = choice[:, 1:2] == expert_l
    named = jnp.where(first | second, 1.0, 0.0).astype(bf16)
    before = jnp.where(row_id > col_id, 1.0, 0.0).astype(bf16)
    base = dot_nn(before, named) + (cap * expert_l).astype(f32)
    slot0 = jnp.sum(jnp.where(first, base, 0.0), axis=1, keepdims=True)
    slot1 = jnp.sum(jnp.where(second, base, 0.0), axis=1, keepdims=True)
    slot_l = iota((tokens, rows), 1).astype(f32)
    places_t[...] = jnp.where((slot_l == slot0) | (slot_l == slot1), 1.0, 0.0).astype(bf16)

    loads[0].wait()
    loads[1].wait()
    for z in range(outer):
        part = slice(z * zrows, (z + 1) * zrows)
        slot_s = (iota((zrows, tokens), 0) + z * zrows).astype(f32)
        in_first = slot_s == slot0_t
        in_second = slot_s == slot1_t
        places = jnp.where(in_first | in_second, 1.0, 0.0).astype(bf16)
        scale = jnp.sum(
            jnp.where(in_first, weight_t[0:1, :], 0.0) + jnp.where(in_second, weight_t[1:2, :], 0.0),
            axis=1, keepdims=True,
        )
        send_g[part, :] = (dot_nn(places, cot[...]) * scale).astype(bf16)
        send_h[part, :] = dot_nn(places, hid[...]).astype(bf16)

    pl.semaphore_wait(barrier, n)

    def all_to_all(send, recv, size, s, r):
        mine = rowblock(me, size)
        return [None] + [
            remote(send.at[rowblock(peers[k], size)], recv.at[mine], s.at[k], r.at[k], peers[k], tp)
            for k in range(1, n)
        ]

    own_rows = rowblock(me, cap)
    copy_g = all_to_all(send_g, g_full.at[tp], cap, g_s, g_r)
    copy_h = all_to_all(send_h, h_full.at[tp], cap, h_s, h_r)
    copy_ret = all_to_all(ret_send, ret_recv, cap, ret_s, ret_r)
    copy_st = all_to_all(st_send, st_recv, srows, st_s, st_r)
    copy_rv = all_to_all(rv_send, rv_recv, srows, rv_s, rv_r)
    far_first = list(range(n - 1, 0, -1))
    for k in far_first:
        copy_g[k].start()
    g_full[tp, own_rows, :] = send_g[own_rows, :]
    h_full[tp, own_rows, :] = send_h[own_rows, :]

    causal = row_id >= col_id
    causal_f = jnp.where(causal, 1.0, 0.0)
    anti_f = jnp.where(row_id <= col_id, 1.0, 0.0)
    cum = dot_full(causal_f, decay[...])
    cum_t = dot_full(decay_t[...], anti_f)
    growth_s[...] = jnp.exp(cum)
    tail_s[...] = jnp.exp(cum[tokens - 1:tokens, :] - cum)
    tot_send[...] = jnp.zeros(tot_send.shape, f32)
    tot_send[0:1, 0:heads] = cum[tokens - 1:tokens, :]
    tot_recv[me] = tot_send[...]
    copy_tot = [None] + [
        remote(tot_send, tot_recv.at[me], tot_s.at[k], tot_r.at[k], peers[k], tp)
        for k in range(1, n)
    ]
    for k in far_first:
        copy_tot[k].start()
    lane = iota((1, 128), 1)
    low_lane = lane < HEAD_DIM
    low = jnp.where(low_lane, 1.0, 0.0)
    low_b, high_b = low.astype(bf16), (1.0 - low).astype(bf16)

    def spread(columns, pair):
        return jnp.where(
            low_lane, columns[:, 2 * pair:2 * pair + 1], columns[:, 2 * pair + 1:2 * pair + 2]
        )

    def tile(index):
        return slice(index * 128, (index + 1) * 128)

    def group_cols(g):
        return slice(g * gwidth, (g + 1) * gwidth)

    entry_b[...] = entry[...].astype(bf16)
    for g in range(groups):
        b_g, c_g = b_in[:, tile(g)], c_in[:, tile(g)]
        inner_prod = dot_nt(c_g, b_g)
        inner_t = dot_nt(b_g, c_g)
        squares = jnp.zeros((tokens, 1), f32)
        gated = []
        for pair in range(g * pairs_in_group, (g + 1) * pairs_in_group):
            mats = []
            for h in (2 * pair, 2 * pair + 1):
                gap = cum[:, h:h + 1] - cum_t[h:h + 1, :]
                fade = jnp.exp(jnp.where(causal, gap, -jnp.inf))
                decays[h] = fade
                mats.append((inner_prod * fade).astype(bf16))
                gap_t = cum_t[h:h + 1, :] - cum[:, h:h + 1]
                mix_t[pair, :, tile(h % 2)] = (
                    inner_t * jnp.exp(jnp.where(row_id <= col_id, gap_t, -jnp.inf))
                ).astype(bf16)
            x = scan_x[:, tile(pair)]
            y = dot_nn(mats[0], x * low_b) + dot_nn(mats[1], x * high_b)
            carry = dot_nt(c_g, entry_b[tile(pair), :])
            out = y + carry * spread(growth_s, pair)
            scan_out[:, tile(pair)] = out
            gate = gate_x[:, tile(pair)].astype(f32)
            value = out * (gate * jax.nn.sigmoid(gate))
            squares = squares + jnp.sum(value * value, axis=1, keepdims=True)
            gated.append(value)
        inv = lax.rsqrt(squares * (1.0 / gwidth) + rms_epsilon)
        inv_rms[g] = inv
        for i, value in enumerate(gated):
            cols = tile(g * pairs_in_group + i)
            flat = value * inv
            unit[:, cols] = flat
            mixed_z[my_z, :, cols] = (flat * gain[:, cols].astype(f32)).astype(bf16)

    copy_mz = [None] + [
        remote(
            mixed_z.at[my_z], mixed_z.at[my_z], mz_s.at[j], mz_r.at[j],
            xor(my_z, j) * inner + my_q, tp,
        )
        for j in range(1, outer)
    ]

    for i in range(2, 7):
        loads[i].wait()
    fwd_g, fwd_h, px = [], [], []
    for j in range(outer):
        zpart = rowblock(xor(my_z, j), zrows)
        fwd_g.append(
            remote(g_full.at[tp, zpart], g_full.at[tp, zpart], fg_s.at[j], fg_r.at[j], me, other)
        )
        fwd_h.append(
            remote(h_full.at[tp, zpart], h_full.at[tp, zpart], fh_s.at[j], fh_r.at[j], me, other)
        )
        px.append(remote(part_send.at[j], part_recv.at[j], px_s.at[j], px_r.at[j], me, other))
    for j in range(outer):
        for k in range(j * inner, (j + 1) * inner):
            if k:
                copy_g[k].wait_recv()
        fwd_g[j].start()
        fwd_g[j].wait_recv()
        zpart = rowblock(xor(my_z, j), zrows)
        act = dot_nt(g_full[0, zpart, :], wd[:, 0:half])
        act = act + dot_nt(g_full[1, zpart, :], wd[:, half:2 * half])
        gate_full = gpre[zpart, :].astype(f32)
        up_full = upre[zpart, :].astype(f32)
        gate_clip = jnp.minimum(gate_full, clamp_limit)
        up_clip = jnp.clip(up_full, -clamp_limit, clamp_limit)
        sig = jax.nn.sigmoid(swish_alpha * gate_clip)
        swish = gate_clip * sig
        active[zpart, :] = ((up_clip + 1.0) * swish).astype(bf16)
        inside = (up_full > -clamp_limit) & (up_full < clamp_limit)
        ug = jnp.where(inside, act * swish, 0.0).astype(bf16)
        slope = sig + swish_alpha * gate_clip * sig * (1.0 - sig)
        gg = jnp.where(gate_full < clamp_limit, act * (up_clip + 1.0) * slope, 0.0).astype(bf16)
        up_grad[zpart, :] = ug
        gate_grad[zpart, :] = gg
        part_send[j] = (dot_nt(gg, wg[other]) + dot_nt(ug, wu[other])).astype(bf16)
        px[j].start()
        own = (dot_nt(gg, wg[tp]) + dot_nt(ug, wu[tp])).astype(bf16)
        px[j].wait_recv()
        ret_send[zpart, :] = (own.astype(f32) + part_recv[j].astype(f32)).astype(bf16)
        if j == 0:
            ret_recv[own_rows, :] = ret_send[own_rows, :]
        for k in range(j * inner, (j + 1) * inner):
            if k:
                copy_ret[k].start()

    for k in far_first:
        copy_h[k].start()

    def down_step(i, carry):
        cols = pl.ds(aligned(i * 256, 256), 256)
        for s in range(2):
            grad_wd[s, :, cols] = dot_tn(active[...], g_full[s, :, cols]).astype(bf16)
        return carry

    lax.fori_loop(0, half // 256, down_step, 0)
    stores = [
        pltpu.make_async_copy(grad_wd.at[0], owd.at[:, 0:half], out_sem.at[0]),
        pltpu.make_async_copy(grad_wd.at[1], owd.at[:, half:2 * half], out_sem.at[1]),
    ]
    stores[0].start()
    stores[1].start()

    for k in range(1, n):
        copy_ret[k].wait_recv()
    moe = dot_nn(places_t[...], ret_recv[...])
    for i in range(per_half):
        cols = slice(i * dchunk, (i + 1) * dchunk)
        hidden[tp * per_half + i] = (cot[:, cols].astype(f32) + moe[:, cols]).astype(bf16)
    own_chunks = pl.ds(tp * per_half, per_half)
    copy_gh = remote(hidden.at[own_chunks], hidden.at[own_chunks], gh_s, gh_r, me, other)
    copy_gh.start()
    loads[7].wait()
    copy_gh.wait_recv()
    hidden_z[my_z] = hidden[my_z]
    my_tokens = pl.ds(aligned(tp * thalf, thalf), thalf)
    copy_hz, fwd_z = [None], [None]
    for j in range(1, outer):
        z = xor(my_z, j)
        copy_hz.append(
            remote(
                hidden.at[z, my_tokens], hidden_z.at[my_z, my_tokens],
                hz_s.at[j], hz_r.at[j], z * inner + my_q, tp,
            )
        )
        fwd_z.append(
            remote(
                hidden_z.at[z, my_tokens], hidden_z.at[z, my_tokens],
                fz_s.at[j], fz_r.at[j], me, other,
            )
        )
    for j in range(outer - 1, 0, -1):
        copy_hz[j].start()

    for g in range(groups):
        c_g = c_in[:, tile(g)]
        gcols = group_cols(g)
        gm = dot_nt(hidden[0], wo[gcols, 0:dchunk])
        for i in range(1, outer):
            gm = gm + dot_nt(hidden[i], wo[gcols, i * dchunk:(i + 1) * dchunk])
        gu = gm * gain[:, gcols].astype(f32)
        flat = unit[:, gcols]
        mean = jnp.sum(gu * flat, axis=1, keepdims=True) * (1.0 / gwidth)
        gg = inv_rms[g] * (gu - flat * mean)
        gate = gate_x[:, gcols].astype(f32)
        sig = jax.nn.sigmoid(gate)
        ogate[:, gcols] = (
            gg * scan_out[:, gcols] * sig * (1.0 + gate * (1.0 - sig))
        ).astype(bf16)
        grad_y = gg * (gate * sig)
        gy[:, gcols] = grad_y
        for i in range(pairs_in_group):
            pair = g * pairs_in_group + i
            grown = (grad_y[:, tile(i)] * spread(growth_s, pair)).astype(bf16)
            st_send[tile(pair), :] = dot_tn(grown, c_g).astype(bf16)
    own_st = rowblock(me, srows)
    for k in far_first:
        copy_st[k].start()
    st_recv[own_st, :] = st_send[own_st, :]
    for j in range(outer - 1, 0, -1):
        copy_mz[j].start()

    for g in range(groups):
        b_g, c_g = b_in[:, tile(g)], c_in[:, tile(g)]
        gw = jnp.zeros((tokens, tokens), f32)
        gc = jnp.zeros((tokens, STATE), f32)
        for i in range(pairs_in_group):
            pair = g * pairs_in_group + i
            gy_t = gy[:, tile(pair)]
            gyb = gy_t.astype(bf16)
            x = scan_x[:, tile(pair)]
            gw = gw + dot_nt(gyb * low_b, x) * decays[2 * pair]
            gw = gw + dot_nt(gyb * high_b, x) * decays[2 * pair + 1]
            grown = (gy_t * spread(growth_s, pair)).astype(bf16)
            gc = gc + dot_nn(grown, entry_b[tile(pair), :])
        gwb = gw.astype(bf16)
        oc[:, tile(g)] = (gc + dot_nn(gwb, b_g)).astype(bf16)
        block_state[g] = dot_tn(gwb, c_g)

    for k in range(1, n):
        copy_tot[k].wait_recv()
        copy_st[k].wait_recv()
    my_head = (me * srows) // HEAD_DIM
    rev = jnp.zeros((srows, STATE), f32)
    for b in range(n - 1, -1, -1):
        part = slice(b * srows, (b + 1) * srows)
        rv_send[part, :] = rev.astype(bf16)
        if b:
            total = jnp.sum(
                jnp.where(lane == my_head, tot_recv[b, 0:1, :], 0.0), axis=1, keepdims=True
            )
            rev = st_recv[part, :].astype(f32) + jnp.exp(total) * rev
    for k in far_first:
        copy_rv[k].start()
    rv_recv[own_st, :] = rv_send[own_st, :]

    for j in range(1, outer):
        copy_hz[j].wait_recv()
        fwd_z[j].start()
    for j in range(1, outer):
        fwd_z[j].wait_recv()
        copy_mz[j].wait_recv()
    copy_rs = [None]
    for q in range(inner - 1, -1, -1):
        target = xor(my_q, q)
        dpart = pl.ds(aligned(target * dcols, dcols), dcols)
        for s in range(half // 512):
            cols = slice(s * 512, (s + 1) * 512)
            total = dot_tn(hidden_z[0, :, dpart], mixed_z[0, :, cols])
            for z in range(1, outer):
                total = total + dot_tn(hidden_z[z, :, dpart], mixed_z[z, :, cols])
            if q:
                rs_send[q, :, cols] = total.astype(bf16)
            else:
                oproj[:, cols] = total
        if q:
            copy = remote(
                rs_send.at[q], rs_recv.at[q], rs_s.at[q], rs_r.at[q], my_z * inner + target, tp
            )
            copy.start()
            copy_rs.append(copy)

    for k in range(1, n):
        copy_rv[k].wait_recv()
    head_l = iota((1, heads), 1)
    grad_a = jnp.zeros((tokens, heads), f32)
    for g in range(groups):
        b_g = b_in[:, tile(g)]
        gb = block_state[g]
        for i in range(pairs_in_group):
            pair = g * pairs_in_group + i
            gy_t = gy[:, tile(pair)]
            gyb = gy_t.astype(bf16)
            x = scan_x[:, tile(pair)]
            xf = x.astype(f32)
            tail = spread(tail_s, pair)
            later = rv_recv[tile(pair), :]
            gx = dot_nn(mix_t[pair, :, 0:tokens], gyb * low_b)
            gx = gx + dot_nn(mix_t[pair, :, tokens:2 * tokens], gyb * high_b)
            gx = gx + dot_nt(b_g, later) * tail
            oscan[:, tile(pair)] = gx.astype(bf16)
            gb = gb + dot_nn((xf * tail).astype(bf16), later)
            diff = gy_t * scan_out[:, tile(pair)] - xf * gx
            sum_low = jnp.sum(jnp.where(low_lane, diff, 0.0), axis=1, keepdims=True)
            sum_high = jnp.sum(jnp.where(low_lane, 0.0, diff), axis=1, keepdims=True)
            grad_a = jnp.where(head_l == 2 * pair, sum_low, grad_a)
            grad_a = jnp.where(head_l == 2 * pair + 1, sum_high, grad_a)
        ob[:, tile(g)] = gb.astype(bf16)
    gat_send[...] = jnp.zeros(gat_send.shape, f32)
    gat_send[0:1, 0:heads] = jnp.sum(grad_a, axis=0, keepdims=True)
    copy_gat = [None] + [
        remote(gat_send, gat_recv.at[me], gat_s.at[k], gat_r.at[k], peers[k], tp)
        for k in range(1, n)
    ]
    for k in far_first:
        copy_gat[k].start()
    gat_recv[me] = gat_send[...]

    for j in range(outer):
        for k in range(j * inner, (j + 1) * inner):
            if k:
                copy_h[k].wait_recv()
        fwd_h[j].start()
    for j in range(outer):
        fwd_h[j].wait_recv()

    def up_step(i, carry):
        cols = pl.ds(aligned(i * 256, 256), 256)
        for s in range(2):
            lhs = h_full[s, :, cols]
            grad_wg[s, cols, :] = dot_tn(lhs, gate_grad[...]).astype(bf16)
            grad_wu[s, cols, :] = dot_tn(lhs, up_grad[...]).astype(bf16)
        return carry

    lax.fori_loop(0, half // 256, up_step, 0)
    for i, (src, dst) in enumerate(((grad_wg, owg), (grad_wu, owu))):
        stores.append(pltpu.make_async_copy(src, dst, out_sem.at[2 + i]))
        stores[-1].start()

    later_sum = dot_full(anti_f, grad_a)
    for k in range(1, n):
        copy_gat[k].wait_recv()
    for b in range(n):
        later_sum = later_sum + jnp.where(b > me, gat_recv[b, 0:1, 0:heads], 0.0)
    odecay[...] = later_sum

    for copy in copy_rs[1:]:
        copy.wait_recv()
    for q in range(1, inner):
        oproj[...] += rs_recv[q].astype(f32)
    for copies in (
        copy_g, copy_h, copy_ret, copy_st, copy_rv, copy_tot, copy_gat, copy_mz, copy_hz, fwd_z,
        copy_rs, fwd_g, fwd_h, px, [copy_gh],
    ):
        for copy in copies:
            if copy is not None:
                copy.wait_send()
    for store in stores:
        store.wait()


def fused_body(
    mixer_output, layer_cotangent, expert_choice, route_weight, gate_pre, up_pre,
    w_gate, w_up, w_down, w_out, norm_gain, scan_in, gate_in, b_proj, c_proj,
    log_decay, entry_state,
):
    n = lax.axis_size("sp")
    outer = 4
    inner = n // outer
    tokens, width = mixer_output.shape
    half = width // 2
    rows, units = gate_pre.shape[1:]
    cap = rows // n
    heads = log_decay.shape[1]
    channels = scan_in.shape[1]
    state_rows = heads * HEAD_DIM
    srows = state_rows // n
    groups = b_proj.shape[1] // STATE
    pairs = heads // 2
    dchunk = width // outer
    dcols = width // n
    vm = pltpu.VMEM
    dma = pltpu.SemaphoreType.DMA
    wide = jax.ShapeDtypeStruct
    vspec = pl.BlockSpec(memory_space=pltpu.VMEM)
    aspec = pl.BlockSpec(memory_space=pl.ANY)
    scratch = [
        vm((tokens, half), bf16), vm((tokens, half), bf16),
        vm((rows, units), bf16), vm((rows, units), bf16),
        vm((2, half, units), bf16), vm((2, half, units), bf16),
        vm((units, width), bf16), vm((channels, width), bf16),
        vm((rows, half), bf16), vm((rows, half), bf16),
        vm((2, rows, half), bf16), vm((2, rows, half), bf16),
        vm((outer, rows // outer, half), bf16), vm((outer, rows // outer, half), bf16),
        vm((rows, half), bf16), vm((rows, half), bf16),
        vm((rows, units), bf16), vm((rows, units), bf16), vm((rows, units), bf16),
        vm((tokens, rows), bf16),
        vm((outer, tokens, channels), bf16), vm((outer, tokens, dchunk), bf16),
        vm((outer, tokens, dchunk), bf16),
        vm((inner, dcols, channels), bf16), vm((inner, dcols, channels), bf16),
        vm((tokens, channels), f32), vm((tokens, channels), f32), vm((groups, tokens, 1), f32),
        vm((tokens, channels), f32), vm((pairs, tokens, 2 * tokens), bf16),
        vm((heads, tokens, tokens), f32), vm((tokens, heads), f32), vm((tokens, heads), f32),
        vm((state_rows, STATE), bf16), vm((groups, tokens, STATE), f32),
        vm((state_rows, STATE), bf16), vm((state_rows, STATE), bf16),
        vm((state_rows, STATE), bf16), vm((state_rows, STATE), bf16),
        vm((8, 128), f32), vm((n, 8, 128), f32), vm((8, 128), f32), vm((n, 8, 128), f32),
        vm((2, half, units), bf16), vm((2, half, units), bf16), vm((2, units, half), bf16),
        dma((8,)), dma((4,)),
    ]
    scratch += [dma((n,))] * 14
    scratch += [dma((outer,))] * 8
    scratch += [dma, dma]
    scratch += [dma((outer,))] * 4
    scratch += [dma((inner,))] * 2
    outs = pl.pallas_call(
        functools.partial(fused, (n, outer, cap)),
        out_shape=(
            wide((2, half, units), bf16), wide((2, half, units), bf16), wide((units, width), bf16),
            wide((dcols, channels), f32), wide((tokens, channels), bf16),
            wide((tokens, channels), bf16), wide((tokens, groups * STATE), bf16),
            wide((tokens, groups * STATE), bf16), wide((tokens, heads), f32),
        ),
        in_specs=[vspec] * 11 + [aspec] * 8,
        out_specs=(aspec,) * 3 + (vspec,) * 6,
        scratch_shapes=scratch,
        compiler_params=pltpu.CompilerParams(
            collective_id=0, has_side_effects=True, vmem_limit_bytes=64 * 1024 * 1024 - 128 * 1024
        ),
        name="fused",
    )(
        expert_choice, expert_choice.T, route_weight.T, log_decay, log_decay.T,
        norm_gain[None], scan_in, gate_in, b_proj, c_proj,
        entry_state.reshape(state_rows, STATE),
        layer_cotangent, mixer_output, gate_pre[0], up_pre[0],
        w_gate.reshape(2, half, units), w_up.reshape(2, half, units), w_down[0], w_out,
    )
    gwg, gwu, gwd, proj, gscan, ggate, gb, gc, gdecay = outs
    return (
        gwg.reshape(1, width, units), gwu.reshape(1, width, units), gwd[None],
        proj, gscan, ggate, gb, gc, gdecay,
    )


def entry_slots(expert_choice, expert_count, capacity):
    tokens, top_count = expert_choice.shape
    targets = expert_choice.reshape(-1)
    experts = jnp.arange(expert_count, dtype=jnp.int32)
    one_hot = (targets[:, None] == experts[None, :]).astype(jnp.float32)
    entries = jnp.arange(tokens * top_count, dtype=jnp.int32)
    before = (entries[:, None] > entries[None, :]).astype(jnp.bfloat16)
    earlier = jnp.dot(before, one_hot.astype(jnp.bfloat16), preferred_element_type=jnp.float32)
    ranks = jnp.sum(earlier * one_hot, axis=1).astype(jnp.int32)
    return (targets * capacity + ranks).reshape(tokens, top_count)


def expert_side(grad_rows, gate_value, up_value, gate_weight, up_weight, down_weight):
    act_grad = jnp.einsum("rd,fd->rf", grad_rows, down_weight, preferred_element_type=jnp.float32)
    gate_full = gate_value.astype(jnp.float32)
    up_full = up_value.astype(jnp.float32)
    gate_clip = jnp.minimum(gate_full, clamp_limit)
    up_clip = jnp.clip(up_full, -clamp_limit, clamp_limit)
    sigmoid_gate = jax.nn.sigmoid(swish_alpha * gate_clip)
    swish_gate = gate_clip * sigmoid_gate
    active = ((up_clip + 1.0) * swish_gate).astype(jnp.bfloat16)
    up_grad = jnp.where(
        (up_full > -clamp_limit) & (up_full < clamp_limit), act_grad * swish_gate, 0.0
    ).astype(jnp.bfloat16)
    slope = sigmoid_gate + swish_alpha * gate_clip * sigmoid_gate * (1.0 - sigmoid_gate)
    gate_grad = jnp.where(gate_full < clamp_limit, act_grad * (up_clip + 1.0) * slope, 0.0).astype(
        jnp.bfloat16
    )
    partial_rows = jnp.einsum(
        "rf,df->rd", gate_grad, gate_weight, preferred_element_type=jnp.float32
    )
    partial_rows = partial_rows + jnp.einsum(
        "rf,df->rd", up_grad, up_weight, preferred_element_type=jnp.float32
    )
    return (active, gate_grad, up_grad, partial_rows)


def exchange(pieces):
    return lax.all_to_all(pieces, "sp", split_axis=0, concat_axis=0, tiled=True)


def tell_all(vector):
    return exchange(jnp.broadcast_to(vector, (lax.axis_size("sp"), *vector.shape)))


def later_states(block_state, totals):
    count = lax.axis_size("sp")
    heads, channels, width = block_state.shape
    rows = heads * channels // count
    spots = jnp.arange(count)
    between = (
        (spots[:, None, None] < spots[None, None, :]) & (spots[None, None, :] < spots[None, :, None])
    ).astype(jnp.float32)
    gaps = jnp.einsum("bck,kh->bch", between, totals, precision=lax.Precision.HIGHEST)
    later = spots[:, None, None] < spots[None, :, None]
    weights = jnp.where(later, jnp.exp(gaps), 0.0)
    first = lax.axis_index("sp") * rows
    picks = (
        ((first + jnp.arange(rows)) // channels)[None, :] == jnp.arange(heads)[:, None]
    ).astype(jnp.float32)
    weights = jnp.einsum("bch,hr->bcr", weights, picks, precision=lax.Precision.HIGHEST)
    dealt = lax.all_to_all(
        block_state.astype(jnp.bfloat16).reshape(count, rows, width),
        "sp",
        split_axis=0,
        concat_axis=0,
        tiled=True,
    ).astype(jnp.float32)
    sums = jnp.sum(weights[:, :, :, None] * dealt[None], axis=1)
    back = lax.all_to_all(
        sums.astype(jnp.bfloat16), "sp", split_axis=0, concat_axis=0, tiled=True
    )
    return back.reshape(heads, channels, width)


def body(
    mixer_output,
    layer_cotangent,
    expert_choice,
    route_weight,
    gate_pre,
    up_pre,
    w_gate,
    w_up,
    w_down,
    w_out,
    norm_gain,
    scan_in,
    gate_in,
    b_proj,
    c_proj,
    log_decay,
    entry_state,
):
    expert_count = lax.axis_size("sp")
    tokens_here = mixer_output.shape[0]
    model_width = mixer_output.shape[1]
    top_count = expert_choice.shape[1]
    capacity = gate_pre.shape[1] // expert_count
    columns = model_width // lax.axis_size("tp")
    first_column = lax.axis_index("tp") * columns
    own_cotangent = lax.dynamic_slice_in_dim(layer_cotangent, first_column, columns, 1).astype(
        jnp.float32
    )
    own_hidden = lax.dynamic_slice_in_dim(mixer_output, first_column, columns, 1)
    slots = entry_slots(expert_choice, expert_count, capacity)
    slot_ids = jnp.arange(expert_count * capacity, dtype=jnp.int32)
    places = (slots.T[:, None, :] == slot_ids[None, :, None]).astype(jnp.bfloat16)
    token_places = places.sum(axis=0)
    weighted = (route_weight.T[:, :, None] * own_cotangent[None]).astype(jnp.bfloat16)

    def dispatch(rows):
        arrived = lax.all_to_all(
            rows.astype(jnp.bfloat16).reshape(expert_count, capacity, columns),
            "sp",
            split_axis=0,
            concat_axis=0,
            tiled=True,
        ).reshape(-1, columns)
        return lax.all_gather(arrived, "tp", axis=1, tiled=True)

    recv_grads = dispatch(
        jnp.einsum("kst,ktd->sd", places, weighted, preferred_element_type=jnp.float32)
    )
    active, gate_grad, up_grad, partial_rows = expert_side(
        recv_grads,
        gate_pre[0],
        up_pre[0],
        w_gate[0],
        w_up[0],
        w_down[0],
    )
    summed = lax.psum_scatter(
        partial_rows.astype(jnp.bfloat16), "tp", scatter_dimension=1, tiled=True
    )
    returned = lax.all_to_all(
        summed.reshape(expert_count, capacity, -1), "sp", split_axis=0, concat_axis=0, tiled=True
    )
    head_count = log_decay.shape[1]
    group_count = b_proj.shape[1] // STATE
    per_group = head_count // group_count
    scan_heads = scan_in.reshape(tokens_here, head_count, HEAD_DIM)
    b_groups = b_proj.reshape(tokens_here, group_count, STATE)
    c_groups = c_proj.reshape(tokens_here, group_count, STATE)
    x_float = scan_heads.astype(jnp.float32)
    token_locations = jnp.arange(tokens_here)
    causal = token_locations[:, None] >= token_locations[None, :]
    causal_float = causal.astype(jnp.float32)
    cumulative = jnp.dot(causal_float, log_decay, precision=lax.Precision.HIGHEST)
    growth = jnp.exp(cumulative)
    block_decays = tell_all(lax.optimization_barrier((cumulative[-1], summed))[0])
    tail_decay = jnp.exp(cumulative[-1][None, :] - cumulative)
    log_gaps = cumulative.T[:, :, None] - cumulative.T[:, None, :]
    decay_mat = jnp.exp(jnp.where(causal[None], log_gaps, -jnp.inf))
    inner_prod = jnp.einsum("tgn,sgn->gts", c_groups, b_groups, preferred_element_type=jnp.float32)
    mix_weights = (jnp.repeat(inner_prod, per_group, axis=0) * decay_mat).astype(jnp.bfloat16)
    state_groups = entry_state.astype(jnp.bfloat16).reshape(group_count, per_group, HEAD_DIM, STATE)
    y_inner = jnp.einsum(
        "hts,shp->thp", mix_weights, scan_heads, preferred_element_type=jnp.float32
    )
    y_carry = jnp.einsum(
        "tgn,grpn->tgrp", c_groups, state_groups, preferred_element_type=jnp.float32
    ).reshape(tokens_here, head_count, HEAD_DIM)
    scan_out = y_inner + y_carry * growth[:, :, None]
    gate_float = gate_in.astype(jnp.float32)
    gate_sig = jax.nn.sigmoid(gate_float)
    gate_silu = gate_float * gate_sig
    gated = scan_out.reshape(tokens_here, -1) * gate_silu
    grouped = gated.reshape(tokens_here, group_count, -1)
    inv_rms = lax.rsqrt(jnp.mean(grouped * grouped, axis=-1, keepdims=True) + rms_epsilon)
    unit = grouped * inv_rms
    gain_groups = norm_gain.astype(jnp.float32).reshape(group_count, -1)
    mixed = (unit * gain_groups).reshape(tokens_here, -1).astype(jnp.bfloat16)
    all_mixed = lax.all_gather(mixed, "sp", axis=0, tiled=True)
    returned, mixed = lax.optimization_barrier((returned, mixed))
    moe_terms = jnp.einsum(
        "st,sd->td",
        token_places,
        returned.reshape(-1, columns),
        preferred_element_type=jnp.float32,
    )
    grad_hidden = lax.all_gather(
        (own_cotangent + moe_terms).astype(jnp.bfloat16), "tp", axis=1, tiled=True
    )
    late_hidden, grad_hidden = lax.optimization_barrier((own_hidden, grad_hidden))
    recv_hidden = dispatch(
        jnp.einsum("st,td->sd", token_places, late_hidden, preferred_element_type=jnp.float32)
    )
    down_wgrad = jnp.einsum(
        "rf,rd->fd", active, recv_grads, preferred_element_type=jnp.float32
    ).astype(jnp.bfloat16)
    gate_wgrad = jnp.einsum(
        "rd,rf->df", recv_hidden, gate_grad, preferred_element_type=jnp.float32
    ).astype(jnp.bfloat16)
    up_wgrad = jnp.einsum(
        "rd,rf->df", recv_hidden, up_grad, preferred_element_type=jnp.float32
    ).astype(jnp.bfloat16)
    own_block = lax.all_to_all(
        grad_hidden.reshape(tokens_here, expert_count, -1).transpose(1, 0, 2),
        "sp",
        split_axis=0,
        concat_axis=0,
        tiled=True,
    )
    grad_out_proj = jnp.einsum(
        "td,ti->di",
        own_block.reshape(-1, own_block.shape[2]),
        all_mixed,
        preferred_element_type=jnp.float32,
    )
    grad_mixed = jnp.einsum("td,id->ti", grad_hidden, w_out, preferred_element_type=jnp.float32)
    grad_unit = grad_mixed.reshape(tokens_here, group_count, -1) * gain_groups
    grad_grouped = inv_rms * (grad_unit - unit * jnp.mean(grad_unit * unit, axis=-1, keepdims=True))
    grad_gated = grad_grouped.reshape(tokens_here, -1)
    grad_gate_in = (
        grad_gated
        * scan_out.reshape(tokens_here, -1)
        * gate_sig
        * (1.0 + gate_float * (1.0 - gate_sig))
    ).astype(jnp.bfloat16)
    grad_y = (grad_gated * gate_silu).reshape(tokens_here, head_count, HEAD_DIM)
    grad_y_b = grad_y.astype(jnp.bfloat16)
    grad_x_inner = jnp.einsum(
        "hts,thp->shp", mix_weights, grad_y_b, preferred_element_type=jnp.float32
    )
    grad_weights = (
        jnp.einsum("thp,shp->hts", grad_y_b, scan_heads, preferred_element_type=jnp.float32)
        * decay_mat
    )
    grad_weights = (
        grad_weights.reshape(group_count, per_group, tokens_here, tokens_here)
        .sum(axis=1)
        .astype(jnp.bfloat16)
    )
    grad_c_inner = jnp.einsum(
        "gts,sgn->tgn", grad_weights, b_groups, preferred_element_type=jnp.float32
    )
    grad_b_inner = jnp.einsum(
        "gts,tgn->sgn", grad_weights, c_groups, preferred_element_type=jnp.float32
    )
    grown_grads = (grad_y * growth[:, :, None]).astype(jnp.bfloat16).reshape(
        tokens_here, group_count, per_group, HEAD_DIM
    )
    grad_c_carry = jnp.einsum(
        "tgrp,grpn->tgn", grown_grads, state_groups, preferred_element_type=jnp.float32
    )
    block_state = jnp.einsum(
        "tgrp,tgn->grpn", grown_grads, c_groups, preferred_element_type=jnp.float32
    ).reshape(head_count, HEAD_DIM, STATE)
    x_tail = (x_float * tail_decay[:, :, None]).astype(jnp.bfloat16).reshape(
        tokens_here, group_count, per_group, HEAD_DIM
    )
    later_state = later_states(block_state, block_decays)
    later_groups = later_state.reshape(group_count, per_group, HEAD_DIM, STATE)
    grad_x_carry = jnp.einsum(
        "sgn,grpn->sgrp", b_groups, later_groups, preferred_element_type=jnp.float32
    ).reshape(tokens_here, head_count, HEAD_DIM)
    grad_x = grad_x_inner + grad_x_carry * tail_decay[:, :, None]
    grad_b_carry = jnp.einsum(
        "sgrp,grpn->sgn", x_tail, later_groups, preferred_element_type=jnp.float32
    )
    grad_a = jnp.sum(grad_y * scan_out, axis=2) - jnp.sum(x_float * grad_x, axis=2)
    block_totals = tell_all(jnp.sum(grad_a, axis=0))
    is_later = jnp.arange(expert_count) > lax.axis_index("sp")
    later_grad = jnp.sum(jnp.where(is_later[:, None], block_totals, 0.0), axis=0)
    grad_log_decay = (
        jnp.dot(causal_float.T, grad_a, precision=lax.Precision.HIGHEST) + later_grad[None, :]
    )
    grad_scan_in = grad_x.reshape(tokens_here, -1).astype(jnp.bfloat16)
    grad_b_proj = (grad_b_inner + grad_b_carry).reshape(tokens_here, -1).astype(jnp.bfloat16)
    grad_c_proj = (grad_c_inner + grad_c_carry).reshape(tokens_here, -1).astype(jnp.bfloat16)
    return (
        gate_wgrad[None],
        up_wgrad[None],
        down_wgrad[None],
        grad_out_proj,
        grad_scan_in,
        grad_gate_in,
        grad_b_proj,
        grad_c_proj,
        grad_log_decay,
    )


def solution(mesh):
    in_specs = (
        P("sp", None),
        P("sp", None),
        P("sp", None),
        P("sp", None),
        P("sp", None, "tp"),
        P("sp", None, "tp"),
        P("sp", None, "tp"),
        P("sp", None, "tp"),
        P("sp", "tp", None),
        P("tp", None),
        P("tp"),
        P("sp", "tp"),
        P("sp", "tp"),
        P("sp", "tp"),
        P("sp", "tp"),
        P("sp", "tp"),
        P("sp", "tp", None, None),
    )
    out_specs = (
        P("sp", None, "tp"),
        P("sp", None, "tp"),
        P("sp", "tp", None),
        P("sp", "tp"),
        P("sp", "tp"),
        P("sp", "tp"),
        P("sp", "tp"),
        P("sp", "tp"),
        P("sp", "tp"),
    )
    def run(*args):
        count = mesh.shape["sp"]
        capacity = args[4].shape[1] // count
        simple = mesh.shape["tp"] != 2 or count % 4 or count & (count - 1) or capacity % 16
        return (body if simple else fused_body)(*args)

    return jax.shard_map(run, mesh=mesh, in_specs=in_specs, out_specs=out_specs, check_vma=False)
```

```python
import functools

import jax
import jax.numpy as jnp
from jax import lax
from jax.sharding import PartitionSpec as P

from jax.experimental import pallas as pl
from jax.experimental.pallas import tpu as pltpu

HEAD_DIM = 64
STATE = 128


rms_epsilon = 1e-05
clamp_limit = 7.0
swish_alpha = 1.702


MESH = pl.DeviceIdType.MESH
f32, bf16 = jnp.float32, jnp.bfloat16


def dot_nn(a, b):
    return jnp.dot(a, b, preferred_element_type=f32)


def dot_nt(a, b):
    return lax.dot_general(a, b, (((1,), (1,)), ((), ())), preferred_element_type=f32)


def dot_tn(a, b):
    return lax.dot_general(a, b, (((0,), (0,)), ((), ())), preferred_element_type=f32)


def dot_full(a, b):
    return jnp.dot(a, b, precision=lax.Precision.HIGHEST, preferred_element_type=f32)


def xor(value, bits):
    bit = 1
    while bit <= bits:
        if bits & bit:
            value = value + bit * (1 - 2 * ((value // bit) % 2))
        bit *= 2
    return value


def iota(shape, dim):
    return lax.broadcasted_iota(jnp.int32, shape, dim)


def aligned(value, unit):
    return pl.multiple_of(value, unit)


ORDER = (0, 2, 3, 1)
PLAN = {'sent': (), 'forward': (), ('chunk', 0): (), ('chunk', 1): (), ('chunk', 2): (), ('chunk', 3): (), 'experts': ('hid0', 'mz0'), 'down': ('hid1', 'mz1'), 'combined': (), 'states': ('hid2', 'mz2'), 'inner': ('hid3', 'mz3'), 'later': ('proj',)}


def fused(
    dims,
    choice_t, weight_t, decay_t, gain, scan_x, gate_x, b_in, c_in, entry,
    cot_hbm, hid_hbm, gpre_hbm, upre_hbm, wg_hbm, wu_hbm, wd_hbm, wo_hbm,
    owg, owu, owd, oproj, oscan, ogate, ob, oc, odecay,
    cot, hid_z, gpre, upre, wg, wu, wd, wo,
    send_g, send_h, g_full, h_full, part_send, part_recv, ret_send, ret_recv,
    active, gate_grad, up_grad, places_t,
    mixed_z, hidden, hidden_z, rs_send, rs_recv,
    scan_out, unit, inv_rms, gy, mix_t, decays, growth_s, tail_s, entry_b, block_state,
    st_send, st_recv, rv_send, rv_recv, tot_send, tot_recv, slot_recv, gat_send, gat_recv,
    grad_wg, grad_wu, grad_wd,
    in_sem, out_sem, g_s, g_r, ret_s, ret_r, st_s, st_r, rv_s, rv_r,
    tot_s, tot_r, gat_s, gat_r, fg_s, fg_r, fh_s, fh_r, px_s, px_r, sl_s, sl_r, mz_line, hid_line, h_s, h_r,
    gh_s, gh_r, hz_s, hz_r, fz_s, fz_r, rs_s, rs_r,
):
    n, outer, cap = dims
    inner = n // outer
    tokens, half = cot.shape
    rows = n * cap
    zrows = inner * cap
    heads = decay_t.shape[0]
    groups = b_in.shape[1] // STATE
    pairs_in_group = heads // groups // 2
    gwidth = pairs_in_group * 128
    per_half = outer // 2
    dchunk = hidden.shape[2]
    srows = st_send.shape[0] // n
    dcols = dchunk // inner
    thalf = tokens // 2
    me = lax.axis_index("sp")
    tp = lax.axis_index("tp")
    other = 1 - tp
    my_z = me // inner
    my_q = me % inner
    peers = [xor(me, k) for k in range(n)]

    def remote(src, dst, s, r, sp_id, tp_id):
        return pltpu.make_async_remote_copy(
            src_ref=src, dst_ref=dst, send_sem=s, recv_sem=r,
            device_id=(sp_id, tp_id), device_id_type=MESH,
        )

    def rowblock(block, size):
        return pl.ds(aligned(block * size, size), size)

    barrier = pltpu.get_barrier_semaphore()
    for k in range(1, n):
        pl.semaphore_signal(barrier, inc=1, device_id=(peers[k], tp), device_id_type=MESH)
    pl.semaphore_signal(barrier, inc=1, device_id=(me, other), device_id_type=MESH)

    own_cols = pl.ds(aligned(tp * half, half), half)
    loads = [
        pltpu.make_async_copy(cot_hbm.at[:, own_cols], cot, in_sem.at[0]),
        pltpu.make_async_copy(hid_hbm.at[:, own_cols], hid_z.at[my_z], in_sem.at[1]),
        pltpu.make_async_copy(wd_hbm, wd, in_sem.at[2]),
        pltpu.make_async_copy(gpre_hbm, gpre, in_sem.at[3]),
        pltpu.make_async_copy(upre_hbm, upre, in_sem.at[4]),
        pltpu.make_async_copy(wg_hbm, wg, in_sem.at[5]),
        pltpu.make_async_copy(wu_hbm, wu, in_sem.at[6]),
        pltpu.make_async_copy(wo_hbm, wo, in_sem.at[7]),
    ]
    for load in loads:
        load.start()

    expert_s = iota((n, tokens), 0)
    first_t = choice_t[0:1, :] == expert_s
    second_t = choice_t[1:2, :] == expert_s
    row_id = iota((tokens, tokens), 0)
    col_id = iota((tokens, tokens), 1)
    named_t = jnp.where(first_t | second_t, 1.0, 0.0).astype(bf16)
    before_t = jnp.where(row_id < col_id, 1.0, 0.0).astype(bf16)
    base_t = dot_nn(named_t, before_t) + (cap * expert_s).astype(f32)
    slot0_t = jnp.sum(jnp.where(first_t, base_t, 0.0), axis=0, keepdims=True)
    slot1_t = jnp.sum(jnp.where(second_t, base_t, 0.0), axis=0, keepdims=True)

    def column(row):
        return jnp.sum(jnp.where(row_id == col_id, row, 0.0), axis=1, keepdims=True)

    slot0, slot1 = column(slot0_t), column(slot1_t)
    slot_l = iota((tokens, rows), 1).astype(f32)
    places_t[...] = jnp.where((slot_l == slot0) | (slot_l == slot1), 1.0, 0.0).astype(bf16)

    slot_recv[my_z] = jnp.zeros(slot_recv.shape[1:], f32)
    slot_recv[my_z, 0:1, :] = slot0_t
    slot_recv[my_z, 1:2, :] = slot1_t
    loads[0].wait()
    for z in range(outer):
        part = slice(z * zrows, (z + 1) * zrows)
        slot_s = (iota((zrows, tokens), 0) + z * zrows).astype(f32)
        in_first = slot_s == slot0_t
        in_second = slot_s == slot1_t
        places = jnp.where(in_first | in_second, 1.0, 0.0).astype(bf16)
        scale = jnp.sum(
            jnp.where(in_first, weight_t[0:1, :], 0.0) + jnp.where(in_second, weight_t[1:2, :], 0.0),
            axis=1, keepdims=True,
        )
        send_g[part, :] = (dot_nn(places, cot[...]) * scale).astype(bf16)

    pl.semaphore_wait(barrier, n)

    def line(buf, sems):
        def up(s):
            block = (my_z - s + outer) % outer
            return remote(
                buf.at[block], buf.at[block], sems.at[0, s], sems.at[1, s], (me + inner) % n, tp
            )

        def down(s):
            block = (my_z + s) % outer
            return remote(
                buf.at[block], buf.at[block], sems.at[2, s], sems.at[3, s],
                (me - inner + n) % n, tp,
            )

        def send(s, drain=False):
            @pl.when((my_z >= s) & (my_z < outer - 1))
            def _():
                up(s).wait_send() if drain else up(s).start()

            @pl.when((my_z + s < outer) & (my_z > 0))
            def _():
                down(s).wait_send() if drain else down(s).start()

        def take(s):
            @pl.when(my_z > s)
            def _():
                up(s).wait_recv()

            @pl.when(my_z + s + 1 < outer)
            def _():
                down(s).wait_recv()

        return send, take

    send_hid, take_hid = line(hid_z, hid_line)
    send_mz, take_mz = line(mixed_z, mz_line)

    def at(point):
        for step in PLAN[point]:
            steps[step]()

    def all_to_all(send, recv, size, s, r):
        mine = rowblock(me, size)
        return [None] + [
            remote(send.at[rowblock(peers[k], size)], recv.at[mine], s.at[k], r.at[k], peers[k], tp)
            for k in range(1, n)
        ]

    own_rows = rowblock(me, cap)
    copy_g = all_to_all(send_g, g_full.at[tp], cap, g_s, g_r)
    copy_ret = all_to_all(ret_send, ret_recv, cap, ret_s, ret_r)
    copy_st = all_to_all(st_send, st_recv, srows, st_s, st_r)
    copy_rv = all_to_all(rv_send, rv_recv, srows, rv_s, rv_r)
    far_first = list(range(n - 1, 0, -1))
    for k in far_first:
        copy_g[k].start()
    g_full[tp, own_rows, :] = send_g[own_rows, :]

    copy_rs = [None]

    def output_projection():
        for j in range(1, outer):
            copy_hz[j].wait_recv()
            fwd_z[j].start()
        for j in range(1, outer):
            fwd_z[j].wait_recv()
        for q in range(inner - 1, -1, -1):
            target = xor(my_q, q)
            dpart = pl.ds(aligned(target * dcols, dcols), dcols)
            for s in range(half // 512):
                cols = slice(s * 512, (s + 1) * 512)
                total = dot_tn(hidden_z[0, :, dpart], mixed_z[0, :, cols])
                for z in range(1, outer):
                    total = total + dot_tn(hidden_z[z, :, dpart], mixed_z[z, :, cols])
                if q:
                    rs_send[q, :, cols] = total.astype(bf16)
                else:
                    oproj[:, cols] = total
            if q:
                copy = remote(
                    rs_send.at[q], rs_recv.at[q], rs_s.at[q], rs_r.at[q], my_z * inner + target, tp
                )
                copy.start()
                copy_rs.append(copy)

    copy_h = []

    def hidden_block(b, j):
        slot_h = (iota((zrows, tokens), 0) + my_z * zrows).astype(f32)
        found = (slot_h == slot_recv[b, 0:1, :]) | (slot_h == slot_recv[b, 1:2, :])
        places = jnp.where(found, 1.0, 0.0).astype(bf16)
        send_h[j] = dot_nn(places, hid_z[b]).astype(bf16)
        dest = pl.ds(aligned((b * inner + my_q) * cap, cap), cap)
        for q in range(1, inner):
            target = xor(my_q, q)
            copy = remote(
                send_h.at[j, rowblock(target, cap)], h_full.at[tp, dest],
                h_s.at[j, q], h_r.at[j, q], my_z * inner + target, tp,
            )
            copy.start()
            copy_h.append(copy)
        h_full[tp, dest, :] = send_h[j, rowblock(my_q, cap), :]

    def hidden_own():
        loads[1].wait()
        send_hid(0)
        hidden_block(my_z, 0)

    def hidden_send():
        loads[1].wait()
        send_hid(0)

    def hidden_rest():
        take_hid(outer - 2)
        for j in range(1, outer):
            copy_sl[j].wait_recv()
        for j in range(1, outer):
            hidden_block(xor(my_z, j), j)

    def pass_on(send, take, s):
        take(s - 1)
        send(s)

    steps = {
        "hid0": hidden_own,
        "hid0s": hidden_send,
        "hid0b": lambda: hidden_block(my_z, 0),
        "hid1": lambda: pass_on(send_hid, take_hid, 1),
        "hid2": lambda: pass_on(send_hid, take_hid, 2),
        "hid3": hidden_rest,
        "mz0": lambda: send_mz(0),
        "mz1": lambda: pass_on(send_mz, take_mz, 1),
        "mz2": lambda: pass_on(send_mz, take_mz, 2),
        "mz3": lambda: take_mz(outer - 2),
        "proj": output_projection,
    }

    causal = row_id >= col_id
    causal_f = jnp.where(causal, 1.0, 0.0)
    anti_f = jnp.where(row_id <= col_id, 1.0, 0.0)
    cum_t = dot_full(decay_t[...], anti_f)
    cum = cum_t.T
    growth_s[...] = jnp.exp(cum)
    tail_s[...] = jnp.exp(cum[tokens - 1:tokens, :] - cum)
    tot_send[...] = jnp.zeros(tot_send.shape, f32)
    tot_send[0:1, 0:heads] = cum[tokens - 1:tokens, :]
    tot_recv[me] = tot_send[...]
    copy_tot = [None] + [
        remote(tot_send, tot_recv.at[me], tot_s.at[k], tot_r.at[k], peers[k], tp)
        for k in range(1, n)
    ]
    for k in far_first:
        copy_tot[k].start()
    copy_sl = [None] + [
        remote(
            slot_recv.at[my_z], slot_recv.at[my_z], sl_s.at[j], sl_r.at[j],
            xor(my_z, j) * inner + my_q, tp,
        )
        for j in range(1, outer)
    ]
    for j in range(1, outer):
        copy_sl[j].start()
    at("sent")
    lane = iota((1, 128), 1)
    low_lane = lane < HEAD_DIM
    low = jnp.where(low_lane, 1.0, 0.0)
    low_b, high_b = low.astype(bf16), (1.0 - low).astype(bf16)

    def spread(columns, pair):
        return jnp.where(
            low_lane, columns[:, 2 * pair:2 * pair + 1], columns[:, 2 * pair + 1:2 * pair + 2]
        )

    def tile(index):
        return slice(index * 128, (index + 1) * 128)

    def gain_row(index):
        return gain[index:index + 1, :].astype(f32)

    def group_cols(g):
        return slice(g * gwidth, (g + 1) * gwidth)

    entry_b[...] = entry[...].astype(bf16)
    for g in range(groups):
        b_g, c_g = b_in[:, tile(g)], c_in[:, tile(g)]
        inner_prod = dot_nt(c_g, b_g)
        inner_t = dot_nt(b_g, c_g)
        squares = jnp.zeros((tokens, 1), f32)
        gated = []
        for pair in range(g * pairs_in_group, (g + 1) * pairs_in_group):
            mats = []
            for h in (2 * pair, 2 * pair + 1):
                gap = cum[:, h:h + 1] - cum_t[h:h + 1, :]
                fade = jnp.exp(jnp.where(causal, gap, -jnp.inf))
                decays[h] = fade
                mats.append((inner_prod * fade).astype(bf16))
                gap_t = cum_t[h:h + 1, :] - cum[:, h:h + 1]
                mix_t[pair, :, tile(h % 2)] = (
                    inner_t * jnp.exp(jnp.where(row_id <= col_id, gap_t, -jnp.inf))
                ).astype(bf16)
            x = scan_x[:, tile(pair)]
            y = dot_nn(mats[0], x * low_b) + dot_nn(mats[1], x * high_b)
            carry = dot_nt(c_g, entry_b[tile(pair), :])
            out = y + carry * spread(growth_s, pair)
            scan_out[:, tile(pair)] = out
            gate = gate_x[:, tile(pair)].astype(f32)
            value = out * (gate * jax.nn.sigmoid(gate))
            squares = squares + jnp.sum(value * value, axis=1, keepdims=True)
            gated.append(value)
        inv = lax.rsqrt(squares * (1.0 / gwidth) + rms_epsilon)
        inv_rms[g] = inv
        for i, value in enumerate(gated):
            cols = tile(g * pairs_in_group + i)
            flat = value * inv
            unit[:, cols] = flat
            mixed_z[my_z, :, cols] = (flat * gain_row(g * pairs_in_group + i)).astype(bf16)

    at("forward")

    for i in range(2, 7):
        loads[i].wait()
    fwd_g, fwd_h, px = [], [], []
    for j in range(outer):
        zpart = rowblock(xor(my_z, j), zrows)
        fwd_g.append(
            remote(g_full.at[tp, zpart], g_full.at[tp, zpart], fg_s.at[j], fg_r.at[j], me, other)
        )
        fwd_h.append(
            remote(h_full.at[tp, zpart], h_full.at[tp, zpart], fh_s.at[j], fh_r.at[j], me, other)
        )
        px.append(remote(part_send.at[j], part_recv.at[j], px_s.at[j], px_r.at[j], me, other))
    for count, j in enumerate(ORDER):
        for k in range(j * inner, (j + 1) * inner):
            if k:
                copy_g[k].wait_recv()
        fwd_g[j].start()
        fwd_g[j].wait_recv()
        zpart = rowblock(xor(my_z, j), zrows)
        act = dot_nt(g_full[0, zpart, :], wd[:, 0:half])
        act = act + dot_nt(g_full[1, zpart, :], wd[:, half:2 * half])
        gate_full = gpre[zpart, :].astype(f32)
        up_full = upre[zpart, :].astype(f32)
        gate_clip = jnp.minimum(gate_full, clamp_limit)
        up_clip = jnp.clip(up_full, -clamp_limit, clamp_limit)
        sig = jax.nn.sigmoid(swish_alpha * gate_clip)
        swish = gate_clip * sig
        active[zpart, :] = ((up_clip + 1.0) * swish).astype(bf16)
        inside = (up_full > -clamp_limit) & (up_full < clamp_limit)
        ug = jnp.where(inside, act * swish, 0.0).astype(bf16)
        slope = sig + swish_alpha * gate_clip * sig * (1.0 - sig)
        gg = jnp.where(gate_full < clamp_limit, act * (up_clip + 1.0) * slope, 0.0).astype(bf16)
        up_grad[zpart, :] = ug
        gate_grad[zpart, :] = gg
        part_send[j] = (dot_nt(gg, wg[other]) + dot_nt(ug, wu[other])).astype(bf16)
        px[j].start()
        own = (dot_nt(gg, wg[tp]) + dot_nt(ug, wu[tp])).astype(bf16)
        px[j].wait_recv()
        ret_send[zpart, :] = (own.astype(f32) + part_recv[j].astype(f32)).astype(bf16)
        if j == 0:
            ret_recv[own_rows, :] = ret_send[own_rows, :]
        for k in range(j * inner, (j + 1) * inner):
            if k:
                copy_ret[k].start()
        at(("chunk", count))

    at("experts")

    def down_step(i, carry):
        cols = pl.ds(aligned(i * 256, 256), 256)
        for s in range(2):
            grad_wd[s, :, cols] = dot_tn(active[...], g_full[s, :, cols]).astype(bf16)
        return carry

    lax.fori_loop(0, half // 256, down_step, 0)
    stores = [
        pltpu.make_async_copy(grad_wd.at[0], owd.at[:, 0:half], out_sem.at[0]),
        pltpu.make_async_copy(grad_wd.at[1], owd.at[:, half:2 * half], out_sem.at[1]),
    ]
    stores[0].start()
    stores[1].start()

    at("down")
    for k in range(1, n):
        copy_ret[k].wait_recv()
    moe = dot_nn(places_t[...], ret_recv[...])
    for i in range(per_half):
        cols = slice(i * dchunk, (i + 1) * dchunk)
        hidden[tp * per_half + i] = (cot[:, cols].astype(f32) + moe[:, cols]).astype(bf16)
    own_chunks = pl.ds(tp * per_half, per_half)
    copy_gh = remote(hidden.at[own_chunks], hidden.at[own_chunks], gh_s, gh_r, me, other)
    copy_gh.start()
    loads[7].wait()
    copy_gh.wait_recv()
    hidden_z[my_z] = hidden[my_z]
    my_tokens = pl.ds(aligned(tp * thalf, thalf), thalf)
    copy_hz, fwd_z = [None], [None]
    for j in range(1, outer):
        z = xor(my_z, j)
        copy_hz.append(
            remote(
                hidden.at[z, my_tokens], hidden_z.at[my_z, my_tokens],
                hz_s.at[j], hz_r.at[j], z * inner + my_q, tp,
            )
        )
        fwd_z.append(
            remote(
                hidden_z.at[z, my_tokens], hidden_z.at[z, my_tokens],
                fz_s.at[j], fz_r.at[j], me, other,
            )
        )
    for j in range(outer - 1, 0, -1):
        copy_hz[j].start()
    at("combined")

    for g in range(groups):
        c_g = c_in[:, tile(g)]
        gcols = group_cols(g)
        gm = dot_nt(hidden[0], wo[gcols, 0:dchunk])
        for i in range(1, outer):
            gm = gm + dot_nt(hidden[i], wo[gcols, i * dchunk:(i + 1) * dchunk])
        gu = jnp.concatenate(
            [
                gm[:, tile(i)] * gain_row(g * pairs_in_group + i)
                for i in range(pairs_in_group)
            ],
            axis=1,
        )
        flat = unit[:, gcols]
        mean = jnp.sum(gu * flat, axis=1, keepdims=True) * (1.0 / gwidth)
        gg = inv_rms[g] * (gu - flat * mean)
        gate = gate_x[:, gcols].astype(f32)
        sig = jax.nn.sigmoid(gate)
        ogate[:, gcols] = (
            gg * scan_out[:, gcols] * sig * (1.0 + gate * (1.0 - sig))
        ).astype(bf16)
        grad_y = gg * (gate * sig)
        gy[:, gcols] = grad_y
        for i in range(pairs_in_group):
            pair = g * pairs_in_group + i
            grown = (grad_y[:, tile(i)] * spread(growth_s, pair)).astype(bf16)
            st_send[tile(pair), :] = dot_tn(grown, c_g).astype(bf16)
    own_st = rowblock(me, srows)
    for k in far_first:
        copy_st[k].start()
    st_recv[own_st, :] = st_send[own_st, :]
    at("states")

    for g in range(groups):
        b_g, c_g = b_in[:, tile(g)], c_in[:, tile(g)]
        gw = jnp.zeros((tokens, tokens), f32)
        gc = jnp.zeros((tokens, STATE), f32)
        for i in range(pairs_in_group):
            pair = g * pairs_in_group + i
            gy_t = gy[:, tile(pair)]
            gyb = gy_t.astype(bf16)
            x = scan_x[:, tile(pair)]
            gw = gw + dot_nt(gyb * low_b, x) * decays[2 * pair]
            gw = gw + dot_nt(gyb * high_b, x) * decays[2 * pair + 1]
            grown = (gy_t * spread(growth_s, pair)).astype(bf16)
            gc = gc + dot_nn(grown, entry_b[tile(pair), :])
        gwb = gw.astype(bf16)
        oc[:, tile(g)] = (gc + dot_nn(gwb, b_g)).astype(bf16)
        block_state[g] = dot_tn(gwb, c_g)

    at("inner")

    for k in range(1, n):
        copy_tot[k].wait_recv()
        copy_st[k].wait_recv()
    my_head = (me * srows) // HEAD_DIM
    rev = jnp.zeros((srows, STATE), f32)
    for b in range(n - 1, -1, -1):
        part = slice(b * srows, (b + 1) * srows)
        rv_send[part, :] = rev.astype(bf16)
        if b:
            total = jnp.sum(
                jnp.where(lane == my_head, tot_recv[b, 0:1, :], 0.0), axis=1, keepdims=True
            )
            rev = st_recv[part, :].astype(f32) + jnp.exp(total) * rev
    for k in far_first:
        copy_rv[k].start()
    rv_recv[own_st, :] = rv_send[own_st, :]
    at("later")

    for k in range(1, n):
        copy_rv[k].wait_recv()
    head_l = iota((1, heads), 1)
    grad_a = jnp.zeros((tokens, heads), f32)
    for g in range(groups):
        b_g = b_in[:, tile(g)]
        gb = block_state[g]
        for i in range(pairs_in_group):
            pair = g * pairs_in_group + i
            gy_t = gy[:, tile(pair)]
            gyb = gy_t.astype(bf16)
            x = scan_x[:, tile(pair)]
            xf = x.astype(f32)
            tail = spread(tail_s, pair)
            later = rv_recv[tile(pair), :]
            gx = dot_nn(mix_t[pair, :, 0:tokens], gyb * low_b)
            gx = gx + dot_nn(mix_t[pair, :, tokens:2 * tokens], gyb * high_b)
            gx = gx + dot_nt(b_g, later) * tail
            oscan[:, tile(pair)] = gx.astype(bf16)
            gb = gb + dot_nn((xf * tail).astype(bf16), later)
            diff = gy_t * scan_out[:, tile(pair)] - xf * gx
            sum_low = jnp.sum(jnp.where(low_lane, diff, 0.0), axis=1, keepdims=True)
            sum_high = jnp.sum(jnp.where(low_lane, 0.0, diff), axis=1, keepdims=True)
            grad_a = jnp.where(head_l == 2 * pair, sum_low, grad_a)
            grad_a = jnp.where(head_l == 2 * pair + 1, sum_high, grad_a)
        ob[:, tile(g)] = gb.astype(bf16)
    grad_t = grad_a.T
    gat_send[...] = jnp.broadcast_to(jnp.sum(grad_t, axis=1, keepdims=True), gat_send.shape)
    copy_gat = [None] + [
        remote(gat_send, gat_recv.at[me], gat_s.at[k], gat_r.at[k], peers[k], tp)
        for k in range(1, n)
    ]
    for k in far_first:
        copy_gat[k].start()
    gat_recv[me] = gat_send[...]

    for j in range(outer):
        for copy in copy_h[j * (inner - 1):(j + 1) * (inner - 1)]:
            copy.wait_recv()
        fwd_h[j].start()
    for j in range(outer):
        fwd_h[j].wait_recv()

    def up_step(i, carry):
        cols = pl.ds(aligned(i * 256, 256), 256)
        for s in range(2):
            lhs = h_full[s, :, cols]
            grad_wg[s, cols, :] = dot_tn(lhs, gate_grad[...]).astype(bf16)
            grad_wu[s, cols, :] = dot_tn(lhs, up_grad[...]).astype(bf16)
        return carry

    lax.fori_loop(0, half // 256, up_step, 0)
    for i, (src, dst) in enumerate(((grad_wg, owg), (grad_wu, owu))):
        stores.append(pltpu.make_async_copy(src, dst, out_sem.at[2 + i]))
        stores[-1].start()

    later_sum = dot_full(grad_t, causal_f)
    for k in range(1, n):
        copy_gat[k].wait_recv()
    for b in range(n):
        later_sum = later_sum + jnp.where(b > me, gat_recv[b, :, 0:1], 0.0)
    odecay[...] = later_sum

    for copy in copy_rs[1:]:
        copy.wait_recv()
    for q in range(1, inner):
        oproj[...] += rs_recv[q].astype(f32)
    for copies in (
        copy_g, copy_h, copy_ret, copy_st, copy_rv, copy_tot, copy_gat, copy_sl, copy_hz, fwd_z,
        copy_rs, fwd_g, fwd_h, px, [copy_gh],
    ):
        for copy in copies:
            if copy is not None:
                copy.wait_send()
    for s in range(outer - 1):
        send_hid(s, drain=True)
        send_mz(s, drain=True)
    for store in stores:
        store.wait()


def pass_through(count, *refs):
    ins, outs, held = refs[:count], refs[count:2 * count], refs[2 * count:3 * count]
    in_sem, out_sem = refs[3 * count:]
    reads = [pltpu.make_async_copy(ins[i], held[i], in_sem.at[i]) for i in range(count)]
    writes = [pltpu.make_async_copy(held[i], outs[i], out_sem.at[i]) for i in range(count)]
    for read in reads:
        read.start()
    for read, write in zip(reads, writes):
        read.wait()
        write.start()
    for write in writes:
        write.wait()


def hand_over(arrays):
    count = len(arrays)
    pieces = []
    for array in arrays:
        pieces.append(jax.ShapeDtypeStruct(array.shape, array.dtype))
    aspec = pl.BlockSpec(memory_space=pl.ANY)
    return pl.pallas_call(
        functools.partial(pass_through, count),
        out_shape=tuple(pieces),
        in_specs=[aspec] * count,
        out_specs=(aspec,) * count,
        scratch_shapes=[pltpu.VMEM(p.shape, p.dtype) for p in pieces]
        + [pltpu.SemaphoreType.DMA((count,))] * 2,
        name="hand_over",
    )(*arrays)


def fused_body(
    mixer_output, layer_cotangent, expert_choice, route_weight, gate_pre, up_pre,
    w_gate, w_up, w_down, w_out, norm_gain, scan_in, gate_in, b_proj, c_proj,
    log_decay, entry_state,
):
    n = lax.axis_size("sp")
    outer = 4
    inner = n // outer
    tokens, width = mixer_output.shape
    half = width // 2
    rows, units = gate_pre.shape[1:]
    cap = rows // n
    heads = log_decay.shape[1]
    channels = scan_in.shape[1]
    state_rows = heads * HEAD_DIM
    srows = state_rows // n
    groups = b_proj.shape[1] // STATE
    pairs = heads // 2
    dchunk = width // outer
    dcols = width // n
    vm = pltpu.VMEM
    dma = pltpu.SemaphoreType.DMA
    wide = jax.ShapeDtypeStruct
    vspec = pl.BlockSpec(memory_space=pltpu.VMEM)
    aspec = pl.BlockSpec(memory_space=pl.ANY)
    scratch = [
        vm((tokens, half), bf16), vm((outer, tokens, half), bf16),
        vm((rows, units), bf16), vm((rows, units), bf16),
        vm((2, half, units), bf16), vm((2, half, units), bf16),
        vm((units, width), bf16), vm((channels, width), bf16),
        vm((rows, half), bf16), vm((outer, rows // outer, half), bf16),
        vm((2, rows, half), bf16), vm((2, rows, half), bf16),
        vm((outer, rows // outer, half), bf16), vm((outer, rows // outer, half), bf16),
        vm((rows, half), bf16), vm((rows, half), bf16),
        vm((rows, units), bf16), vm((rows, units), bf16), vm((rows, units), bf16),
        vm((tokens, rows), bf16),
        vm((outer, tokens, channels), bf16), vm((outer, tokens, dchunk), bf16),
        vm((outer, tokens, dchunk), bf16),
        vm((inner, dcols, channels), bf16), vm((inner, dcols, channels), bf16),
        vm((tokens, channels), f32), vm((tokens, channels), f32), vm((groups, tokens, 1), f32),
        vm((tokens, channels), f32), vm((pairs, tokens, 2 * tokens), bf16),
        vm((heads, tokens, tokens), f32), vm((tokens, heads), f32), vm((tokens, heads), f32),
        vm((state_rows, STATE), bf16), vm((groups, tokens, STATE), f32),
        vm((state_rows, STATE), bf16), vm((state_rows, STATE), bf16),
        vm((state_rows, STATE), bf16), vm((state_rows, STATE), bf16),
        vm((8, 128), f32), vm((n, 8, 128), f32), vm((outer, 8, tokens), f32),
        vm((heads, 128), f32), vm((n, heads, 128), f32),
        vm((2, half, units), bf16), vm((2, half, units), bf16), vm((2, units, half), bf16),
        dma((8,)), dma((4,)),
    ]
    scratch += [dma((n,))] * 12
    scratch += [dma((outer,))] * 8
    scratch += [dma((4, outer)), dma((4, outer)), dma((outer, inner)), dma((outer, inner))]
    scratch += [dma, dma]
    scratch += [dma((outer,))] * 4
    scratch += [dma((inner,))] * 2
    outs = pl.pallas_call(
        functools.partial(fused, (n, outer, cap)),
        out_shape=(
            wide((2, half, units), bf16), wide((2, half, units), bf16), wide((units, width), bf16),
            wide((dcols, channels), f32), wide((tokens, channels), bf16),
            wide((tokens, channels), bf16), wide((tokens, groups * STATE), bf16),
            wide((tokens, groups * STATE), bf16), wide((heads, tokens), f32),
        ),
        in_specs=[vspec] * 9 + [aspec] * 8,
        out_specs=(aspec,) * 3 + (vspec,) * 6,
        scratch_shapes=scratch,
        compiler_params=pltpu.CompilerParams(
            collective_id=0, has_side_effects=True, vmem_limit_bytes=64 * 1024 * 1024 - 128 * 1024
        ),
        name="fused",
    )(
        expert_choice.T, route_weight.T, log_decay.T,
        norm_gain.reshape(channels // 128, 128), scan_in, gate_in, b_proj, c_proj,
        entry_state.reshape(state_rows, STATE),
        layer_cotangent, mixer_output, gate_pre[0], up_pre[0],
        w_gate.reshape(2, half, units), w_up.reshape(2, half, units), w_down[0], w_out,
    )
    gwg, gwu, gwd, proj, gscan, ggate, gb, gc, gdecay = hand_over(outs)
    return (
        gwg.reshape(1, width, units), gwu.reshape(1, width, units), gwd[None],
        proj, gscan, ggate, gb, gc, gdecay.T,
    )


def entry_slots(expert_choice, expert_count, capacity):
    tokens, top_count = expert_choice.shape
    targets = expert_choice.reshape(-1)
    experts = jnp.arange(expert_count, dtype=jnp.int32)
    one_hot = (targets[:, None] == experts[None, :]).astype(jnp.float32)
    entries = jnp.arange(tokens * top_count, dtype=jnp.int32)
    before = (entries[:, None] > entries[None, :]).astype(jnp.bfloat16)
    earlier = jnp.dot(before, one_hot.astype(jnp.bfloat16), preferred_element_type=jnp.float32)
    ranks = jnp.sum(earlier * one_hot, axis=1).astype(jnp.int32)
    return (targets * capacity + ranks).reshape(tokens, top_count)


def expert_side(grad_rows, gate_value, up_value, gate_weight, up_weight, down_weight):
    act_grad = jnp.einsum("rd,fd->rf", grad_rows, down_weight, preferred_element_type=jnp.float32)
    gate_full = gate_value.astype(jnp.float32)
    up_full = up_value.astype(jnp.float32)
    gate_clip = jnp.minimum(gate_full, clamp_limit)
    up_clip = jnp.clip(up_full, -clamp_limit, clamp_limit)
    sigmoid_gate = jax.nn.sigmoid(swish_alpha * gate_clip)
    swish_gate = gate_clip * sigmoid_gate
    active = ((up_clip + 1.0) * swish_gate).astype(jnp.bfloat16)
    up_grad = jnp.where(
        (up_full > -clamp_limit) & (up_full < clamp_limit), act_grad * swish_gate, 0.0
    ).astype(jnp.bfloat16)
    slope = sigmoid_gate + swish_alpha * gate_clip * sigmoid_gate * (1.0 - sigmoid_gate)
    gate_grad = jnp.where(gate_full < clamp_limit, act_grad * (up_clip + 1.0) * slope, 0.0).astype(
        jnp.bfloat16
    )
    partial_rows = jnp.einsum(
        "rf,df->rd", gate_grad, gate_weight, preferred_element_type=jnp.float32
    )
    partial_rows = partial_rows + jnp.einsum(
        "rf,df->rd", up_grad, up_weight, preferred_element_type=jnp.float32
    )
    return (active, gate_grad, up_grad, partial_rows)


def exchange(pieces):
    return lax.all_to_all(pieces, "sp", split_axis=0, concat_axis=0, tiled=True)


def tell_all(vector):
    return exchange(jnp.broadcast_to(vector, (lax.axis_size("sp"), *vector.shape)))


def later_states(block_state, totals):
    count = lax.axis_size("sp")
    heads, channels, width = block_state.shape
    rows = heads * channels // count
    spots = jnp.arange(count)
    between = (
        (spots[:, None, None] < spots[None, None, :]) & (spots[None, None, :] < spots[None, :, None])
    ).astype(jnp.float32)
    gaps = jnp.einsum("bck,kh->bch", between, totals, precision=lax.Precision.HIGHEST)
    later = spots[:, None, None] < spots[None, :, None]
    weights = jnp.where(later, jnp.exp(gaps), 0.0)
    first = lax.axis_index("sp") * rows
    picks = (
        ((first + jnp.arange(rows)) // channels)[None, :] == jnp.arange(heads)[:, None]
    ).astype(jnp.float32)
    weights = jnp.einsum("bch,hr->bcr", weights, picks, precision=lax.Precision.HIGHEST)
    dealt = lax.all_to_all(
        block_state.astype(jnp.bfloat16).reshape(count, rows, width),
        "sp",
        split_axis=0,
        concat_axis=0,
        tiled=True,
    ).astype(jnp.float32)
    sums = jnp.sum(weights[:, :, :, None] * dealt[None], axis=1)
    back = lax.all_to_all(
        sums.astype(jnp.bfloat16), "sp", split_axis=0, concat_axis=0, tiled=True
    )
    return back.reshape(heads, channels, width)


def body(
    mixer_output,
    layer_cotangent,
    expert_choice,
    route_weight,
    gate_pre,
    up_pre,
    w_gate,
    w_up,
    w_down,
    w_out,
    norm_gain,
    scan_in,
    gate_in,
    b_proj,
    c_proj,
    log_decay,
    entry_state,
):
    expert_count = lax.axis_size("sp")
    tokens_here = mixer_output.shape[0]
    model_width = mixer_output.shape[1]
    top_count = expert_choice.shape[1]
    capacity = gate_pre.shape[1] // expert_count
    columns = model_width // lax.axis_size("tp")
    first_column = lax.axis_index("tp") * columns
    own_cotangent = lax.dynamic_slice_in_dim(layer_cotangent, first_column, columns, 1).astype(
        jnp.float32
    )
    own_hidden = lax.dynamic_slice_in_dim(mixer_output, first_column, columns, 1)
    slots = entry_slots(expert_choice, expert_count, capacity)
    slot_ids = jnp.arange(expert_count * capacity, dtype=jnp.int32)
    places = (slots.T[:, None, :] == slot_ids[None, :, None]).astype(jnp.bfloat16)
    token_places = places.sum(axis=0)
    weighted = (route_weight.T[:, :, None] * own_cotangent[None]).astype(jnp.bfloat16)

    def dispatch(rows):
        arrived = lax.all_to_all(
            rows.astype(jnp.bfloat16).reshape(expert_count, capacity, columns),
            "sp",
            split_axis=0,
            concat_axis=0,
            tiled=True,
        ).reshape(-1, columns)
        return lax.all_gather(arrived, "tp", axis=1, tiled=True)

    recv_grads = dispatch(
        jnp.einsum("kst,ktd->sd", places, weighted, preferred_element_type=jnp.float32)
    )
    active, gate_grad, up_grad, partial_rows = expert_side(
        recv_grads,
        gate_pre[0],
        up_pre[0],
        w_gate[0],
        w_up[0],
        w_down[0],
    )
    summed = lax.psum_scatter(
        partial_rows.astype(jnp.bfloat16), "tp", scatter_dimension=1, tiled=True
    )
    returned = lax.all_to_all(
        summed.reshape(expert_count, capacity, -1), "sp", split_axis=0, concat_axis=0, tiled=True
    )
    head_count = log_decay.shape[1]
    group_count = b_proj.shape[1] // STATE
    per_group = head_count // group_count
    scan_heads = scan_in.reshape(tokens_here, head_count, HEAD_DIM)
    b_groups = b_proj.reshape(tokens_here, group_count, STATE)
    c_groups = c_proj.reshape(tokens_here, group_count, STATE)
    x_float = scan_heads.astype(jnp.float32)
    token_locations = jnp.arange(tokens_here)
    causal = token_locations[:, None] >= token_locations[None, :]
    causal_float = causal.astype(jnp.float32)
    cumulative = jnp.dot(causal_float, log_decay, precision=lax.Precision.HIGHEST)
    growth = jnp.exp(cumulative)
    block_decays = tell_all(lax.optimization_barrier((cumulative[-1], summed))[0])
    tail_decay = jnp.exp(cumulative[-1][None, :] - cumulative)
    log_gaps = cumulative.T[:, :, None] - cumulative.T[:, None, :]
    decay_mat = jnp.exp(jnp.where(causal[None], log_gaps, -jnp.inf))
    inner_prod = jnp.einsum("tgn,sgn->gts", c_groups, b_groups, preferred_element_type=jnp.float32)
    mix_weights = (jnp.repeat(inner_prod, per_group, axis=0) * decay_mat).astype(jnp.bfloat16)
    state_groups = entry_state.astype(jnp.bfloat16).reshape(group_count, per_group, HEAD_DIM, STATE)
    y_inner = jnp.einsum(
        "hts,shp->thp", mix_weights, scan_heads, preferred_element_type=jnp.float32
    )
    y_carry = jnp.einsum(
        "tgn,grpn->tgrp", c_groups, state_groups, preferred_element_type=jnp.float32
    ).reshape(tokens_here, head_count, HEAD_DIM)
    scan_out = y_inner + y_carry * growth[:, :, None]
    gate_float = gate_in.astype(jnp.float32)
    gate_sig = jax.nn.sigmoid(gate_float)
    gate_silu = gate_float * gate_sig
    gated = scan_out.reshape(tokens_here, -1) * gate_silu
    grouped = gated.reshape(tokens_here, group_count, -1)
    inv_rms = lax.rsqrt(jnp.mean(grouped * grouped, axis=-1, keepdims=True) + rms_epsilon)
    unit = grouped * inv_rms
    gain_groups = norm_gain.astype(jnp.float32).reshape(group_count, -1)
    mixed = (unit * gain_groups).reshape(tokens_here, -1).astype(jnp.bfloat16)
    all_mixed = lax.all_gather(mixed, "sp", axis=0, tiled=True)
    returned, mixed = lax.optimization_barrier((returned, mixed))
    moe_terms = jnp.einsum(
        "st,sd->td",
        token_places,
        returned.reshape(-1, columns),
        preferred_element_type=jnp.float32,
    )
    grad_hidden = lax.all_gather(
        (own_cotangent + moe_terms).astype(jnp.bfloat16), "tp", axis=1, tiled=True
    )
    late_hidden, grad_hidden = lax.optimization_barrier((own_hidden, grad_hidden))
    recv_hidden = dispatch(
        jnp.einsum("st,td->sd", token_places, late_hidden, preferred_element_type=jnp.float32)
    )
    down_wgrad = jnp.einsum(
        "rf,rd->fd", active, recv_grads, preferred_element_type=jnp.float32
    ).astype(jnp.bfloat16)
    gate_wgrad = jnp.einsum(
        "rd,rf->df", recv_hidden, gate_grad, preferred_element_type=jnp.float32
    ).astype(jnp.bfloat16)
    up_wgrad = jnp.einsum(
        "rd,rf->df", recv_hidden, up_grad, preferred_element_type=jnp.float32
    ).astype(jnp.bfloat16)
    own_block = lax.all_to_all(
        grad_hidden.reshape(tokens_here, expert_count, -1).transpose(1, 0, 2),
        "sp",
        split_axis=0,
        concat_axis=0,
        tiled=True,
    )
    grad_out_proj = jnp.einsum(
        "td,ti->di",
        own_block.reshape(-1, own_block.shape[2]),
        all_mixed,
        preferred_element_type=jnp.float32,
    )
    grad_mixed = jnp.einsum("td,id->ti", grad_hidden, w_out, preferred_element_type=jnp.float32)
    grad_unit = grad_mixed.reshape(tokens_here, group_count, -1) * gain_groups
    grad_grouped = inv_rms * (grad_unit - unit * jnp.mean(grad_unit * unit, axis=-1, keepdims=True))
    grad_gated = grad_grouped.reshape(tokens_here, -1)
    grad_gate_in = (
        grad_gated
        * scan_out.reshape(tokens_here, -1)
        * gate_sig
        * (1.0 + gate_float * (1.0 - gate_sig))
    ).astype(jnp.bfloat16)
    grad_y = (grad_gated * gate_silu).reshape(tokens_here, head_count, HEAD_DIM)
    grad_y_b = grad_y.astype(jnp.bfloat16)
    grad_x_inner = jnp.einsum(
        "hts,thp->shp", mix_weights, grad_y_b, preferred_element_type=jnp.float32
    )
    grad_weights = (
        jnp.einsum("thp,shp->hts", grad_y_b, scan_heads, preferred_element_type=jnp.float32)
        * decay_mat
    )
    grad_weights = (
        grad_weights.reshape(group_count, per_group, tokens_here, tokens_here)
        .sum(axis=1)
        .astype(jnp.bfloat16)
    )
    grad_c_inner = jnp.einsum(
        "gts,sgn->tgn", grad_weights, b_groups, preferred_element_type=jnp.float32
    )
    grad_b_inner = jnp.einsum(
        "gts,tgn->sgn", grad_weights, c_groups, preferred_element_type=jnp.float32
    )
    grown_grads = (grad_y * growth[:, :, None]).astype(jnp.bfloat16).reshape(
        tokens_here, group_count, per_group, HEAD_DIM
    )
    grad_c_carry = jnp.einsum(
        "tgrp,grpn->tgn", grown_grads, state_groups, preferred_element_type=jnp.float32
    )
    block_state = jnp.einsum(
        "tgrp,tgn->grpn", grown_grads, c_groups, preferred_element_type=jnp.float32
    ).reshape(head_count, HEAD_DIM, STATE)
    x_tail = (x_float * tail_decay[:, :, None]).astype(jnp.bfloat16).reshape(
        tokens_here, group_count, per_group, HEAD_DIM
    )
    later_state = later_states(block_state, block_decays)
    later_groups = later_state.reshape(group_count, per_group, HEAD_DIM, STATE)
    grad_x_carry = jnp.einsum(
        "sgn,grpn->sgrp", b_groups, later_groups, preferred_element_type=jnp.float32
    ).reshape(tokens_here, head_count, HEAD_DIM)
    grad_x = grad_x_inner + grad_x_carry * tail_decay[:, :, None]
    grad_b_carry = jnp.einsum(
        "sgrp,grpn->sgn", x_tail, later_groups, preferred_element_type=jnp.float32
    )
    grad_a = jnp.sum(grad_y * scan_out, axis=2) - jnp.sum(x_float * grad_x, axis=2)
    block_totals = tell_all(jnp.sum(grad_a, axis=0))
    is_later = jnp.arange(expert_count) > lax.axis_index("sp")
    later_grad = jnp.sum(jnp.where(is_later[:, None], block_totals, 0.0), axis=0)
    grad_log_decay = (
        jnp.dot(causal_float.T, grad_a, precision=lax.Precision.HIGHEST) + later_grad[None, :]
    )
    grad_scan_in = grad_x.reshape(tokens_here, -1).astype(jnp.bfloat16)
    grad_b_proj = (grad_b_inner + grad_b_carry).reshape(tokens_here, -1).astype(jnp.bfloat16)
    grad_c_proj = (grad_c_inner + grad_c_carry).reshape(tokens_here, -1).astype(jnp.bfloat16)
    return (
        gate_wgrad[None],
        up_wgrad[None],
        down_wgrad[None],
        grad_out_proj,
        grad_scan_in,
        grad_gate_in,
        grad_b_proj,
        grad_c_proj,
        grad_log_decay,
    )


def solution(mesh):
    in_specs = (
        P("sp", None),
        P("sp", None),
        P("sp", None),
        P("sp", None),
        P("sp", None, "tp"),
        P("sp", None, "tp"),
        P("sp", None, "tp"),
        P("sp", None, "tp"),
        P("sp", "tp", None),
        P("tp", None),
        P("tp"),
        P("sp", "tp"),
        P("sp", "tp"),
        P("sp", "tp"),
        P("sp", "tp"),
        P("sp", "tp"),
        P("sp", "tp", None, None),
    )
    out_specs = (
        P("sp", None, "tp"),
        P("sp", None, "tp"),
        P("sp", "tp", None),
        P("sp", "tp"),
        P("sp", "tp"),
        P("sp", "tp"),
        P("sp", "tp"),
        P("sp", "tp"),
        P("sp", "tp"),
    )
    def run(*args):
        count = mesh.shape["sp"]
        capacity = args[4].shape[1] // count
        simple = mesh.shape["tp"] != 2 or count % 4 or count & (count - 1) or capacity % 16
        return (body if simple else fused_body)(*args)

    return jax.shard_map(run, mesh=mesh, in_specs=in_specs, out_specs=out_specs, check_vma=False)
```

```python
import functools

import jax
import jax.numpy as jnp
from jax import lax
from jax.sharding import PartitionSpec as P

from jax.experimental import pallas as pl
from jax.experimental.pallas import tpu as pltpu

HEAD_DIM = 64
STATE = 128


rms_epsilon = 1e-05
clamp_limit = 7.0
swish_alpha = 1.702


MESH = pl.DeviceIdType.MESH
f32, bf16 = jnp.float32, jnp.bfloat16


def dot_nn(a, b):
    return jnp.dot(a, b, preferred_element_type=f32)


def dot_nt(a, b):
    return lax.dot_general(a, b, (((1,), (1,)), ((), ())), preferred_element_type=f32)


def dot_tn(a, b):
    return lax.dot_general(a, b, (((0,), (0,)), ((), ())), preferred_element_type=f32)


def dot_full(a, b):
    return jnp.dot(a, b, precision=lax.Precision.HIGHEST, preferred_element_type=f32)


def xor(value, bits):
    bit = 1
    while bit <= bits:
        if bits & bit:
            value = value + bit * (1 - 2 * ((value // bit) % 2))
        bit *= 2
    return value


def iota(shape, dim):
    return lax.broadcasted_iota(jnp.int32, shape, dim)


def aligned(value, unit):
    return pl.multiple_of(value, unit)


PLAN = {'sent': (), ('chunk', 0): (), ('chunk', 1): ('cot2', 'hid0'), ('chunk', 2): ('cot3', 'hid1'), ('chunk', 3): (), 'forward': ('cot1',), 'experts': ('hid2', 'mz0'), 'down': ('hid3', 'mz1'), 'combined': (), 'states': ('mz2',), 'inner': ('mz3',), 'later': ('proj',), 'final': ()}


def fused(
    dims,
    choice_t, weight_t, decay_t, gain, scan_hbm, gate_hbm, b_hbm, c_hbm, entry_hbm,
    cot_hbm, hid_hbm, gpre_hbm, upre_hbm, wg_hbm, wu_hbm, wd_hbm, wo_hbm,
    owg, owu, owd, proj_hbm, oscan_hbm, ogate_hbm, ob_hbm, oc_hbm, odecay,
    scan_x, gate_x, b_in, c_in, entry, oproj, oscan, ogate, ob, oc,
    cot_z, hid_z, gpre, upre, wg, wu, wd, wo,
    send_g, send_h, g_full, h_full, part_send, part_recv, ret_send, ret_recv,
    active, gate_grad, up_grad, places_t,
    mixed_z, hidden, hidden_z, rs_send, rs_recv,
    scan_out, unit, inv_rms, gy, mix_t, decays, growth_s, tail_s, entry_b, block_state,
    st_send, st_recv, rv_send, rv_recv, tot_send, tot_recv, slot_recv, gat_send, gat_recv,
    grad_wg, grad_wu, grad_wd,
    in_sem, out_sem, ret_s, ret_r, st_s, st_r, rv_s, rv_r,
    tot_s, tot_r, gat_s, gat_r, fg_s, fg_r, fh_s, fh_r, px_s, px_r, sl_s, sl_r, mz_line, hid_line, cot_line, h_s, h_r, g_s, g_r,
    gh_s, gh_r, hz_s, hz_r, fz_s, fz_r, rs_s, rs_r,
):
    n, outer, cap = dims
    inner = n // outer
    tokens, half = cot_z.shape[1:]
    rows = n * cap
    zrows = inner * cap
    heads = decay_t.shape[0]
    groups = b_in.shape[1] // STATE
    pairs_in_group = heads // groups // 2
    gwidth = pairs_in_group * 128
    per_half = outer // 2
    dchunk = hidden.shape[2]
    srows = st_send.shape[0] // n
    dcols = dchunk // inner
    thalf = tokens // 2
    me = lax.axis_index("sp")
    tp = lax.axis_index("tp")
    other = 1 - tp
    my_z = me // inner
    my_q = me % inner
    peers = [xor(me, k) for k in range(n)]

    def remote(src, dst, s, r, sp_id, tp_id):
        return pltpu.make_async_remote_copy(
            src_ref=src, dst_ref=dst, send_sem=s, recv_sem=r,
            device_id=(sp_id, tp_id), device_id_type=MESH,
        )

    def rowblock(block, size):
        return pl.ds(aligned(block * size, size), size)

    barrier = pltpu.get_barrier_semaphore()
    for k in range(1, n):
        pl.semaphore_signal(barrier, inc=1, device_id=(peers[k], tp), device_id_type=MESH)
    pl.semaphore_signal(barrier, inc=1, device_id=(me, other), device_id_type=MESH)

    own_cols = pl.ds(aligned(tp * half, half), half)
    loads = [
        pltpu.make_async_copy(cot_hbm.at[:, own_cols], cot_z.at[my_z], in_sem.at[0]),
        pltpu.make_async_copy(hid_hbm.at[:, own_cols], hid_z.at[my_z], in_sem.at[1]),
        pltpu.make_async_copy(wd_hbm, wd, in_sem.at[2]),
        pltpu.make_async_copy(gpre_hbm, gpre, in_sem.at[3]),
        pltpu.make_async_copy(upre_hbm, upre, in_sem.at[4]),
        pltpu.make_async_copy(wg_hbm, wg, in_sem.at[5]),
        pltpu.make_async_copy(wu_hbm, wu, in_sem.at[6]),
        pltpu.make_async_copy(wo_hbm, wo, in_sem.at[7]),
    ]
    pairs_of_refs = (
        (b_hbm, b_in), (c_hbm, c_in), (scan_hbm, scan_x), (entry_hbm, entry), (gate_hbm, gate_x),
    )
    mixer_loads = [
        pltpu.make_async_copy(src, dst, in_sem.at[8 + i])
        for i, (src, dst) in enumerate(pairs_of_refs)
    ]
    stores = []

    def store(src, dst):
        copy = pltpu.make_async_copy(src, dst, out_sem.at[len(stores)])
        copy.start()
        stores.append(copy)

    for load in loads[:2] + mixer_loads + loads[2:]:
        load.start()

    expert_s = iota((n, tokens), 0)
    first_t = choice_t[0:1, :] == expert_s
    second_t = choice_t[1:2, :] == expert_s
    row_id = iota((tokens, tokens), 0)
    col_id = iota((tokens, tokens), 1)
    named_t = jnp.where(first_t | second_t, 1.0, 0.0).astype(bf16)
    before_t = jnp.where(row_id < col_id, 1.0, 0.0).astype(bf16)
    base_t = dot_nn(named_t, before_t) + (cap * expert_s).astype(f32)
    slot0_t = jnp.sum(jnp.where(first_t, base_t, 0.0), axis=0, keepdims=True)
    slot1_t = jnp.sum(jnp.where(second_t, base_t, 0.0), axis=0, keepdims=True)

    def column(row):
        return jnp.sum(jnp.where(row_id == col_id, row, 0.0), axis=1, keepdims=True)

    slot0, slot1 = column(slot0_t), column(slot1_t)
    slot_l = iota((tokens, rows), 1).astype(f32)
    places_t[...] = jnp.where((slot_l == slot0) | (slot_l == slot1), 1.0, 0.0).astype(bf16)

    slot_recv[my_z] = jnp.zeros(slot_recv.shape[1:], f32)
    slot_recv[my_z, 0:1, :] = slot0_t
    slot_recv[my_z, 1:2, :] = slot1_t
    slot_recv[my_z, 2:4, :] = weight_t[...]
    loads[0].wait()
    pl.semaphore_wait(barrier, n)

    def line(buf, sems):
        def up(s):
            block = (my_z - s + outer) % outer
            return remote(
                buf.at[block], buf.at[block], sems.at[0, s], sems.at[1, s], (me + inner) % n, tp
            )

        def down(s):
            block = (my_z + s) % outer
            return remote(
                buf.at[block], buf.at[block], sems.at[2, s], sems.at[3, s],
                (me - inner + n) % n, tp,
            )

        def send(s, drain=False):
            @pl.when((my_z >= s) & (my_z < outer - 1))
            def _():
                up(s).wait_send() if drain else up(s).start()

            @pl.when((my_z + s < outer) & (my_z > 0))
            def _():
                down(s).wait_send() if drain else down(s).start()

        def take(s):
            @pl.when(my_z > s)
            def _():
                up(s).wait_recv()

            @pl.when(my_z + s + 1 < outer)
            def _():
                down(s).wait_recv()

        return send, take

    send_hid, take_hid = line(hid_z, hid_line)
    send_mz, take_mz = line(mixed_z, mz_line)
    send_cot, take_cot = line(cot_z, cot_line)

    def at(point):
        for step in PLAN[point]:
            steps[step]()

    def all_to_all(send, recv, size, s, r):
        mine = rowblock(me, size)
        return [None] + [
            remote(send.at[rowblock(peers[k], size)], recv.at[mine], s.at[k], r.at[k], peers[k], tp)
            for k in range(1, n)
        ]

    own_rows = rowblock(me, cap)
    copy_st = all_to_all(st_send, st_recv, srows, st_s, st_r)
    copy_rv = all_to_all(rv_send, rv_recv, srows, rv_s, rv_r)
    far_first = list(range(n - 1, 0, -1))
    copy_sl = [None] + [
        remote(
            slot_recv.at[my_z], slot_recv.at[my_z], sl_s.at[j], sl_r.at[j],
            xor(my_z, j) * inner + my_q, tp,
        )
        for j in range(1, outer)
    ]
    send_cot(0)
    for j in range(1, outer):
        copy_sl[j].start()

    copy_rs = [None]

    def output_projection():
        for j in range(1, outer):
            copy_hz[j].wait_recv()
            fwd_z[j].start()
        for j in range(1, outer):
            fwd_z[j].wait_recv()
        for q in range(inner - 1, -1, -1):
            target = xor(my_q, q)
            dpart = pl.ds(aligned(target * dcols, dcols), dcols)
            for s in range(half // 512):
                cols = slice(s * 512, (s + 1) * 512)
                total = dot_tn(hidden_z[0, :, dpart], mixed_z[0, :, cols])
                for z in range(1, outer):
                    total = total + dot_tn(hidden_z[z, :, dpart], mixed_z[z, :, cols])
                if q:
                    rs_send[q, :, cols] = total.astype(bf16)
                else:
                    oproj[:, cols] = total
            if q:
                copy = remote(
                    rs_send.at[q], rs_recv.at[q], rs_s.at[q], rs_r.at[q], my_z * inner + target, tp
                )
                copy.start()
                copy_rs.append(copy)

    def plane_dest(b):
        return pl.ds(aligned((b * inner + my_q) * cap, cap), cap)

    def plane_copy(send, full, sems, b, q):
        target = xor(my_q, q)
        return remote(
            send.at[b, rowblock(target, cap)], full.at[tp, plane_dest(b)],
            sems[0].at[b, q], sems[1].at[b, q], my_z * inner + target, tp,
        )

    def hidden_copy(b, q):
        return plane_copy(send_h, h_full, (h_s, h_r), b, q)

    def cot_copy(b, q):
        return plane_copy(send_g, g_full, (g_s, g_r), b, q)

    def deal(b, source, send, full, copy, weighted):
        slot_h = (iota((zrows, tokens), 0) + my_z * zrows).astype(f32)
        in_first = slot_h == slot_recv[b, 0:1, :]
        in_second = slot_h == slot_recv[b, 1:2, :]
        places = jnp.where(in_first | in_second, 1.0, 0.0).astype(bf16)
        rows_b = dot_nn(places, source[b])
        if weighted:
            rows_b = rows_b * jnp.sum(
                jnp.where(in_first, slot_recv[b, 2:3, :], 0.0)
                + jnp.where(in_second, slot_recv[b, 3:4, :], 0.0),
                axis=1, keepdims=True,
            )
        send[b] = rows_b.astype(bf16)
        for q in range(inner - 1, 0, -1):
            copy(b, q).start()
        full[tp, plane_dest(b), :] = send[b, rowblock(my_q, cap), :]

    def hidden_block(b):
        deal(b, hid_z, send_h, h_full, hidden_copy, False)

    def cot_block(b):
        deal(b, cot_z, send_g, g_full, cot_copy, True)

    def at_distance(distance, action):
        @pl.when(my_z >= distance)
        def _():
            action((my_z - distance + outer) % outer)

        @pl.when(my_z + distance < outer)
        def _():
            action((my_z + distance) % outer)

    def cot_next(s):
        if s == 1:
            for j in range(1, outer):
                copy_sl[j].wait_recv()
        take_cot(s - 1)
        if s < outer - 1:
            send_cot(s)
        at_distance(s, cot_block)

    def hidden_own():
        loads[1].wait()
        send_hid(0)
        hidden_block(my_z)

    def hidden_send():
        loads[1].wait()
        send_hid(0)

    def hidden_next(s):
        take_hid(s - 1)
        if s < outer - 1:
            send_hid(s)
        at_distance(s, hidden_block)

    forwarded = []

    def forward_hidden(j):
        for q in range(1, inner):
            hidden_copy(xor(my_z, j), q).wait_recv()
        fwd_h[j].start()
        forwarded.append(j)

    def pass_on(send, take, s):
        take(s - 1)
        send(s)

    steps = {
        "cot1": lambda: cot_next(1),
        "cot2": lambda: cot_next(2),
        "cot3": lambda: cot_next(3),
        "hid0": hidden_own,
        "hid0s": hidden_send,
        "hid0b": lambda: hidden_block(my_z),
        "hid1": lambda: hidden_next(1),
        "hid2": lambda: hidden_next(2),
        "hid3": lambda: hidden_next(3),
        "mz0": lambda: send_mz(0),
        "mz1": lambda: pass_on(send_mz, take_mz, 1),
        "mz2": lambda: pass_on(send_mz, take_mz, 2),
        "mz3": lambda: take_mz(outer - 2),
        "proj": output_projection,
        "fwd0": lambda: forward_hidden(0),
        "fwd1": lambda: forward_hidden(1),
        "fwd2": lambda: forward_hidden(2),
    }

    cot_block(my_z)

    causal = row_id >= col_id
    causal_f = jnp.where(causal, 1.0, 0.0)
    anti_f = jnp.where(row_id <= col_id, 1.0, 0.0)
    cum_t = dot_full(decay_t[...], anti_f)
    cum = cum_t.T
    growth_s[...] = jnp.exp(cum)
    tail_s[...] = jnp.exp(cum[tokens - 1:tokens, :] - cum)
    tot_send[...] = jnp.zeros(tot_send.shape, f32)
    tot_send[0:1, 0:heads] = cum[tokens - 1:tokens, :]
    tot_recv[me] = tot_send[...]
    copy_tot = [None] + [
        remote(tot_send, tot_recv.at[me], tot_s.at[k], tot_r.at[k], peers[k], tp)
        for k in range(1, n)
    ]
    for k in far_first:
        copy_tot[k].start()
    at("sent")
    lane = iota((1, 128), 1)
    low_lane = lane < HEAD_DIM
    low = jnp.where(low_lane, 1.0, 0.0)
    low_b, high_b = low.astype(bf16), (1.0 - low).astype(bf16)

    def spread(columns, pair):
        return jnp.where(
            low_lane, columns[:, 2 * pair:2 * pair + 1], columns[:, 2 * pair + 1:2 * pair + 2]
        )

    def tile(index):
        return slice(index * 128, (index + 1) * 128)

    def gain_row(index):
        return gain[index:index + 1, :].astype(f32)

    def group_cols(g):
        return slice(g * gwidth, (g + 1) * gwidth)

    for load in mixer_loads:
        load.wait()
    entry_b[...] = entry[...].astype(bf16)
    for g in range(groups):
        b_g, c_g = b_in[:, tile(g)], c_in[:, tile(g)]
        inner_prod = dot_nt(c_g, b_g)
        inner_t = dot_nt(b_g, c_g)
        squares = jnp.zeros((tokens, 1), f32)
        gated = []
        for pair in range(g * pairs_in_group, (g + 1) * pairs_in_group):
            mats = []
            for h in (2 * pair, 2 * pair + 1):
                gap = cum[:, h:h + 1] - cum_t[h:h + 1, :]
                fade = jnp.exp(jnp.where(causal, gap, -jnp.inf))
                decays[h] = fade
                mats.append((inner_prod * fade).astype(bf16))
                gap_t = cum_t[h:h + 1, :] - cum[:, h:h + 1]
                mix_t[pair, :, tile(h % 2)] = (
                    inner_t * jnp.exp(jnp.where(row_id <= col_id, gap_t, -jnp.inf))
                ).astype(bf16)
            x = scan_x[:, tile(pair)]
            y = dot_nn(mats[0], x * low_b) + dot_nn(mats[1], x * high_b)
            carry = dot_nt(c_g, entry_b[tile(pair), :])
            out = y + carry * spread(growth_s, pair)
            scan_out[:, tile(pair)] = out
            gate = gate_x[:, tile(pair)].astype(f32)
            value = out * (gate * jax.nn.sigmoid(gate))
            squares = squares + jnp.sum(value * value, axis=1, keepdims=True)
            gated.append(value)
        inv = lax.rsqrt(squares * (1.0 / gwidth) + rms_epsilon)
        inv_rms[g] = inv
        for i, value in enumerate(gated):
            cols = tile(g * pairs_in_group + i)
            flat = value * inv
            unit[:, cols] = flat
            mixed_z[my_z, :, cols] = (flat * gain_row(g * pairs_in_group + i)).astype(bf16)

    at("forward")

    for i in range(2, 7):
        loads[i].wait()
    upper = my_z // per_half
    near = upper * (outer - 1 - my_z) + (1 - upper) * my_z

    def in_turn(position):
        block = near * (1 - position) + (1 - near) * position if position < 2 else position
        return upper * (outer - 1 - block) + (1 - upper) * block

    def return_copy(peer, sem):
        return remote(
            ret_send.at[rowblock(peer, cap)], ret_recv.at[own_rows],
            ret_s.at[peer], ret_r.at[sem], peer, tp,
        )

    fwd_g, fwd_h, px = [], [], []
    for j in range(outer):
        zpart = rowblock(in_turn(j), zrows)
        fwd_g.append(
            remote(g_full.at[tp, zpart], g_full.at[tp, zpart], fg_s.at[j], fg_r.at[j], me, other)
        )
        zpart = rowblock(xor(my_z, j), zrows)
        fwd_h.append(
            remote(h_full.at[tp, zpart], h_full.at[tp, zpart], fh_s.at[j], fh_r.at[j], me, other)
        )
        px.append(remote(part_send.at[j], part_recv.at[j], px_s.at[j], px_r.at[j], me, other))
    for j in range(outer):
        at(("chunk", j))
        block = in_turn(j)
        zpart = rowblock(block, zrows)
        for q in range(1, inner):
            cot_copy(block, q).wait_recv()
        fwd_g[j].start()
        fwd_g[j].wait_recv()
        act = dot_nt(g_full[0, zpart, :], wd[:, 0:half])
        act = act + dot_nt(g_full[1, zpart, :], wd[:, half:2 * half])
        gate_full = gpre[zpart, :].astype(f32)
        up_full = upre[zpart, :].astype(f32)
        gate_clip = jnp.minimum(gate_full, clamp_limit)
        up_clip = jnp.clip(up_full, -clamp_limit, clamp_limit)
        sig = jax.nn.sigmoid(swish_alpha * gate_clip)
        swish = gate_clip * sig
        active[zpart, :] = ((up_clip + 1.0) * swish).astype(bf16)
        inside = (up_full > -clamp_limit) & (up_full < clamp_limit)
        ug = jnp.where(inside, act * swish, 0.0).astype(bf16)
        slope = sig + swish_alpha * gate_clip * sig * (1.0 - sig)
        gg = jnp.where(gate_full < clamp_limit, act * (up_clip + 1.0) * slope, 0.0).astype(bf16)
        up_grad[zpart, :] = ug
        gate_grad[zpart, :] = gg
        part_send[j] = (dot_nt(gg, wg[other]) + dot_nt(ug, wu[other])).astype(bf16)
        px[j].start()
        own = (dot_nt(gg, wg[tp]) + dot_nt(ug, wu[tp])).astype(bf16)
        px[j].wait_recv()
        ret_send[zpart, :] = (own.astype(f32) + part_recv[j].astype(f32)).astype(bf16)
        if j == 0:
            ret_recv[own_rows, :] = ret_send[own_rows, :]
        for q in range(inner - 1, -1, -1):
            if j or q:
                return_copy(block * inner + xor(my_q, q), me).start()

    at("experts")

    def down_step(i, carry):
        cols = pl.ds(aligned(i * 256, 256), 256)
        for s in range(2):
            grad_wd[s, :, cols] = dot_tn(active[...], g_full[s, :, cols]).astype(bf16)
        return carry

    lax.fori_loop(0, half // 256, down_step, 0)
    store(grad_wd.at[0], owd.at[:, 0:half])
    store(grad_wd.at[1], owd.at[:, half:2 * half])

    at("down")
    for k in range(1, n):
        return_copy(peers[k], peers[k]).wait_recv()
    moe = dot_nn(places_t[...], ret_recv[...])
    for i in range(per_half):
        cols = slice(i * dchunk, (i + 1) * dchunk)
        hidden[tp * per_half + i] = (cot_z[my_z, :, cols].astype(f32) + moe[:, cols]).astype(bf16)
    own_chunks = pl.ds(tp * per_half, per_half)
    copy_gh = remote(hidden.at[own_chunks], hidden.at[own_chunks], gh_s, gh_r, me, other)
    copy_gh.start()
    loads[7].wait()
    copy_gh.wait_recv()
    hidden_z[my_z] = hidden[my_z]
    my_tokens = pl.ds(aligned(tp * thalf, thalf), thalf)
    copy_hz, fwd_z = [None], [None]
    for j in range(1, outer):
        z = xor(my_z, j)
        copy_hz.append(
            remote(
                hidden.at[z, my_tokens], hidden_z.at[my_z, my_tokens],
                hz_s.at[j], hz_r.at[j], z * inner + my_q, tp,
            )
        )
        fwd_z.append(
            remote(
                hidden_z.at[z, my_tokens], hidden_z.at[z, my_tokens],
                fz_s.at[j], fz_r.at[j], me, other,
            )
        )
    for j in range(outer - 1, 0, -1):
        copy_hz[j].start()
    at("combined")

    for g in range(groups):
        c_g = c_in[:, tile(g)]
        gcols = group_cols(g)
        gm = dot_nt(hidden[0], wo[gcols, 0:dchunk])
        for i in range(1, outer):
            gm = gm + dot_nt(hidden[i], wo[gcols, i * dchunk:(i + 1) * dchunk])
        gu = jnp.concatenate(
            [
                gm[:, tile(i)] * gain_row(g * pairs_in_group + i)
                for i in range(pairs_in_group)
            ],
            axis=1,
        )
        flat = unit[:, gcols]
        mean = jnp.sum(gu * flat, axis=1, keepdims=True) * (1.0 / gwidth)
        gg = inv_rms[g] * (gu - flat * mean)
        gate = gate_x[:, gcols].astype(f32)
        sig = jax.nn.sigmoid(gate)
        ogate[:, gcols] = (
            gg * scan_out[:, gcols] * sig * (1.0 + gate * (1.0 - sig))
        ).astype(bf16)
        grad_y = gg * (gate * sig)
        gy[:, gcols] = grad_y
        for i in range(pairs_in_group):
            pair = g * pairs_in_group + i
            grown = (grad_y[:, tile(i)] * spread(growth_s, pair)).astype(bf16)
            st_send[tile(pair), :] = dot_tn(grown, c_g).astype(bf16)
    own_st = rowblock(me, srows)
    for k in far_first:
        copy_st[k].start()
    st_recv[own_st, :] = st_send[own_st, :]
    at("states")
    store(ogate, ogate_hbm)

    for g in range(groups):
        b_g, c_g = b_in[:, tile(g)], c_in[:, tile(g)]
        gw = jnp.zeros((tokens, tokens), f32)
        gc = jnp.zeros((tokens, STATE), f32)
        for i in range(pairs_in_group):
            pair = g * pairs_in_group + i
            gy_t = gy[:, tile(pair)]
            gyb = gy_t.astype(bf16)
            x = scan_x[:, tile(pair)]
            gw = gw + dot_nt(gyb * low_b, x) * decays[2 * pair]
            gw = gw + dot_nt(gyb * high_b, x) * decays[2 * pair + 1]
            grown = (gy_t * spread(growth_s, pair)).astype(bf16)
            gc = gc + dot_nn(grown, entry_b[tile(pair), :])
        gwb = gw.astype(bf16)
        oc[:, tile(g)] = (gc + dot_nn(gwb, b_g)).astype(bf16)
        block_state[g] = dot_tn(gwb, c_g)

    store(oc, oc_hbm)
    at("inner")

    for k in range(1, n):
        copy_tot[k].wait_recv()
        copy_st[k].wait_recv()
    my_head = (me * srows) // HEAD_DIM
    rev = jnp.zeros((srows, STATE), f32)
    for b in range(n - 1, -1, -1):
        part = slice(b * srows, (b + 1) * srows)
        rv_send[part, :] = rev.astype(bf16)
        if b:
            total = jnp.sum(
                jnp.where(lane == my_head, tot_recv[b, 0:1, :], 0.0), axis=1, keepdims=True
            )
            rev = st_recv[part, :].astype(f32) + jnp.exp(total) * rev
    for k in far_first:
        copy_rv[k].start()
    rv_recv[own_st, :] = rv_send[own_st, :]
    at("later")

    for k in range(1, n):
        copy_rv[k].wait_recv()
    head_l = iota((1, heads), 1)
    grad_a = jnp.zeros((tokens, heads), f32)
    for g in range(groups):
        b_g = b_in[:, tile(g)]
        gb = block_state[g]
        for i in range(pairs_in_group):
            pair = g * pairs_in_group + i
            gy_t = gy[:, tile(pair)]
            gyb = gy_t.astype(bf16)
            x = scan_x[:, tile(pair)]
            xf = x.astype(f32)
            tail = spread(tail_s, pair)
            later = rv_recv[tile(pair), :]
            gx = dot_nn(mix_t[pair, :, 0:tokens], gyb * low_b)
            gx = gx + dot_nn(mix_t[pair, :, tokens:2 * tokens], gyb * high_b)
            gx = gx + dot_nt(b_g, later) * tail
            oscan[:, tile(pair)] = gx.astype(bf16)
            gb = gb + dot_nn((xf * tail).astype(bf16), later)
            diff = gy_t * scan_out[:, tile(pair)] - xf * gx
            sum_low = jnp.sum(jnp.where(low_lane, diff, 0.0), axis=1, keepdims=True)
            sum_high = jnp.sum(jnp.where(low_lane, 0.0, diff), axis=1, keepdims=True)
            grad_a = jnp.where(head_l == 2 * pair, sum_low, grad_a)
            grad_a = jnp.where(head_l == 2 * pair + 1, sum_high, grad_a)
        ob[:, tile(g)] = gb.astype(bf16)
    store(oscan, oscan_hbm)
    store(ob, ob_hbm)
    grad_t = grad_a.T
    gat_send[...] = jnp.broadcast_to(jnp.sum(grad_t, axis=1, keepdims=True), gat_send.shape)
    copy_gat = [None] + [
        remote(gat_send, gat_recv.at[me], gat_s.at[k], gat_r.at[k], peers[k], tp)
        for k in range(1, n)
    ]
    for k in far_first:
        copy_gat[k].start()
    gat_recv[me] = gat_send[...]

    at("final")
    for j in range(outer):
        if j not in forwarded:
            forward_hidden(j)
    for j in range(outer):
        fwd_h[j].wait_recv()

    def up_step(i, carry):
        cols = pl.ds(aligned(i * 256, 256), 256)
        for s in range(2):
            lhs = h_full[s, :, cols]
            grad_wg[s, cols, :] = dot_tn(lhs, gate_grad[...]).astype(bf16)
            grad_wu[s, cols, :] = dot_tn(lhs, up_grad[...]).astype(bf16)
        return carry

    lax.fori_loop(0, half // 256, up_step, 0)
    store(grad_wg, owg)
    store(grad_wu, owu)

    later_sum = dot_full(grad_t, causal_f)
    for k in range(1, n):
        copy_gat[k].wait_recv()
    for b in range(n):
        later_sum = later_sum + jnp.where(b > me, gat_recv[b, :, 0:1], 0.0)
    odecay[...] = later_sum

    for copy in copy_rs[1:]:
        copy.wait_recv()
    for q in range(1, inner):
        oproj[...] += rs_recv[q].astype(f32)
    store(oproj, proj_hbm)
    for copies in (
        copy_st, copy_rv, copy_tot, copy_gat, copy_sl, copy_hz, fwd_z,
        copy_rs, fwd_g, fwd_h, px, [copy_gh],
    ):
        for copy in copies:
            if copy is not None:
                copy.wait_send()
    for b in range(outer):
        for q in range(1, inner):
            hidden_copy(b, q).wait_send()
            cot_copy(b, q).wait_send()
    for k in range(1, n):
        return_copy(peers[k], peers[k]).wait_send()
    for s in range(outer - 1):
        send_cot(s, drain=True)
        send_hid(s, drain=True)
        send_mz(s, drain=True)
    for copy in stores:
        copy.wait()


def pass_through(count, *refs):
    ins, outs, held = refs[:count], refs[count:2 * count], refs[2 * count:3 * count]
    in_sem, out_sem = refs[3 * count:]
    reads = [pltpu.make_async_copy(ins[i], held[i], in_sem.at[i]) for i in range(count)]
    writes = [pltpu.make_async_copy(held[i], outs[i], out_sem.at[i]) for i in range(count)]
    for read in reads:
        read.start()
    for read, write in zip(reads, writes):
        read.wait()
        write.start()
    for write in writes:
        write.wait()


def hand_over(arrays):
    count = len(arrays)
    pieces = []
    for array in arrays:
        pieces.append(jax.ShapeDtypeStruct(array.shape, array.dtype))
    aspec = pl.BlockSpec(memory_space=pl.ANY)
    return pl.pallas_call(
        functools.partial(pass_through, count),
        out_shape=tuple(pieces),
        in_specs=[aspec] * count,
        out_specs=(aspec,) * count,
        scratch_shapes=[pltpu.VMEM(p.shape, p.dtype) for p in pieces]
        + [pltpu.SemaphoreType.DMA((count,))] * 2,
        name="hand_over",
    )(*arrays)


def fused_body(
    mixer_output, layer_cotangent, expert_choice, route_weight, gate_pre, up_pre,
    w_gate, w_up, w_down, w_out, norm_gain, scan_in, gate_in, b_proj, c_proj,
    log_decay, entry_state,
):
    n = lax.axis_size("sp")
    outer = 4
    inner = n // outer
    tokens, width = mixer_output.shape
    half = width // 2
    rows, units = gate_pre.shape[1:]
    cap = rows // n
    heads = log_decay.shape[1]
    channels = scan_in.shape[1]
    state_rows = heads * HEAD_DIM
    srows = state_rows // n
    groups = b_proj.shape[1] // STATE
    pairs = heads // 2
    dchunk = width // outer
    dcols = width // n
    vm = pltpu.VMEM
    dma = pltpu.SemaphoreType.DMA
    wide = jax.ShapeDtypeStruct
    vspec = pl.BlockSpec(memory_space=pltpu.VMEM)
    aspec = pl.BlockSpec(memory_space=pl.ANY)
    scratch = [
        vm((tokens, channels), bf16), vm((tokens, channels), bf16),
        vm((tokens, groups * STATE), bf16), vm((tokens, groups * STATE), bf16),
        vm((state_rows, STATE), f32), vm((dcols, channels), f32),
        vm((tokens, channels), bf16), vm((tokens, channels), bf16),
        vm((tokens, groups * STATE), bf16), vm((tokens, groups * STATE), bf16),
        vm((outer, tokens, half), bf16), vm((outer, tokens, half), bf16),
        vm((rows, units), bf16), vm((rows, units), bf16),
        vm((2, half, units), bf16), vm((2, half, units), bf16),
        vm((units, width), bf16), vm((channels, width), bf16),
        vm((outer, rows // outer, half), bf16), vm((outer, rows // outer, half), bf16),
        vm((2, rows, half), bf16), vm((2, rows, half), bf16),
        vm((outer, rows // outer, half), bf16), vm((outer, rows // outer, half), bf16),
        vm((rows, half), bf16), vm((rows, half), bf16),
        vm((rows, units), bf16), vm((rows, units), bf16), vm((rows, units), bf16),
        vm((tokens, rows), bf16),
        vm((outer, tokens, channels), bf16), vm((outer, tokens, dchunk), bf16),
        vm((outer, tokens, dchunk), bf16),
        vm((inner, dcols, channels), bf16), vm((inner, dcols, channels), bf16),
        vm((tokens, channels), f32), vm((tokens, channels), f32), vm((groups, tokens, 1), f32),
        vm((tokens, channels), f32), vm((pairs, tokens, 2 * tokens), bf16),
        vm((heads, tokens, tokens), f32), vm((tokens, heads), f32), vm((tokens, heads), f32),
        vm((state_rows, STATE), bf16), vm((groups, tokens, STATE), f32),
        vm((state_rows, STATE), bf16), vm((state_rows, STATE), bf16),
        vm((state_rows, STATE), bf16), vm((state_rows, STATE), bf16),
        vm((8, 128), f32), vm((n, 8, 128), f32), vm((outer, 8, tokens), f32),
        vm((heads, 128), f32), vm((n, heads, 128), f32),
        vm((2, half, units), bf16), vm((2, half, units), bf16), vm((2, units, half), bf16),
        dma((13,)), dma((9,)),
    ]
    scratch += [dma((n,))] * 10
    scratch += [dma((outer,))] * 8
    scratch += [dma((4, outer))] * 3 + [dma((outer, inner))] * 4
    scratch += [dma, dma]
    scratch += [dma((outer,))] * 4
    scratch += [dma((inner,))] * 2
    outs = pl.pallas_call(
        functools.partial(fused, (n, outer, cap)),
        out_shape=(
            wide((2, half, units), bf16), wide((2, half, units), bf16), wide((units, width), bf16),
            wide((dcols, channels), f32), wide((tokens, channels), bf16),
            wide((tokens, channels), bf16), wide((tokens, groups * STATE), bf16),
            wide((tokens, groups * STATE), bf16), wide((heads, tokens), f32),
        ),
        in_specs=[vspec] * 4 + [aspec] * 13,
        out_specs=(aspec,) * 8 + (vspec,),
        scratch_shapes=scratch,
        compiler_params=pltpu.CompilerParams(
            collective_id=0, has_side_effects=True, vmem_limit_bytes=64 * 1024 * 1024 - 128 * 1024
        ),
        name="fused",
    )(
        expert_choice.T, route_weight.T, log_decay.T,
        norm_gain.reshape(channels // 128, 128), scan_in, gate_in, b_proj, c_proj,
        entry_state.reshape(state_rows, STATE),
        layer_cotangent, mixer_output, gate_pre[0], up_pre[0],
        w_gate.reshape(2, half, units), w_up.reshape(2, half, units), w_down[0], w_out,
    )
    gwg, gwu, gwd, proj, gscan, ggate, gb, gc, gdecay = hand_over(outs)
    return (
        gwg.reshape(1, width, units), gwu.reshape(1, width, units), gwd[None],
        proj, gscan, ggate, gb, gc, gdecay.T,
    )


def entry_slots(expert_choice, expert_count, capacity):
    tokens, top_count = expert_choice.shape
    targets = expert_choice.reshape(-1)
    experts = jnp.arange(expert_count, dtype=jnp.int32)
    one_hot = (targets[:, None] == experts[None, :]).astype(jnp.float32)
    entries = jnp.arange(tokens * top_count, dtype=jnp.int32)
    before = (entries[:, None] > entries[None, :]).astype(jnp.bfloat16)
    earlier = jnp.dot(before, one_hot.astype(jnp.bfloat16), preferred_element_type=jnp.float32)
    ranks = jnp.sum(earlier * one_hot, axis=1).astype(jnp.int32)
    return (targets * capacity + ranks).reshape(tokens, top_count)


def expert_side(grad_rows, gate_value, up_value, gate_weight, up_weight, down_weight):
    act_grad = jnp.einsum("rd,fd->rf", grad_rows, down_weight, preferred_element_type=jnp.float32)
    gate_full = gate_value.astype(jnp.float32)
    up_full = up_value.astype(jnp.float32)
    gate_clip = jnp.minimum(gate_full, clamp_limit)
    up_clip = jnp.clip(up_full, -clamp_limit, clamp_limit)
    sigmoid_gate = jax.nn.sigmoid(swish_alpha * gate_clip)
    swish_gate = gate_clip * sigmoid_gate
    active = ((up_clip + 1.0) * swish_gate).astype(jnp.bfloat16)
    up_grad = jnp.where(
        (up_full > -clamp_limit) & (up_full < clamp_limit), act_grad * swish_gate, 0.0
    ).astype(jnp.bfloat16)
    slope = sigmoid_gate + swish_alpha * gate_clip * sigmoid_gate * (1.0 - sigmoid_gate)
    gate_grad = jnp.where(gate_full < clamp_limit, act_grad * (up_clip + 1.0) * slope, 0.0).astype(
        jnp.bfloat16
    )
    partial_rows = jnp.einsum(
        "rf,df->rd", gate_grad, gate_weight, preferred_element_type=jnp.float32
    )
    partial_rows = partial_rows + jnp.einsum(
        "rf,df->rd", up_grad, up_weight, preferred_element_type=jnp.float32
    )
    return (active, gate_grad, up_grad, partial_rows)


def exchange(pieces):
    return lax.all_to_all(pieces, "sp", split_axis=0, concat_axis=0, tiled=True)


def tell_all(vector):
    return exchange(jnp.broadcast_to(vector, (lax.axis_size("sp"), *vector.shape)))


def later_states(block_state, totals):
    count = lax.axis_size("sp")
    heads, channels, width = block_state.shape
    rows = heads * channels // count
    spots = jnp.arange(count)
    between = (
        (spots[:, None, None] < spots[None, None, :]) & (spots[None, None, :] < spots[None, :, None])
    ).astype(jnp.float32)
    gaps = jnp.einsum("bck,kh->bch", between, totals, precision=lax.Precision.HIGHEST)
    later = spots[:, None, None] < spots[None, :, None]
    weights = jnp.where(later, jnp.exp(gaps), 0.0)
    first = lax.axis_index("sp") * rows
    picks = (
        ((first + jnp.arange(rows)) // channels)[None, :] == jnp.arange(heads)[:, None]
    ).astype(jnp.float32)
    weights = jnp.einsum("bch,hr->bcr", weights, picks, precision=lax.Precision.HIGHEST)
    dealt = lax.all_to_all(
        block_state.astype(jnp.bfloat16).reshape(count, rows, width),
        "sp",
        split_axis=0,
        concat_axis=0,
        tiled=True,
    ).astype(jnp.float32)
    sums = jnp.sum(weights[:, :, :, None] * dealt[None], axis=1)
    back = lax.all_to_all(
        sums.astype(jnp.bfloat16), "sp", split_axis=0, concat_axis=0, tiled=True
    )
    return back.reshape(heads, channels, width)


def body(
    mixer_output,
    layer_cotangent,
    expert_choice,
    route_weight,
    gate_pre,
    up_pre,
    w_gate,
    w_up,
    w_down,
    w_out,
    norm_gain,
    scan_in,
    gate_in,
    b_proj,
    c_proj,
    log_decay,
    entry_state,
):
    expert_count = lax.axis_size("sp")
    tokens_here = mixer_output.shape[0]
    model_width = mixer_output.shape[1]
    top_count = expert_choice.shape[1]
    capacity = gate_pre.shape[1] // expert_count
    columns = model_width // lax.axis_size("tp")
    first_column = lax.axis_index("tp") * columns
    own_cotangent = lax.dynamic_slice_in_dim(layer_cotangent, first_column, columns, 1).astype(
        jnp.float32
    )
    own_hidden = lax.dynamic_slice_in_dim(mixer_output, first_column, columns, 1)
    slots = entry_slots(expert_choice, expert_count, capacity)
    slot_ids = jnp.arange(expert_count * capacity, dtype=jnp.int32)
    places = (slots.T[:, None, :] == slot_ids[None, :, None]).astype(jnp.bfloat16)
    token_places = places.sum(axis=0)
    weighted = (route_weight.T[:, :, None] * own_cotangent[None]).astype(jnp.bfloat16)

    def dispatch(rows):
        arrived = lax.all_to_all(
            rows.astype(jnp.bfloat16).reshape(expert_count, capacity, columns),
            "sp",
            split_axis=0,
            concat_axis=0,
            tiled=True,
        ).reshape(-1, columns)
        return lax.all_gather(arrived, "tp", axis=1, tiled=True)

    recv_grads = dispatch(
        jnp.einsum("kst,ktd->sd", places, weighted, preferred_element_type=jnp.float32)
    )
    active, gate_grad, up_grad, partial_rows = expert_side(
        recv_grads,
        gate_pre[0],
        up_pre[0],
        w_gate[0],
        w_up[0],
        w_down[0],
    )
    summed = lax.psum_scatter(
        partial_rows.astype(jnp.bfloat16), "tp", scatter_dimension=1, tiled=True
    )
    returned = lax.all_to_all(
        summed.reshape(expert_count, capacity, -1), "sp", split_axis=0, concat_axis=0, tiled=True
    )
    head_count = log_decay.shape[1]
    group_count = b_proj.shape[1] // STATE
    per_group = head_count // group_count
    scan_heads = scan_in.reshape(tokens_here, head_count, HEAD_DIM)
    b_groups = b_proj.reshape(tokens_here, group_count, STATE)
    c_groups = c_proj.reshape(tokens_here, group_count, STATE)
    x_float = scan_heads.astype(jnp.float32)
    token_locations = jnp.arange(tokens_here)
    causal = token_locations[:, None] >= token_locations[None, :]
    causal_float = causal.astype(jnp.float32)
    cumulative = jnp.dot(causal_float, log_decay, precision=lax.Precision.HIGHEST)
    growth = jnp.exp(cumulative)
    block_decays = tell_all(lax.optimization_barrier((cumulative[-1], summed))[0])
    tail_decay = jnp.exp(cumulative[-1][None, :] - cumulative)
    log_gaps = cumulative.T[:, :, None] - cumulative.T[:, None, :]
    decay_mat = jnp.exp(jnp.where(causal[None], log_gaps, -jnp.inf))
    inner_prod = jnp.einsum("tgn,sgn->gts", c_groups, b_groups, preferred_element_type=jnp.float32)
    mix_weights = (jnp.repeat(inner_prod, per_group, axis=0) * decay_mat).astype(jnp.bfloat16)
    state_groups = entry_state.astype(jnp.bfloat16).reshape(group_count, per_group, HEAD_DIM, STATE)
    y_inner = jnp.einsum(
        "hts,shp->thp", mix_weights, scan_heads, preferred_element_type=jnp.float32
    )
    y_carry = jnp.einsum(
        "tgn,grpn->tgrp", c_groups, state_groups, preferred_element_type=jnp.float32
    ).reshape(tokens_here, head_count, HEAD_DIM)
    scan_out = y_inner + y_carry * growth[:, :, None]
    gate_float = gate_in.astype(jnp.float32)
    gate_sig = jax.nn.sigmoid(gate_float)
    gate_silu = gate_float * gate_sig
    gated = scan_out.reshape(tokens_here, -1) * gate_silu
    grouped = gated.reshape(tokens_here, group_count, -1)
    inv_rms = lax.rsqrt(jnp.mean(grouped * grouped, axis=-1, keepdims=True) + rms_epsilon)
    unit = grouped * inv_rms
    gain_groups = norm_gain.astype(jnp.float32).reshape(group_count, -1)
    mixed = (unit * gain_groups).reshape(tokens_here, -1).astype(jnp.bfloat16)
    all_mixed = lax.all_gather(mixed, "sp", axis=0, tiled=True)
    returned, mixed = lax.optimization_barrier((returned, mixed))
    moe_terms = jnp.einsum(
        "st,sd->td",
        token_places,
        returned.reshape(-1, columns),
        preferred_element_type=jnp.float32,
    )
    grad_hidden = lax.all_gather(
        (own_cotangent + moe_terms).astype(jnp.bfloat16), "tp", axis=1, tiled=True
    )
    late_hidden, grad_hidden = lax.optimization_barrier((own_hidden, grad_hidden))
    recv_hidden = dispatch(
        jnp.einsum("st,td->sd", token_places, late_hidden, preferred_element_type=jnp.float32)
    )
    down_wgrad = jnp.einsum(
        "rf,rd->fd", active, recv_grads, preferred_element_type=jnp.float32
    ).astype(jnp.bfloat16)
    gate_wgrad = jnp.einsum(
        "rd,rf->df", recv_hidden, gate_grad, preferred_element_type=jnp.float32
    ).astype(jnp.bfloat16)
    up_wgrad = jnp.einsum(
        "rd,rf->df", recv_hidden, up_grad, preferred_element_type=jnp.float32
    ).astype(jnp.bfloat16)
    own_block = lax.all_to_all(
        grad_hidden.reshape(tokens_here, expert_count, -1).transpose(1, 0, 2),
        "sp",
        split_axis=0,
        concat_axis=0,
        tiled=True,
    )
    grad_out_proj = jnp.einsum(
        "td,ti->di",
        own_block.reshape(-1, own_block.shape[2]),
        all_mixed,
        preferred_element_type=jnp.float32,
    )
    grad_mixed = jnp.einsum("td,id->ti", grad_hidden, w_out, preferred_element_type=jnp.float32)
    grad_unit = grad_mixed.reshape(tokens_here, group_count, -1) * gain_groups
    grad_grouped = inv_rms * (grad_unit - unit * jnp.mean(grad_unit * unit, axis=-1, keepdims=True))
    grad_gated = grad_grouped.reshape(tokens_here, -1)
    grad_gate_in = (
        grad_gated
        * scan_out.reshape(tokens_here, -1)
        * gate_sig
        * (1.0 + gate_float * (1.0 - gate_sig))
    ).astype(jnp.bfloat16)
    grad_y = (grad_gated * gate_silu).reshape(tokens_here, head_count, HEAD_DIM)
    grad_y_b = grad_y.astype(jnp.bfloat16)
    grad_x_inner = jnp.einsum(
        "hts,thp->shp", mix_weights, grad_y_b, preferred_element_type=jnp.float32
    )
    grad_weights = (
        jnp.einsum("thp,shp->hts", grad_y_b, scan_heads, preferred_element_type=jnp.float32)
        * decay_mat
    )
    grad_weights = (
        grad_weights.reshape(group_count, per_group, tokens_here, tokens_here)
        .sum(axis=1)
        .astype(jnp.bfloat16)
    )
    grad_c_inner = jnp.einsum(
        "gts,sgn->tgn", grad_weights, b_groups, preferred_element_type=jnp.float32
    )
    grad_b_inner = jnp.einsum(
        "gts,tgn->sgn", grad_weights, c_groups, preferred_element_type=jnp.float32
    )
    grown_grads = (grad_y * growth[:, :, None]).astype(jnp.bfloat16).reshape(
        tokens_here, group_count, per_group, HEAD_DIM
    )
    grad_c_carry = jnp.einsum(
        "tgrp,grpn->tgn", grown_grads, state_groups, preferred_element_type=jnp.float32
    )
    block_state = jnp.einsum(
        "tgrp,tgn->grpn", grown_grads, c_groups, preferred_element_type=jnp.float32
    ).reshape(head_count, HEAD_DIM, STATE)
    x_tail = (x_float * tail_decay[:, :, None]).astype(jnp.bfloat16).reshape(
        tokens_here, group_count, per_group, HEAD_DIM
    )
    later_state = later_states(block_state, block_decays)
    later_groups = later_state.reshape(group_count, per_group, HEAD_DIM, STATE)
    grad_x_carry = jnp.einsum(
        "sgn,grpn->sgrp", b_groups, later_groups, preferred_element_type=jnp.float32
    ).reshape(tokens_here, head_count, HEAD_DIM)
    grad_x = grad_x_inner + grad_x_carry * tail_decay[:, :, None]
    grad_b_carry = jnp.einsum(
        "sgrp,grpn->sgn", x_tail, later_groups, preferred_element_type=jnp.float32
    )
    grad_a = jnp.sum(grad_y * scan_out, axis=2) - jnp.sum(x_float * grad_x, axis=2)
    block_totals = tell_all(jnp.sum(grad_a, axis=0))
    is_later = jnp.arange(expert_count) > lax.axis_index("sp")
    later_grad = jnp.sum(jnp.where(is_later[:, None], block_totals, 0.0), axis=0)
    grad_log_decay = (
        jnp.dot(causal_float.T, grad_a, precision=lax.Precision.HIGHEST) + later_grad[None, :]
    )
    grad_scan_in = grad_x.reshape(tokens_here, -1).astype(jnp.bfloat16)
    grad_b_proj = (grad_b_inner + grad_b_carry).reshape(tokens_here, -1).astype(jnp.bfloat16)
    grad_c_proj = (grad_c_inner + grad_c_carry).reshape(tokens_here, -1).astype(jnp.bfloat16)
    return (
        gate_wgrad[None],
        up_wgrad[None],
        down_wgrad[None],
        grad_out_proj,
        grad_scan_in,
        grad_gate_in,
        grad_b_proj,
        grad_c_proj,
        grad_log_decay,
    )


def solution(mesh):
    in_specs = (
        P("sp", None),
        P("sp", None),
        P("sp", None),
        P("sp", None),
        P("sp", None, "tp"),
        P("sp", None, "tp"),
        P("sp", None, "tp"),
        P("sp", None, "tp"),
        P("sp", "tp", None),
        P("tp", None),
        P("tp"),
        P("sp", "tp"),
        P("sp", "tp"),
        P("sp", "tp"),
        P("sp", "tp"),
        P("sp", "tp"),
        P("sp", "tp", None, None),
    )
    out_specs = (
        P("sp", None, "tp"),
        P("sp", None, "tp"),
        P("sp", "tp", None),
        P("sp", "tp"),
        P("sp", "tp"),
        P("sp", "tp"),
        P("sp", "tp"),
        P("sp", "tp"),
        P("sp", "tp"),
    )
    def run(*args):
        count = mesh.shape["sp"]
        capacity = args[4].shape[1] // count
        simple = mesh.shape["tp"] != 2 or count % 4 or count & (count - 1) or capacity % 16
        return (body if simple else fused_body)(*args)

    return jax.shard_map(run, mesh=mesh, in_specs=in_specs, out_specs=out_specs, check_vma=False)
```

```python
import functools

import jax
import jax.numpy as jnp
from jax import lax
from jax.sharding import PartitionSpec as P

from jax.experimental import pallas as pl
from jax.experimental.pallas import tpu as pltpu

HEAD_DIM = 64
STATE = 128


rms_epsilon = 1e-05
clamp_limit = 7.0
swish_alpha = 1.702


MESH = pl.DeviceIdType.MESH
f32, bf16 = jnp.float32, jnp.bfloat16


def dot_nn(a, b):
    return jnp.dot(a, b, preferred_element_type=f32)


def dot_nt(a, b):
    return lax.dot_general(a, b, (((1,), (1,)), ((), ())), preferred_element_type=f32)


def dot_tn(a, b):
    return lax.dot_general(a, b, (((0,), (0,)), ((), ())), preferred_element_type=f32)


def dot_full(a, b):
    return jnp.dot(a, b, precision=lax.Precision.HIGHEST, preferred_element_type=f32)


def xor(value, bits):
    bit = 1
    while bit <= bits:
        if bits & bit:
            value = value + bit * (1 - 2 * ((value // bit) % 2))
        bit *= 2
    return value


def iota(shape, dim):
    return lax.broadcasted_iota(jnp.int32, shape, dim)


def aligned(value, unit):
    return pl.multiple_of(value, unit)


PLAN = {'sent': (), ('chunk', 0): (), ('chunk', 1): ('cot2', 'hid0'), ('chunk', 2): ('cot3', 'hid1'), ('chunk', 3): (), 'forward': ('cot1',), 'experts': ('hid2', 'mz0'), 'down': ('hid3', 'mz1'), 'combined': (), 'states': ('mz2',), 'inner': ('mz3',), 'later': ('proj',), 'final': ()}


def fused(
    dims,
    choice_t, weight_t, decay_t, gain, scan_hbm, gate_hbm, b_hbm, c_hbm, entry_hbm,
    cot_hbm, hid_hbm, gpre_hbm, upre_hbm, wg_hbm, wu_hbm, wd_hbm, wo_hbm,
    owg, owu, owd, proj_hbm, oscan_hbm, ogate_hbm, ob_hbm, oc_hbm, odecay,
    scan_x, gate_x, b_in, c_in, entry, oproj, oscan, ogate, ob, oc,
    cot_z, hid_z, gpre, upre, wg, wu, wd, wo,
    send_g, send_h, g_full, h_full, part_send, part_recv, ret_send, ret_recv,
    active, gate_grad, up_grad, places_t,
    mixed_z, hidden, hidden_z, rs_send, rs_recv,
    scan_out, unit, inv_rms, gy, mix_t, decays, growth_s, tail_s, entry_b, block_state,
    st_send, st_recv, rv_send, rv_recv, tot_send, tot_recv, slot_recv, gat_send, gat_recv,
    grad_wg, grad_wu, grad_wd,
    in_sem, out_sem, ret_s, ret_r, st_s, st_r, rv_s, rv_r,
    tot_s, tot_r, gat_s, gat_r, fg_s, fg_r, fh_s, fh_r, px_s, px_r, sl_s, sl_r, mz_line, hid_line, cot_line, h_s, h_r, g_s, g_r,
    gh_s, gh_r, hz_s, hz_r, fz_s, fz_r, rs_s, rs_r,
):
    n, outer, cap = dims
    inner = n // outer
    tokens, half = cot_z.shape[1:]
    rows = n * cap
    zrows = inner * cap
    heads = decay_t.shape[0]
    groups = b_in.shape[1] // STATE
    pairs_in_group = heads // groups // 2
    gwidth = pairs_in_group * 128
    per_half = outer // 2
    dchunk = hidden.shape[2]
    srows = st_send.shape[0] // n
    dcols = dchunk // inner
    thalf = tokens // 2
    me = lax.axis_index("sp")
    tp = lax.axis_index("tp")
    other = 1 - tp
    my_z = me // inner
    my_q = me % inner
    peers = [xor(me, k) for k in range(n)]

    def remote(src, dst, s, r, sp_id, tp_id):
        return pltpu.make_async_remote_copy(
            src_ref=src, dst_ref=dst, send_sem=s, recv_sem=r,
            device_id=(sp_id, tp_id), device_id_type=MESH,
        )

    def rowblock(block, size):
        return pl.ds(aligned(block * size, size), size)

    barrier = pltpu.get_barrier_semaphore()
    for k in range(1, n):
        pl.semaphore_signal(barrier, inc=1, device_id=(peers[k], tp), device_id_type=MESH)
    pl.semaphore_signal(barrier, inc=1, device_id=(me, other), device_id_type=MESH)

    own_cols = pl.ds(aligned(tp * half, half), half)
    loads = [
        pltpu.make_async_copy(cot_hbm.at[:, own_cols], cot_z.at[my_z], in_sem.at[0]),
        pltpu.make_async_copy(hid_hbm.at[:, own_cols], hid_z.at[my_z], in_sem.at[1]),
        pltpu.make_async_copy(wd_hbm, wd, in_sem.at[2]),
        pltpu.make_async_copy(gpre_hbm, gpre, in_sem.at[3]),
        pltpu.make_async_copy(upre_hbm, upre, in_sem.at[4]),
        pltpu.make_async_copy(wg_hbm, wg, in_sem.at[5]),
        pltpu.make_async_copy(wu_hbm, wu, in_sem.at[6]),
        pltpu.make_async_copy(wo_hbm, wo, in_sem.at[7]),
    ]
    pairs_of_refs = (
        (b_hbm, b_in), (c_hbm, c_in), (scan_hbm, scan_x), (entry_hbm, entry), (gate_hbm, gate_x),
    )
    mixer_loads = [
        pltpu.make_async_copy(src, dst, in_sem.at[8 + i])
        for i, (src, dst) in enumerate(pairs_of_refs)
    ]
    stores = []

    def store(src, dst):
        copy = pltpu.make_async_copy(src, dst, out_sem.at[len(stores)])
        copy.start()
        stores.append(copy)

    for load in loads[:2] + mixer_loads + loads[2:]:
        load.start()

    expert_s = iota((n, tokens), 0)
    first_t = choice_t[0:1, :] == expert_s
    second_t = choice_t[1:2, :] == expert_s
    row_id = iota((tokens, tokens), 0)
    col_id = iota((tokens, tokens), 1)
    named_t = jnp.where(first_t | second_t, 1.0, 0.0).astype(bf16)
    before_t = jnp.where(row_id < col_id, 1.0, 0.0).astype(bf16)
    base_t = dot_nn(named_t, before_t) + (cap * expert_s).astype(f32)
    slot0_t = jnp.sum(jnp.where(first_t, base_t, 0.0), axis=0, keepdims=True)
    slot1_t = jnp.sum(jnp.where(second_t, base_t, 0.0), axis=0, keepdims=True)

    def column(row):
        return jnp.sum(jnp.where(row_id == col_id, row, 0.0), axis=1, keepdims=True)

    slot0, slot1 = column(slot0_t), column(slot1_t)
    slot_l = iota((tokens, rows), 1).astype(f32)
    places_t[...] = jnp.where((slot_l == slot0) | (slot_l == slot1), 1.0, 0.0).astype(bf16)

    slot_recv[my_z] = jnp.zeros(slot_recv.shape[1:], f32)
    slot_recv[my_z, 0:1, :] = slot0_t
    slot_recv[my_z, 1:2, :] = slot1_t
    slot_recv[my_z, 2:4, :] = weight_t[...]
    loads[0].wait()
    pl.semaphore_wait(barrier, n)

    def line(buf, sems):
        def up(s):
            block = (my_z - s + outer) % outer
            return remote(
                buf.at[block], buf.at[block], sems.at[0, s], sems.at[1, s], (me + inner) % n, tp
            )

        def down(s):
            block = (my_z + s) % outer
            return remote(
                buf.at[block], buf.at[block], sems.at[2, s], sems.at[3, s],
                (me - inner + n) % n, tp,
            )

        def send(s, drain=False):
            @pl.when((my_z >= s) & (my_z < outer - 1))
            def _():
                up(s).wait_send() if drain else up(s).start()

            @pl.when((my_z + s < outer) & (my_z > 0))
            def _():
                down(s).wait_send() if drain else down(s).start()

        def take(s):
            @pl.when(my_z > s)
            def _():
                up(s).wait_recv()

            @pl.when(my_z + s + 1 < outer)
            def _():
                down(s).wait_recv()

        return send, take

    send_hid, take_hid = line(hid_z, hid_line)
    send_mz, take_mz = line(mixed_z, mz_line)
    send_cot, take_cot = line(cot_z, cot_line)

    def at(point):
        for step in PLAN[point]:
            steps[step]()

    def all_to_all(send, recv, size, s, r):
        mine = rowblock(me, size)
        return [None] + [
            remote(send.at[rowblock(peers[k], size)], recv.at[mine], s.at[k], r.at[k], peers[k], tp)
            for k in range(1, n)
        ]

    own_rows = rowblock(me, cap)
    copy_st = all_to_all(st_send, st_recv, srows, st_s, st_r)
    copy_rv = all_to_all(rv_send, rv_recv, srows, rv_s, rv_r)
    far_first = list(range(n - 1, 0, -1))
    copy_sl = [None] + [
        remote(
            slot_recv.at[my_z], slot_recv.at[my_z], sl_s.at[j], sl_r.at[j],
            xor(my_z, j) * inner + my_q, tp,
        )
        for j in range(1, outer)
    ]
    send_cot(0)
    for j in range(1, outer):
        copy_sl[j].start()

    copy_rs = [None]

    def output_projection():
        for j in range(1, outer):
            copy_hz[j].wait_recv()
            fwd_z[j].start()
        for j in range(1, outer):
            fwd_z[j].wait_recv()
        for q in range(inner - 1, -1, -1):
            target = xor(my_q, q)
            dpart = pl.ds(aligned(target * dcols, dcols), dcols)
            for s in range(half // 512):
                cols = slice(s * 512, (s + 1) * 512)
                total = dot_tn(hidden_z[0, :, dpart], mixed_z[0, :, cols])
                for z in range(1, outer):
                    total = total + dot_tn(hidden_z[z, :, dpart], mixed_z[z, :, cols])
                if q:
                    rs_send[q, :, cols] = total.astype(bf16)
                else:
                    oproj[:, cols] = total
            if q:
                copy = remote(
                    rs_send.at[q], rs_recv.at[q], rs_s.at[q], rs_r.at[q], my_z * inner + target, tp
                )
                copy.start()
                copy_rs.append(copy)

    def plane_dest(b):
        return pl.ds(aligned((b * inner + my_q) * cap, cap), cap)

    def plane_copy(send, full, sems, b, q):
        target = xor(my_q, q)
        return remote(
            send.at[b, rowblock(target, cap)], full.at[tp, plane_dest(b)],
            sems[0].at[b, q], sems[1].at[b, q], my_z * inner + target, tp,
        )

    def hidden_copy(b, q):
        return plane_copy(send_h, h_full, (h_s, h_r), b, q)

    def cot_copy(b, q):
        return plane_copy(send_g, g_full, (g_s, g_r), b, q)

    def deal(b, source, send, full, copy, weighted):
        slot_h = (iota((zrows, tokens), 0) + my_z * zrows).astype(f32)
        in_first = slot_h == slot_recv[b, 0:1, :]
        in_second = slot_h == slot_recv[b, 1:2, :]
        places = jnp.where(in_first | in_second, 1.0, 0.0).astype(bf16)
        rows_b = dot_nn(places, source[b])
        if weighted:
            rows_b = rows_b * jnp.sum(
                jnp.where(in_first, slot_recv[b, 2:3, :], 0.0)
                + jnp.where(in_second, slot_recv[b, 3:4, :], 0.0),
                axis=1, keepdims=True,
            )
        send[b] = rows_b.astype(bf16)
        for q in range(inner - 1, 0, -1):
            copy(b, q).start()
        full[tp, plane_dest(b), :] = send[b, rowblock(my_q, cap), :]

    def hidden_block(b):
        deal(b, hid_z, send_h, h_full, hidden_copy, False)

    def cot_block(b):
        deal(b, cot_z, send_g, g_full, cot_copy, True)

    def at_distance(distance, action):
        @pl.when(my_z >= distance)
        def _():
            action((my_z - distance + outer) % outer)

        @pl.when(my_z + distance < outer)
        def _():
            action((my_z + distance) % outer)

    def cot_next(s):
        if s == 1:
            for j in range(1, outer):
                copy_sl[j].wait_recv()
        take_cot(s - 1)
        if s < outer - 1:
            send_cot(s)
        at_distance(s, cot_block)

    def hidden_own():
        loads[1].wait()
        send_hid(0)
        hidden_block(my_z)

    def hidden_send():
        loads[1].wait()
        send_hid(0)

    def hidden_next(s):
        take_hid(s - 1)
        if s < outer - 1:
            send_hid(s)
        at_distance(s, hidden_block)

    forwarded = []

    def forward_hidden(j):
        for q in range(1, inner):
            hidden_copy(xor(my_z, j), q).wait_recv()
        fwd_h[j].start()
        forwarded.append(j)

    def pass_on(send, take, s):
        take(s - 1)
        send(s)

    steps = {
        "cot1": lambda: cot_next(1),
        "cot2": lambda: cot_next(2),
        "cot3": lambda: cot_next(3),
        "hid0": hidden_own,
        "hid0s": hidden_send,
        "hid0b": lambda: hidden_block(my_z),
        "hid1": lambda: hidden_next(1),
        "hid2": lambda: hidden_next(2),
        "hid3": lambda: hidden_next(3),
        "mz0": lambda: send_mz(0),
        "mz1": lambda: pass_on(send_mz, take_mz, 1),
        "mz2": lambda: pass_on(send_mz, take_mz, 2),
        "mz3": lambda: take_mz(outer - 2),
        "proj": output_projection,
        "fwd0": lambda: forward_hidden(0),
        "fwd1": lambda: forward_hidden(1),
        "fwd2": lambda: forward_hidden(2),
    }

    cot_block(my_z)

    causal = row_id >= col_id
    causal_f = jnp.where(causal, 1.0, 0.0)
    anti_f = jnp.where(row_id <= col_id, 1.0, 0.0)
    cum_t = dot_full(decay_t[...], anti_f)
    cum = cum_t.T
    growth_s[...] = jnp.exp(cum)
    tail_s[...] = jnp.exp(cum[tokens - 1:tokens, :] - cum)
    tot_send[...] = jnp.zeros(tot_send.shape, f32)
    tot_send[0:1, 0:heads] = cum[tokens - 1:tokens, :]
    tot_recv[me] = tot_send[...]
    copy_tot = [None] + [
        remote(tot_send, tot_recv.at[me], tot_s.at[k], tot_r.at[k], peers[k], tp)
        for k in range(1, n)
    ]
    for k in far_first:
        copy_tot[k].start()
    at("sent")
    lane = iota((1, 128), 1)
    low_lane = lane < HEAD_DIM
    low = jnp.where(low_lane, 1.0, 0.0)
    low_b, high_b = low.astype(bf16), (1.0 - low).astype(bf16)

    def spread(columns, pair):
        return jnp.where(
            low_lane, columns[:, 2 * pair:2 * pair + 1], columns[:, 2 * pair + 1:2 * pair + 2]
        )

    def tile(index):
        return slice(index * 128, (index + 1) * 128)

    def gain_row(index):
        return gain[index:index + 1, :].astype(f32)

    def group_cols(g):
        return slice(g * gwidth, (g + 1) * gwidth)

    for load in mixer_loads:
        load.wait()
    entry_b[...] = entry[...].astype(bf16)
    for g in range(groups):
        b_g, c_g = b_in[:, tile(g)], c_in[:, tile(g)]
        inner_prod = dot_nt(c_g, b_g)
        inner_t = dot_nt(b_g, c_g)
        squares = jnp.zeros((tokens, 1), f32)
        gated = []
        for pair in range(g * pairs_in_group, (g + 1) * pairs_in_group):
            mats = []
            for h in (2 * pair, 2 * pair + 1):
                gap = cum[:, h:h + 1] - cum_t[h:h + 1, :]
                fade = jnp.exp(jnp.where(causal, gap, -jnp.inf))
                decays[h] = fade
                mats.append((inner_prod * fade).astype(bf16))
                gap_t = cum_t[h:h + 1, :] - cum[:, h:h + 1]
                mix_t[pair, :, tile(h % 2)] = (
                    inner_t * jnp.exp(jnp.where(row_id <= col_id, gap_t, -jnp.inf))
                ).astype(bf16)
            x = scan_x[:, tile(pair)]
            y = dot_nn(mats[0], x * low_b) + dot_nn(mats[1], x * high_b)
            carry = dot_nt(c_g, entry_b[tile(pair), :])
            out = y + carry * spread(growth_s, pair)
            scan_out[:, tile(pair)] = out
            gate = gate_x[:, tile(pair)].astype(f32)
            value = out * (gate * jax.nn.sigmoid(gate))
            squares = squares + jnp.sum(value * value, axis=1, keepdims=True)
            gated.append(value)
        inv = lax.rsqrt(squares * (1.0 / gwidth) + rms_epsilon)
        inv_rms[g] = inv
        for i, value in enumerate(gated):
            cols = tile(g * pairs_in_group + i)
            flat = value * inv
            unit[:, cols] = flat
            mixed_z[my_z, :, cols] = (flat * gain_row(g * pairs_in_group + i)).astype(bf16)

    at("forward")

    for i in range(2, 7):
        loads[i].wait()
    upper = my_z // per_half
    near = upper * (outer - 1 - my_z) + (1 - upper) * my_z

    def in_turn(position):
        block = near * (1 - position) + (1 - near) * position if position < 2 else position
        return upper * (outer - 1 - block) + (1 - upper) * block

    def return_copy(peer, sem):
        return remote(
            ret_send.at[rowblock(peer, cap)], ret_recv.at[own_rows],
            ret_s.at[peer], ret_r.at[sem], peer, tp,
        )

    fwd_g, fwd_h, px = [], [], []
    for j in range(outer):
        zpart = rowblock(in_turn(j), zrows)
        fwd_g.append(
            remote(g_full.at[tp, zpart], g_full.at[tp, zpart], fg_s.at[j], fg_r.at[j], me, other)
        )
        zpart = rowblock(xor(my_z, j), zrows)
        fwd_h.append(
            remote(h_full.at[tp, zpart], h_full.at[tp, zpart], fh_s.at[j], fh_r.at[j], me, other)
        )
        px.append(remote(part_send.at[j], part_recv.at[j], px_s.at[j], px_r.at[j], me, other))
    for j in range(outer):
        at(("chunk", j))
        block = in_turn(j)
        zpart = rowblock(block, zrows)
        for q in range(1, inner):
            cot_copy(block, q).wait_recv()
        fwd_g[j].start()
        fwd_g[j].wait_recv()
        act = dot_nt(g_full[0, zpart, :], wd[:, 0:half])
        act = act + dot_nt(g_full[1, zpart, :], wd[:, half:2 * half])
        gate_full = gpre[zpart, :].astype(f32)
        up_full = upre[zpart, :].astype(f32)
        gate_clip = jnp.minimum(gate_full, clamp_limit)
        up_clip = jnp.clip(up_full, -clamp_limit, clamp_limit)
        sig = jax.nn.sigmoid(swish_alpha * gate_clip)
        swish = gate_clip * sig
        active[zpart, :] = ((up_clip + 1.0) * swish).astype(bf16)
        inside = (up_full > -clamp_limit) & (up_full < clamp_limit)
        ug = jnp.where(inside, act * swish, 0.0).astype(bf16)
        slope = sig + swish_alpha * gate_clip * sig * (1.0 - sig)
        gg = jnp.where(gate_full < clamp_limit, act * (up_clip + 1.0) * slope, 0.0).astype(bf16)
        up_grad[zpart, :] = ug
        gate_grad[zpart, :] = gg
        part_send[j] = (dot_nt(gg, wg[other]) + dot_nt(ug, wu[other])).astype(bf16)
        px[j].start()
        own = (dot_nt(gg, wg[tp]) + dot_nt(ug, wu[tp])).astype(bf16)
        px[j].wait_recv()
        ret_send[zpart, :] = (own.astype(f32) + part_recv[j].astype(f32)).astype(bf16)
        if j == 0:
            ret_recv[own_rows, :] = ret_send[own_rows, :]
        for q in range(inner - 1, -1, -1):
            if j or q:
                return_copy(block * inner + xor(my_q, q), me).start()

    at("experts")

    def down_step(i, carry):
        cols = pl.ds(aligned(i * 256, 256), 256)
        for s in range(2):
            grad_wd[s, :, cols] = dot_tn(active[...], g_full[s, :, cols]).astype(bf16)
        return carry

    lax.fori_loop(0, half // 256, down_step, 0)
    store(grad_wd.at[0], owd.at[:, 0:half])
    store(grad_wd.at[1], owd.at[:, half:2 * half])

    at("down")
    for k in range(1, n):
        return_copy(peers[k], peers[k]).wait_recv()
    moe = dot_nn(places_t[...], ret_recv[...])
    for i in range(per_half):
        cols = slice(i * dchunk, (i + 1) * dchunk)
        hidden[tp * per_half + i] = (cot_z[my_z, :, cols].astype(f32) + moe[:, cols]).astype(bf16)
    own_chunks = pl.ds(tp * per_half, per_half)
    copy_gh = remote(hidden.at[own_chunks], hidden.at[own_chunks], gh_s, gh_r, me, other)
    copy_gh.start()
    loads[7].wait()
    copy_gh.wait_recv()
    hidden_z[my_z] = hidden[my_z]
    my_tokens = pl.ds(aligned(tp * thalf, thalf), thalf)
    copy_hz, fwd_z = [None], [None]
    for j in range(1, outer):
        z = xor(my_z, j)
        copy_hz.append(
            remote(
                hidden.at[z, my_tokens], hidden_z.at[my_z, my_tokens],
                hz_s.at[j], hz_r.at[j], z * inner + my_q, tp,
            )
        )
        fwd_z.append(
            remote(
                hidden_z.at[z, my_tokens], hidden_z.at[z, my_tokens],
                fz_s.at[j], fz_r.at[j], me, other,
            )
        )
    at("combined")

    for g in range(groups):
        c_g = c_in[:, tile(g)]
        gcols = group_cols(g)
        gm = dot_nt(hidden[0], wo[gcols, 0:dchunk])
        for i in range(1, outer):
            gm = gm + dot_nt(hidden[i], wo[gcols, i * dchunk:(i + 1) * dchunk])
        gu = jnp.concatenate(
            [
                gm[:, tile(i)] * gain_row(g * pairs_in_group + i)
                for i in range(pairs_in_group)
            ],
            axis=1,
        )
        flat = unit[:, gcols]
        mean = jnp.sum(gu * flat, axis=1, keepdims=True) * (1.0 / gwidth)
        gg = inv_rms[g] * (gu - flat * mean)
        gate = gate_x[:, gcols].astype(f32)
        sig = jax.nn.sigmoid(gate)
        ogate[:, gcols] = (
            gg * scan_out[:, gcols] * sig * (1.0 + gate * (1.0 - sig))
        ).astype(bf16)
        grad_y = gg * (gate * sig)
        gy[:, gcols] = grad_y
        for i in range(pairs_in_group):
            pair = g * pairs_in_group + i
            grown = (grad_y[:, tile(i)] * spread(growth_s, pair)).astype(bf16)
            st_send[tile(pair), :] = dot_tn(grown, c_g).astype(bf16)
    own_st = rowblock(me, srows)
    for k in far_first:
        copy_st[k].start()
    for j in range(outer - 1, 0, -1):
        copy_hz[j].start()
    st_recv[own_st, :] = st_send[own_st, :]
    at("states")
    store(ogate, ogate_hbm)

    for g in range(groups):
        b_g, c_g = b_in[:, tile(g)], c_in[:, tile(g)]
        gw = jnp.zeros((tokens, tokens), f32)
        gc = jnp.zeros((tokens, STATE), f32)
        for i in range(pairs_in_group):
            pair = g * pairs_in_group + i
            gy_t = gy[:, tile(pair)]
            gyb = gy_t.astype(bf16)
            x = scan_x[:, tile(pair)]
            gw = gw + dot_nt(gyb * low_b, x) * decays[2 * pair]
            gw = gw + dot_nt(gyb * high_b, x) * decays[2 * pair + 1]
            grown = (gy_t * spread(growth_s, pair)).astype(bf16)
            gc = gc + dot_nn(grown, entry_b[tile(pair), :])
        gwb = gw.astype(bf16)
        oc[:, tile(g)] = (gc + dot_nn(gwb, b_g)).astype(bf16)
        block_state[g] = dot_tn(gwb, c_g)

    store(oc, oc_hbm)
    at("inner")

    for k in range(1, n):
        copy_tot[k].wait_recv()
        copy_st[k].wait_recv()
    my_head = (me * srows) // HEAD_DIM
    rev = jnp.zeros((srows, STATE), f32)
    for b in range(n - 1, -1, -1):
        part = slice(b * srows, (b + 1) * srows)
        rv_send[part, :] = rev.astype(bf16)
        if b:
            total = jnp.sum(
                jnp.where(lane == my_head, tot_recv[b, 0:1, :], 0.0), axis=1, keepdims=True
            )
            rev = st_recv[part, :].astype(f32) + jnp.exp(total) * rev
    for k in far_first:
        copy_rv[k].start()
    rv_recv[own_st, :] = rv_send[own_st, :]
    at("later")

    for k in range(1, n):
        copy_rv[k].wait_recv()
    head_l = iota((1, heads), 1)
    grad_a = jnp.zeros((tokens, heads), f32)
    for g in range(groups):
        b_g = b_in[:, tile(g)]
        gb = block_state[g]
        for i in range(pairs_in_group):
            pair = g * pairs_in_group + i
            gy_t = gy[:, tile(pair)]
            gyb = gy_t.astype(bf16)
            x = scan_x[:, tile(pair)]
            xf = x.astype(f32)
            tail = spread(tail_s, pair)
            later = rv_recv[tile(pair), :]
            gx = dot_nn(mix_t[pair, :, 0:tokens], gyb * low_b)
            gx = gx + dot_nn(mix_t[pair, :, tokens:2 * tokens], gyb * high_b)
            gx = gx + dot_nt(b_g, later) * tail
            oscan[:, tile(pair)] = gx.astype(bf16)
            gb = gb + dot_nn((xf * tail).astype(bf16), later)
            diff = gy_t * scan_out[:, tile(pair)] - xf * gx
            sum_low = jnp.sum(jnp.where(low_lane, diff, 0.0), axis=1, keepdims=True)
            sum_high = jnp.sum(jnp.where(low_lane, 0.0, diff), axis=1, keepdims=True)
            grad_a = jnp.where(head_l == 2 * pair, sum_low, grad_a)
            grad_a = jnp.where(head_l == 2 * pair + 1, sum_high, grad_a)
        ob[:, tile(g)] = gb.astype(bf16)
    store(oscan, oscan_hbm)
    store(ob, ob_hbm)
    grad_t = grad_a.T
    gat_send[...] = jnp.broadcast_to(jnp.sum(grad_t, axis=1, keepdims=True), gat_send.shape)
    copy_gat = [None] + [
        remote(gat_send, gat_recv.at[me], gat_s.at[k], gat_r.at[k], peers[k], tp)
        for k in range(1, n)
    ]
    for k in far_first:
        copy_gat[k].start()
    gat_recv[me] = gat_send[...]

    at("final")
    for j in range(outer):
        if j not in forwarded:
            forward_hidden(j)
    for j in range(outer):
        fwd_h[j].wait_recv()

    def up_step(i, carry):
        cols = pl.ds(aligned(i * 256, 256), 256)
        for s in range(2):
            lhs = h_full[s, :, cols]
            grad_wg[s, cols, :] = dot_tn(lhs, gate_grad[...]).astype(bf16)
            grad_wu[s, cols, :] = dot_tn(lhs, up_grad[...]).astype(bf16)
        return carry

    lax.fori_loop(0, half // 256, up_step, 0)
    store(grad_wg, owg)
    store(grad_wu, owu)

    later_sum = dot_full(grad_t, causal_f)
    for k in range(1, n):
        copy_gat[k].wait_recv()
    for b in range(n):
        later_sum = later_sum + jnp.where(b > me, gat_recv[b, :, 0:1], 0.0)
    odecay[...] = later_sum

    for copy in copy_rs[1:]:
        copy.wait_recv()
    for q in range(1, inner):
        oproj[...] += rs_recv[q].astype(f32)
    store(oproj, proj_hbm)
    for copies in (
        copy_st, copy_rv, copy_tot, copy_gat, copy_sl, copy_hz, fwd_z,
        copy_rs, fwd_g, fwd_h, px, [copy_gh],
    ):
        for copy in copies:
            if copy is not None:
                copy.wait_send()
    for b in range(outer):
        for q in range(1, inner):
            hidden_copy(b, q).wait_send()
            cot_copy(b, q).wait_send()
    for k in range(1, n):
        return_copy(peers[k], peers[k]).wait_send()
    for s in range(outer - 1):
        send_cot(s, drain=True)
        send_hid(s, drain=True)
        send_mz(s, drain=True)
    for copy in stores:
        copy.wait()


def pass_through(count, *refs):
    ins, outs, held = refs[:count], refs[count:2 * count], refs[2 * count:3 * count]
    in_sem, out_sem = refs[3 * count:]
    reads = [pltpu.make_async_copy(ins[i], held[i], in_sem.at[i]) for i in range(count)]
    writes = [pltpu.make_async_copy(held[i], outs[i], out_sem.at[i]) for i in range(count)]
    for read in reads:
        read.start()
    for read, write in zip(reads, writes):
        read.wait()
        write.start()
    for write in writes:
        write.wait()


def hand_over(arrays):
    count = len(arrays)
    pieces = []
    for array in arrays:
        pieces.append(jax.ShapeDtypeStruct(array.shape, array.dtype))
    aspec = pl.BlockSpec(memory_space=pl.ANY)
    return pl.pallas_call(
        functools.partial(pass_through, count),
        out_shape=tuple(pieces),
        in_specs=[aspec] * count,
        out_specs=(aspec,) * count,
        scratch_shapes=[pltpu.VMEM(p.shape, p.dtype) for p in pieces]
        + [pltpu.SemaphoreType.DMA((count,))] * 2,
        name="hand_over",
    )(*arrays)


def fused_body(
    mixer_output, layer_cotangent, expert_choice, route_weight, gate_pre, up_pre,
    w_gate, w_up, w_down, w_out, norm_gain, scan_in, gate_in, b_proj, c_proj,
    log_decay, entry_state,
):
    n = lax.axis_size("sp")
    outer = 4
    inner = n // outer
    tokens, width = mixer_output.shape
    half = width // 2
    rows, units = gate_pre.shape[1:]
    cap = rows // n
    heads = log_decay.shape[1]
    channels = scan_in.shape[1]
    state_rows = heads * HEAD_DIM
    srows = state_rows // n
    groups = b_proj.shape[1] // STATE
    pairs = heads // 2
    dchunk = width // outer
    dcols = width // n
    vm = pltpu.VMEM
    dma = pltpu.SemaphoreType.DMA
    wide = jax.ShapeDtypeStruct
    vspec = pl.BlockSpec(memory_space=pltpu.VMEM)
    aspec = pl.BlockSpec(memory_space=pl.ANY)
    scratch = [
        vm((tokens, channels), bf16), vm((tokens, channels), bf16),
        vm((tokens, groups * STATE), bf16), vm((tokens, groups * STATE), bf16),
        vm((state_rows, STATE), f32), vm((dcols, channels), f32),
        vm((tokens, channels), bf16), vm((tokens, channels), bf16),
        vm((tokens, groups * STATE), bf16), vm((tokens, groups * STATE), bf16),
        vm((outer, tokens, half), bf16), vm((outer, tokens, half), bf16),
        vm((rows, units), bf16), vm((rows, units), bf16),
        vm((2, half, units), bf16), vm((2, half, units), bf16),
        vm((units, width), bf16), vm((channels, width), bf16),
        vm((outer, rows // outer, half), bf16), vm((outer, rows // outer, half), bf16),
        vm((2, rows, half), bf16), vm((2, rows, half), bf16),
        vm((outer, rows // outer, half), bf16), vm((outer, rows // outer, half), bf16),
        vm((rows, half), bf16), vm((rows, half), bf16),
        vm((rows, units), bf16), vm((rows, units), bf16), vm((rows, units), bf16),
        vm((tokens, rows), bf16),
        vm((outer, tokens, channels), bf16), vm((outer, tokens, dchunk), bf16),
        vm((outer, tokens, dchunk), bf16),
        vm((inner, dcols, channels), bf16), vm((inner, dcols, channels), bf16),
        vm((tokens, channels), f32), vm((tokens, channels), f32), vm((groups, tokens, 1), f32),
        vm((tokens, channels), f32), vm((pairs, tokens, 2 * tokens), bf16),
        vm((heads, tokens, tokens), f32), vm((tokens, heads), f32), vm((tokens, heads), f32),
        vm((state_rows, STATE), bf16), vm((groups, tokens, STATE), f32),
        vm((state_rows, STATE), bf16), vm((state_rows, STATE), bf16),
        vm((state_rows, STATE), bf16), vm((state_rows, STATE), bf16),
        vm((8, 128), f32), vm((n, 8, 128), f32), vm((outer, 8, tokens), f32),
        vm((heads, 128), f32), vm((n, heads, 128), f32),
        vm((2, half, units), bf16), vm((2, half, units), bf16), vm((2, units, half), bf16),
        dma((13,)), dma((9,)),
    ]
    scratch += [dma((n,))] * 10
    scratch += [dma((outer,))] * 8
    scratch += [dma((4, outer))] * 3 + [dma((outer, inner))] * 4
    scratch += [dma, dma]
    scratch += [dma((outer,))] * 4
    scratch += [dma((inner,))] * 2
    outs = pl.pallas_call(
        functools.partial(fused, (n, outer, cap)),
        out_shape=(
            wide((2, half, units), bf16), wide((2, half, units), bf16), wide((units, width), bf16),
            wide((dcols, channels), f32), wide((tokens, channels), bf16),
            wide((tokens, channels), bf16), wide((tokens, groups * STATE), bf16),
            wide((tokens, groups * STATE), bf16), wide((heads, tokens), f32),
        ),
        in_specs=[vspec] * 4 + [aspec] * 13,
        out_specs=(aspec,) * 8 + (vspec,),
        scratch_shapes=scratch,
        compiler_params=pltpu.CompilerParams(
            collective_id=0, has_side_effects=True, vmem_limit_bytes=64 * 1024 * 1024 - 128 * 1024
        ),
        name="fused",
    )(
        expert_choice.T, route_weight.T, log_decay.T,
        norm_gain.reshape(channels // 128, 128), scan_in, gate_in, b_proj, c_proj,
        entry_state.reshape(state_rows, STATE),
        layer_cotangent, mixer_output, gate_pre[0], up_pre[0],
        w_gate.reshape(2, half, units), w_up.reshape(2, half, units), w_down[0], w_out,
    )
    gwg, gwu, gwd, proj, gscan, ggate, gb, gc, gdecay = hand_over(outs)
    return (
        gwg.reshape(1, width, units), gwu.reshape(1, width, units), gwd[None],
        proj, gscan, ggate, gb, gc, gdecay.T,
    )


def entry_slots(expert_choice, expert_count, capacity):
    tokens, top_count = expert_choice.shape
    targets = expert_choice.reshape(-1)
    experts = jnp.arange(expert_count, dtype=jnp.int32)
    one_hot = (targets[:, None] == experts[None, :]).astype(jnp.float32)
    entries = jnp.arange(tokens * top_count, dtype=jnp.int32)
    before = (entries[:, None] > entries[None, :]).astype(jnp.bfloat16)
    earlier = jnp.dot(before, one_hot.astype(jnp.bfloat16), preferred_element_type=jnp.float32)
    ranks = jnp.sum(earlier * one_hot, axis=1).astype(jnp.int32)
    return (targets * capacity + ranks).reshape(tokens, top_count)


def expert_side(grad_rows, gate_value, up_value, gate_weight, up_weight, down_weight):
    act_grad = jnp.einsum("rd,fd->rf", grad_rows, down_weight, preferred_element_type=jnp.float32)
    gate_full = gate_value.astype(jnp.float32)
    up_full = up_value.astype(jnp.float32)
    gate_clip = jnp.minimum(gate_full, clamp_limit)
    up_clip = jnp.clip(up_full, -clamp_limit, clamp_limit)
    sigmoid_gate = jax.nn.sigmoid(swish_alpha * gate_clip)
    swish_gate = gate_clip * sigmoid_gate
    active = ((up_clip + 1.0) * swish_gate).astype(jnp.bfloat16)
    up_grad = jnp.where(
        (up_full > -clamp_limit) & (up_full < clamp_limit), act_grad * swish_gate, 0.0
    ).astype(jnp.bfloat16)
    slope = sigmoid_gate + swish_alpha * gate_clip * sigmoid_gate * (1.0 - sigmoid_gate)
    gate_grad = jnp.where(gate_full < clamp_limit, act_grad * (up_clip + 1.0) * slope, 0.0).astype(
        jnp.bfloat16
    )
    partial_rows = jnp.einsum(
        "rf,df->rd", gate_grad, gate_weight, preferred_element_type=jnp.float32
    )
    partial_rows = partial_rows + jnp.einsum(
        "rf,df->rd", up_grad, up_weight, preferred_element_type=jnp.float32
    )
    return (active, gate_grad, up_grad, partial_rows)


def exchange(pieces):
    return lax.all_to_all(pieces, "sp", split_axis=0, concat_axis=0, tiled=True)


def tell_all(vector):
    return exchange(jnp.broadcast_to(vector, (lax.axis_size("sp"), *vector.shape)))


def later_states(block_state, totals):
    count = lax.axis_size("sp")
    heads, channels, width = block_state.shape
    rows = heads * channels // count
    spots = jnp.arange(count)
    between = (
        (spots[:, None, None] < spots[None, None, :]) & (spots[None, None, :] < spots[None, :, None])
    ).astype(jnp.float32)
    gaps = jnp.einsum("bck,kh->bch", between, totals, precision=lax.Precision.HIGHEST)
    later = spots[:, None, None] < spots[None, :, None]
    weights = jnp.where(later, jnp.exp(gaps), 0.0)
    first = lax.axis_index("sp") * rows
    picks = (
        ((first + jnp.arange(rows)) // channels)[None, :] == jnp.arange(heads)[:, None]
    ).astype(jnp.float32)
    weights = jnp.einsum("bch,hr->bcr", weights, picks, precision=lax.Precision.HIGHEST)
    dealt = lax.all_to_all(
        block_state.astype(jnp.bfloat16).reshape(count, rows, width),
        "sp",
        split_axis=0,
        concat_axis=0,
        tiled=True,
    ).astype(jnp.float32)
    sums = jnp.sum(weights[:, :, :, None] * dealt[None], axis=1)
    back = lax.all_to_all(
        sums.astype(jnp.bfloat16), "sp", split_axis=0, concat_axis=0, tiled=True
    )
    return back.reshape(heads, channels, width)


def body(
    mixer_output,
    layer_cotangent,
    expert_choice,
    route_weight,
    gate_pre,
    up_pre,
    w_gate,
    w_up,
    w_down,
    w_out,
    norm_gain,
    scan_in,
    gate_in,
    b_proj,
    c_proj,
    log_decay,
    entry_state,
):
    expert_count = lax.axis_size("sp")
    tokens_here = mixer_output.shape[0]
    model_width = mixer_output.shape[1]
    top_count = expert_choice.shape[1]
    capacity = gate_pre.shape[1] // expert_count
    columns = model_width // lax.axis_size("tp")
    first_column = lax.axis_index("tp") * columns
    own_cotangent = lax.dynamic_slice_in_dim(layer_cotangent, first_column, columns, 1).astype(
        jnp.float32
    )
    own_hidden = lax.dynamic_slice_in_dim(mixer_output, first_column, columns, 1)
    slots = entry_slots(expert_choice, expert_count, capacity)
    slot_ids = jnp.arange(expert_count * capacity, dtype=jnp.int32)
    places = (slots.T[:, None, :] == slot_ids[None, :, None]).astype(jnp.bfloat16)
    token_places = places.sum(axis=0)
    weighted = (route_weight.T[:, :, None] * own_cotangent[None]).astype(jnp.bfloat16)

    def dispatch(rows):
        arrived = lax.all_to_all(
            rows.astype(jnp.bfloat16).reshape(expert_count, capacity, columns),
            "sp",
            split_axis=0,
            concat_axis=0,
            tiled=True,
        ).reshape(-1, columns)
        return lax.all_gather(arrived, "tp", axis=1, tiled=True)

    recv_grads = dispatch(
        jnp.einsum("kst,ktd->sd", places, weighted, preferred_element_type=jnp.float32)
    )
    active, gate_grad, up_grad, partial_rows = expert_side(
        recv_grads,
        gate_pre[0],
        up_pre[0],
        w_gate[0],
        w_up[0],
        w_down[0],
    )
    summed = lax.psum_scatter(
        partial_rows.astype(jnp.bfloat16), "tp", scatter_dimension=1, tiled=True
    )
    returned = lax.all_to_all(
        summed.reshape(expert_count, capacity, -1), "sp", split_axis=0, concat_axis=0, tiled=True
    )
    head_count = log_decay.shape[1]
    group_count = b_proj.shape[1] // STATE
    per_group = head_count // group_count
    scan_heads = scan_in.reshape(tokens_here, head_count, HEAD_DIM)
    b_groups = b_proj.reshape(tokens_here, group_count, STATE)
    c_groups = c_proj.reshape(tokens_here, group_count, STATE)
    x_float = scan_heads.astype(jnp.float32)
    token_locations = jnp.arange(tokens_here)
    causal = token_locations[:, None] >= token_locations[None, :]
    causal_float = causal.astype(jnp.float32)
    cumulative = jnp.dot(causal_float, log_decay, precision=lax.Precision.HIGHEST)
    growth = jnp.exp(cumulative)
    block_decays = tell_all(lax.optimization_barrier((cumulative[-1], summed))[0])
    tail_decay = jnp.exp(cumulative[-1][None, :] - cumulative)
    log_gaps = cumulative.T[:, :, None] - cumulative.T[:, None, :]
    decay_mat = jnp.exp(jnp.where(causal[None], log_gaps, -jnp.inf))
    inner_prod = jnp.einsum("tgn,sgn->gts", c_groups, b_groups, preferred_element_type=jnp.float32)
    mix_weights = (jnp.repeat(inner_prod, per_group, axis=0) * decay_mat).astype(jnp.bfloat16)
    state_groups = entry_state.astype(jnp.bfloat16).reshape(group_count, per_group, HEAD_DIM, STATE)
    y_inner = jnp.einsum(
        "hts,shp->thp", mix_weights, scan_heads, preferred_element_type=jnp.float32
    )
    y_carry = jnp.einsum(
        "tgn,grpn->tgrp", c_groups, state_groups, preferred_element_type=jnp.float32
    ).reshape(tokens_here, head_count, HEAD_DIM)
    scan_out = y_inner + y_carry * growth[:, :, None]
    gate_float = gate_in.astype(jnp.float32)
    gate_sig = jax.nn.sigmoid(gate_float)
    gate_silu = gate_float * gate_sig
    gated = scan_out.reshape(tokens_here, -1) * gate_silu
    grouped = gated.reshape(tokens_here, group_count, -1)
    inv_rms = lax.rsqrt(jnp.mean(grouped * grouped, axis=-1, keepdims=True) + rms_epsilon)
    unit = grouped * inv_rms
    gain_groups = norm_gain.astype(jnp.float32).reshape(group_count, -1)
    mixed = (unit * gain_groups).reshape(tokens_here, -1).astype(jnp.bfloat16)
    all_mixed = lax.all_gather(mixed, "sp", axis=0, tiled=True)
    returned, mixed = lax.optimization_barrier((returned, mixed))
    moe_terms = jnp.einsum(
        "st,sd->td",
        token_places,
        returned.reshape(-1, columns),
        preferred_element_type=jnp.float32,
    )
    grad_hidden = lax.all_gather(
        (own_cotangent + moe_terms).astype(jnp.bfloat16), "tp", axis=1, tiled=True
    )
    late_hidden, grad_hidden = lax.optimization_barrier((own_hidden, grad_hidden))
    recv_hidden = dispatch(
        jnp.einsum("st,td->sd", token_places, late_hidden, preferred_element_type=jnp.float32)
    )
    down_wgrad = jnp.einsum(
        "rf,rd->fd", active, recv_grads, preferred_element_type=jnp.float32
    ).astype(jnp.bfloat16)
    gate_wgrad = jnp.einsum(
        "rd,rf->df", recv_hidden, gate_grad, preferred_element_type=jnp.float32
    ).astype(jnp.bfloat16)
    up_wgrad = jnp.einsum(
        "rd,rf->df", recv_hidden, up_grad, preferred_element_type=jnp.float32
    ).astype(jnp.bfloat16)
    own_block = lax.all_to_all(
        grad_hidden.reshape(tokens_here, expert_count, -1).transpose(1, 0, 2),
        "sp",
        split_axis=0,
        concat_axis=0,
        tiled=True,
    )
    grad_out_proj = jnp.einsum(
        "td,ti->di",
        own_block.reshape(-1, own_block.shape[2]),
        all_mixed,
        preferred_element_type=jnp.float32,
    )
    grad_mixed = jnp.einsum("td,id->ti", grad_hidden, w_out, preferred_element_type=jnp.float32)
    grad_unit = grad_mixed.reshape(tokens_here, group_count, -1) * gain_groups
    grad_grouped = inv_rms * (grad_unit - unit * jnp.mean(grad_unit * unit, axis=-1, keepdims=True))
    grad_gated = grad_grouped.reshape(tokens_here, -1)
    grad_gate_in = (
        grad_gated
        * scan_out.reshape(tokens_here, -1)
        * gate_sig
        * (1.0 + gate_float * (1.0 - gate_sig))
    ).astype(jnp.bfloat16)
    grad_y = (grad_gated * gate_silu).reshape(tokens_here, head_count, HEAD_DIM)
    grad_y_b = grad_y.astype(jnp.bfloat16)
    grad_x_inner = jnp.einsum(
        "hts,thp->shp", mix_weights, grad_y_b, preferred_element_type=jnp.float32
    )
    grad_weights = (
        jnp.einsum("thp,shp->hts", grad_y_b, scan_heads, preferred_element_type=jnp.float32)
        * decay_mat
    )
    grad_weights = (
        grad_weights.reshape(group_count, per_group, tokens_here, tokens_here)
        .sum(axis=1)
        .astype(jnp.bfloat16)
    )
    grad_c_inner = jnp.einsum(
        "gts,sgn->tgn", grad_weights, b_groups, preferred_element_type=jnp.float32
    )
    grad_b_inner = jnp.einsum(
        "gts,tgn->sgn", grad_weights, c_groups, preferred_element_type=jnp.float32
    )
    grown_grads = (grad_y * growth[:, :, None]).astype(jnp.bfloat16).reshape(
        tokens_here, group_count, per_group, HEAD_DIM
    )
    grad_c_carry = jnp.einsum(
        "tgrp,grpn->tgn", grown_grads, state_groups, preferred_element_type=jnp.float32
    )
    block_state = jnp.einsum(
        "tgrp,tgn->grpn", grown_grads, c_groups, preferred_element_type=jnp.float32
    ).reshape(head_count, HEAD_DIM, STATE)
    x_tail = (x_float * tail_decay[:, :, None]).astype(jnp.bfloat16).reshape(
        tokens_here, group_count, per_group, HEAD_DIM
    )
    later_state = later_states(block_state, block_decays)
    later_groups = later_state.reshape(group_count, per_group, HEAD_DIM, STATE)
    grad_x_carry = jnp.einsum(
        "sgn,grpn->sgrp", b_groups, later_groups, preferred_element_type=jnp.float32
    ).reshape(tokens_here, head_count, HEAD_DIM)
    grad_x = grad_x_inner + grad_x_carry * tail_decay[:, :, None]
    grad_b_carry = jnp.einsum(
        "sgrp,grpn->sgn", x_tail, later_groups, preferred_element_type=jnp.float32
    )
    grad_a = jnp.sum(grad_y * scan_out, axis=2) - jnp.sum(x_float * grad_x, axis=2)
    block_totals = tell_all(jnp.sum(grad_a, axis=0))
    is_later = jnp.arange(expert_count) > lax.axis_index("sp")
    later_grad = jnp.sum(jnp.where(is_later[:, None], block_totals, 0.0), axis=0)
    grad_log_decay = (
        jnp.dot(causal_float.T, grad_a, precision=lax.Precision.HIGHEST) + later_grad[None, :]
    )
    grad_scan_in = grad_x.reshape(tokens_here, -1).astype(jnp.bfloat16)
    grad_b_proj = (grad_b_inner + grad_b_carry).reshape(tokens_here, -1).astype(jnp.bfloat16)
    grad_c_proj = (grad_c_inner + grad_c_carry).reshape(tokens_here, -1).astype(jnp.bfloat16)
    return (
        gate_wgrad[None],
        up_wgrad[None],
        down_wgrad[None],
        grad_out_proj,
        grad_scan_in,
        grad_gate_in,
        grad_b_proj,
        grad_c_proj,
        grad_log_decay,
    )


def solution(mesh):
    in_specs = (
        P("sp", None),
        P("sp", None),
        P("sp", None),
        P("sp", None),
        P("sp", None, "tp"),
        P("sp", None, "tp"),
        P("sp", None, "tp"),
        P("sp", None, "tp"),
        P("sp", "tp", None),
        P("tp", None),
        P("tp"),
        P("sp", "tp"),
        P("sp", "tp"),
        P("sp", "tp"),
        P("sp", "tp"),
        P("sp", "tp"),
        P("sp", "tp", None, None),
    )
    out_specs = (
        P("sp", None, "tp"),
        P("sp", None, "tp"),
        P("sp", "tp", None),
        P("sp", "tp"),
        P("sp", "tp"),
        P("sp", "tp"),
        P("sp", "tp"),
        P("sp", "tp"),
        P("sp", "tp"),
    )
    def run(*args):
        count = mesh.shape["sp"]
        capacity = args[4].shape[1] // count
        simple = mesh.shape["tp"] != 2 or count % 4 or count & (count - 1) or capacity % 16
        return (body if simple else fused_body)(*args)

    return jax.shard_map(run, mesh=mesh, in_specs=in_specs, out_specs=out_specs, check_vma=False)
```
